32 devices in a mesh: sp: 4 (over z), fs: 4 (over y, x), tp: 2 (over core).
Axes of the slice: x: 2, y: 2, z: 4, core: 2. Of those that a mesh axis runs over, the one named last changes fastest.
Arguments:
- tokens: bfloat16 [4, 4096, 2048], P('fs', ('sp', 'tp')), may hold values from -6 to 6
- norm_gain: float32 [2048], replicated, may hold values from 0.1 to 1.9
- w_gate: bfloat16 [2048, 1024], P(('sp', 'fs'), 'tp'), may hold values from -0.125 to 0.125
- w_value: bfloat16 [2048, 1024], P(('sp', 'fs'), 'tp'), may hold values from -0.125 to 0.125
- w_bkey: bfloat16 [2048, 1024], P(('sp', 'fs'), 'tp'), may hold values from -0.125 to 0.125
- w_query: bfloat16 [2048, 1024], P(('sp', 'fs'), 'tp'), may hold values from -0.125 to 0.125
- w_pool_in: bfloat16 [2048, 1024], P(('sp', 'fs'), 'tp'), may hold values from -0.125 to 0.125
- w_step: bfloat16 [2048, 2, 16], replicated, may hold values from -0.125 to 0.125
- step_bias: float32 [2, 16], replicated, may hold values from -1 to 1
- decay_rate: float32 [2, 16], replicated, may hold values from 4.8828125e-06 to 0.06
- decay_shift: float32 [4, 16, 2, 4096], P('fs', 'tp', None, 'sp'), may hold values from 0 to 2.2
- conv_value: bfloat16 [5, 1024], replicated, may hold values from -2.5 to 2.5
- conv_bkey: bfloat16 [5, 1024], replicated, may hold values from -2.5 to 2.5
- conv_query: bfloat16 [5, 1024], replicated, may hold values from -2.5 to 2.5
- mix_gain: float32 [1024], replicated, may hold values from 0.1 to 1.9
- pool_mix: bfloat16 [8, 128, 128], replicated, may hold values from -0.5 to 0.5
- pool_gain: float32 [1024], replicated, may hold values from 0.1 to 1.9
- w_out_ssd: bfloat16 [1024, 2048], P('tp', ('sp', 'fs')), may hold values from -0.125 to 0.125
- w_out_pool: bfloat16 [1024, 2048], P('tp', ('sp', 'fs')), may hold values from -0.125 to 0.125
Outputs:
- mixed: bfloat16 [4, 4096, 2048], P('fs', ('sp', 'tp'))
The draws below stay inside these ranges and needn't reach their ends.
All inputs are finite; a program needn't handle non-finite values.
Results may differ from the reference program's by a relative error of at most 0.014.
Values may be sent and summed in bfloat16 or wider, within the bound.
A program may use at most 128 MiB of HBM per device.

```python
import jax
import jax.numpy as jnp
from jax import lax

D = 2048
HEAD_DIM = 64
DUALITY_HEADS = 16
GROUPS = 8
STATE = 128
CONV_WIDTH = 5
POOL_GROUPS = 8
POOL_DIM = 128
SPAN = 128
TOK_SP = 1024
SEQUENCE_LENGTH = 4096
BATCH_SEQUENCES = 4
D_SSM = 1024
D_POOL = 1024
N_TP = 2


def draw_decay_rate(key, part):
    order_key, slow_key, fast_key = jax.random.split(jax.random.fold_in(key, 11), 3)
    ranking = jax.random.permutation(order_key, 2 * DUALITY_HEADS)
    slow_count = DUALITY_HEADS
    slow_rate = jax.random.uniform(slow_key, (2 * DUALITY_HEADS,), jnp.float32, 0.02, 0.2) / SEQUENCE_LENGTH
    fast_rate = jax.random.uniform(fast_key, (2 * DUALITY_HEADS,), jnp.float32, 0.02, 0.06)
    rates = jnp.where(ranking < slow_count, slow_rate, fast_rate)
    return rates.reshape(2, DUALITY_HEADS).astype(jnp.float32)


def draw_decay_shift(key, part):
    random_keys = jax.random.split(jax.random.fold_in(key, 23), 4)
    token_position = jnp.arange(SEQUENCE_LENGTH, dtype=jnp.int32)
    segment = token_position // TOK_SP
    segments = SEQUENCE_LENGTH // TOK_SP
    low_end, high_end = (0.4, 2.5)
    factor = jnp.exp(jax.random.uniform(random_keys[0], (BATCH_SEQUENCES, DUALITY_HEADS, 2, segments), jnp.float32, jnp.log(low_end), jnp.log(high_end)))
    roughness = jax.random.uniform(random_keys[1], (BATCH_SEQUENCES, DUALITY_HEADS, 2, SEQUENCE_LENGTH), jnp.float32, 0.5, 1.5)
    reference_level = jnp.take(factor, segment, axis=3) * roughness * (0.3 / SEQUENCE_LENGTH)
    spike_places = jax.random.randint(random_keys[2], (BATCH_SEQUENCES, DUALITY_HEADS, 2, 3), 0, SEQUENCE_LENGTH)
    spike_length = jax.random.uniform(random_keys[3], (BATCH_SEQUENCES, DUALITY_HEADS, 2, 3), jnp.float32, 0.22, 0.69)
    match_count = (token_position[None, None, None, None, :] == spike_places[..., None]).astype(jnp.float32)
    spike_runs = jnp.sum(match_count * spike_length[..., None], axis=3)
    return (reference_level + spike_runs).astype(jnp.float32)


def levels(stream_key, shape, pieces, low, top_value):
    loudness = 1.0
    for dim, parts in pieces:
        steps = jax.random.uniform(jax.random.fold_in(jax.random.fold_in(stream_key, 6), dim), (parts,), jnp.float32, low / len(pieces), top_value / len(pieces))
        loudness = loudness * jnp.repeat(jnp.exp(steps), shape[dim] // parts).reshape((-1,) + (1,) * (len(shape) - 1 - dim))
    return loudness


def gaussian(own_key, extent, deviation, bound, cuts=(), held_as=jnp.bfloat16):
    array = deviation * jax.random.normal(own_key, extent, jnp.float32)
    if cuts:
        array = array * levels(own_key, extent, cuts, -0.22, 0.18)
    return jnp.clip(array, -bound, bound).astype(held_as)


def setup_inputs(seed: int = 0) -> dict:
    splits = jax.random.split(jax.random.key(seed), 20)
    tokens = gaussian(splits[0], (BATCH_SEQUENCES, SEQUENCE_LENGTH, D), 1.0, 6.0, ((0, 4), (1, 8)))
    norm_gain = jnp.clip(1.0 + 0.18 * jax.random.normal(splits[1], (D,), jnp.float32), 0.1, 1.9)
    w_gate = gaussian(splits[2], (D, D_SSM), D ** -0.5, 0.125, ((0, 16), (1, 2)))
    w_value = gaussian(splits[3], (D, D_SSM), D ** -0.5, 0.125, ((0, 16), (1, 2)))
    w_bkey = gaussian(splits[4], (D, GROUPS * STATE), D ** -0.5, 0.125, ((0, 16), (1, 2)))
    w_query = gaussian(splits[5], (D, GROUPS * STATE), D ** -0.5, 0.125, ((0, 16), (1, 2)))
    w_pool_in = gaussian(splits[6], (D, D_POOL), D ** -0.5, 0.125, ((0, 16), (1, 2)))
    w_step = gaussian(splits[7], (D, 2, DUALITY_HEADS), D ** -0.5, 0.125)
    step_bias = jnp.clip(jax.random.uniform(splits[8], (2, DUALITY_HEADS), jnp.float32, -1.0, 1.0), -1.0, 1.0)
    decay_rate = draw_decay_rate(jax.random.fold_in(splits[19], 71), 0)
    decay_shift = draw_decay_shift(jax.random.fold_in(splits[19], 71), 0)
    conv_value = gaussian(splits[11], (CONV_WIDTH, D_SSM), CONV_WIDTH ** -0.5, 2.5)
    conv_bkey = gaussian(splits[12], (CONV_WIDTH, GROUPS * STATE), CONV_WIDTH ** -0.5, 2.5)
    conv_query = gaussian(splits[13], (CONV_WIDTH, GROUPS * STATE), CONV_WIDTH ** -0.5, 2.5)
    mix_gain = jnp.clip(1.0 + 0.18 * jax.random.normal(splits[14], (D_SSM,), jnp.float32), 0.1, 1.9)
    pool_mix = gaussian(splits[15], (POOL_GROUPS, POOL_DIM, POOL_DIM), POOL_DIM ** -0.5, 0.5)
    pool_gain = jnp.clip(1.0 + 0.18 * jax.random.normal(splits[16], (D_POOL,), jnp.float32), 0.1, 1.9)
    w_out_ssd = gaussian(splits[17], (D_SSM, D), (D_SSM + D_POOL) ** -0.5, 0.125, ((0, 2), (1, 16)))
    w_out_pool = gaussian(splits[18], (D_POOL, D), (D_SSM + D_POOL) ** -0.5, 0.125, ((0, 2), (1, 16)))
    return {"tokens": tokens, "norm_gain": norm_gain, "w_gate": w_gate, "w_value": w_value, "w_bkey": w_bkey, "w_query": w_query, "w_pool_in": w_pool_in, "w_step": w_step, "step_bias": step_bias, "decay_rate": decay_rate, "decay_shift": decay_shift, "conv_value": conv_value, "conv_bkey": conv_bkey, "conv_query": conv_query, "mix_gain": mix_gain, "pool_mix": pool_mix, "pool_gain": pool_gain, "w_out_ssd": w_out_ssd, "w_out_pool": w_out_pool}


EPSILON = 1e-06
HIGHEST = lax.Precision.HIGHEST
WINDOWS = (2, 4, 8, 16)

def blockwise(values, bkeys, queries, steps, logs):
    length, heads, head_width = values.shape
    groups, state_width = (bkeys.shape[1], bkeys.shape[2])
    per_group = heads // groups
    blocks = length // SPAN
    weighted = (values * jnp.transpose(steps)[:, :, None]).reshape(blocks, SPAN, groups, per_group, head_width)
    key_blocks = bkeys.reshape(blocks, SPAN, groups, state_width)
    query_blocks = queries.reshape(blocks, SPAN, groups, state_width)
    inner = jnp.cumsum(logs.reshape(heads, blocks, SPAN), axis=-1)
    lower = jnp.tril(jnp.ones((SPAN, SPAN), dtype=bool))
    within = jnp.exp(jnp.where(lower, inner[..., :, None] - inner[..., None, :], -jnp.inf))
    within = within.reshape(groups, per_group, blocks, SPAN, SPAN)
    scores = jnp.einsum('clgn,csgn->cgls', query_blocks, key_blocks, precision=HIGHEST)
    diagonal = jnp.einsum('cgls,gkcls,csgkp->clgkp', scores, within, weighted, precision=HIGHEST)
    tails = jnp.exp(inner[..., -1:] - inner).reshape(groups, per_group, blocks, SPAN)
    ends = jnp.einsum('clgn,gkcl,clgkp->cgkpn', key_blocks, tails, weighted, precision=HIGHEST)
    totals = inner[..., -1]
    upto = jnp.cumsum(totals, axis=-1)
    before = upto - totals
    block_ids = jnp.arange(blocks, dtype=jnp.int32)
    earlier = block_ids[None, :] < block_ids[:, None]
    between = jnp.exp(jnp.where(earlier[None], before[:, :, None] - upto[:, None, :], -jnp.inf))
    between = between.reshape(groups, per_group, blocks, blocks)
    prior = jnp.einsum('gkcj,jgkpn->cgkpn', between, ends, precision=HIGHEST)
    reach = jnp.exp(inner).reshape(groups, per_group, blocks, SPAN)
    offdiag = jnp.einsum('clgn,cgkpn,gkcl->clgkp', query_blocks, prior, reach, precision=HIGHEST)
    return (diagonal + offdiag).reshape(length, heads, head_width)

def centred(projected, taps):
    margin = CONV_WIDTH // 2
    length = projected.shape[0]
    padded = jnp.pad(projected, ((margin, margin), (0, 0)))
    running = jnp.zeros(projected.shape, jnp.float32)
    for offset in range(CONV_WIDTH):
        running = running + padded[offset:offset + length].astype(jnp.float32) * taps[offset].astype(jnp.float32)
    return running

def box_mean(column, window):
    length = column.shape[0]
    prefix = jnp.pad(jnp.cumsum(column, axis=0), ((1, 0), (0, 0)))
    where_now = jnp.arange(length, dtype=jnp.int32)
    lower = jnp.clip(where_now - window // 2, 0, length).astype(jnp.int32)
    upper = jnp.clip(where_now + window - window // 2, 0, length).astype(jnp.int32)
    counts = (upper - lower).astype(jnp.float32)
    return (prefix[upper] - prefix[lower]) / counts[:, None]

def reference(tokens, norm_gain, w_gate, w_value, w_bkey, w_query, w_pool_in, w_step, step_bias, decay_rate, decay_shift, conv_value, conv_bkey, conv_query, mix_gain, pool_mix, pool_gain, w_out_ssd, w_out_pool):

    def one_sequence(paired):
        rows, shift = paired
        length = rows.shape[0]
        widened = rows.astype(jnp.float32)
        normed = (widened * lax.rsqrt(lax.optimization_barrier(jnp.mean(widened * widened, axis=-1, keepdims=True)) + EPSILON) * norm_gain).astype(jnp.bfloat16)
        gate = jnp.dot(normed, w_gate, preferred_element_type=jnp.float32).astype(jnp.bfloat16)
        value = jnp.dot(normed, w_value, preferred_element_type=jnp.float32).astype(jnp.bfloat16)
        bkey = jnp.dot(normed, w_bkey, preferred_element_type=jnp.float32).astype(jnp.bfloat16)
        query = jnp.dot(normed, w_query, preferred_element_type=jnp.float32).astype(jnp.bfloat16)
        pooled = jnp.dot(normed, w_pool_in, preferred_element_type=jnp.float32).astype(jnp.bfloat16)
        raw_steps = jnp.dot(normed, w_step.reshape(D, 2 * DUALITY_HEADS), preferred_element_type=jnp.float32)
        steps = jax.nn.softplus(raw_steps.reshape(length, 2, DUALITY_HEADS) + step_bias).transpose(1, 2, 0)
        logs = -decay_rate[:, :, None] * steps - shift.transpose(1, 0, 2)
        values = jax.nn.silu(centred(value, conv_value)).reshape(length, DUALITY_HEADS, HEAD_DIM)
        bkeys = jax.nn.silu(centred(bkey, conv_bkey)).reshape(length, GROUPS, STATE)
        queries = jax.nn.silu(centred(query, conv_query)).reshape(length, GROUPS, STATE)
        forward = blockwise(values, bkeys, queries, steps[0], logs[0])
        backward = blockwise(values[::-1], bkeys[::-1], queries[::-1], steps[1][:, ::-1], logs[1][:, ::-1])[::-1]
        heads_out = forward + backward
        gated = heads_out.reshape(length, D_SSM) * jax.nn.silu(gate.astype(jnp.float32))
        ssd_mix = (gated * lax.rsqrt(lax.optimization_barrier(jnp.mean(gated * gated, axis=-1, keepdims=True)) + EPSILON) * mix_gain).astype(jnp.bfloat16)
        pool_rows = pooled.astype(jnp.float32).reshape(length, POOL_GROUPS, POOL_DIM)
        differences = []
        for group in range(POOL_GROUPS):
            column = pool_rows[:, group]
            differences.append(box_mean(column, WINDOWS[group % 4]) - column)
        pool_diff = jnp.stack(differences, axis=1).astype(jnp.bfloat16)
        mapped = jnp.einsum('sgc,gcd->sgd', pool_diff.astype(jnp.float32), pool_mix.astype(jnp.float32))
        pool_out = (mapped.reshape(length, D_POOL) * pool_gain).astype(jnp.bfloat16)
        ssd_part = D_SSM // N_TP
        pool_part = D_POOL // N_TP
        summed = jnp.zeros((length, D), jnp.float32)
        for member in range(N_TP):
            partial_value = jnp.dot(ssd_mix[:, member * ssd_part:(member + 1) * ssd_part], w_out_ssd[member * ssd_part:(member + 1) * ssd_part], preferred_element_type=jnp.float32)
            partial_value = partial_value + jnp.dot(pool_out[:, member * pool_part:(member + 1) * pool_part], w_out_pool[member * pool_part:(member + 1) * pool_part], preferred_element_type=jnp.float32)
            rounded = lax.optimization_barrier(partial_value.astype(jnp.bfloat16))
            summed = summed + rounded.astype(jnp.float32)
        return summed.astype(jnp.bfloat16)
    return lax.map(one_sequence, (tokens, decay_shift))
```

```python
import functools

import jax
import jax.numpy as jnp
from jax import lax
from jax.experimental import pallas as pl
from jax.experimental.pallas import tpu as pltpu
from jax.sharding import PartitionSpec as P

HEAD_DIM = 64
DUALITY_HEADS = 16
GROUPS = 8
STATE = 128
CONV_WIDTH = 5
POOL_GROUPS = 8
POOL_DIM = 128
SPAN = 128
REACH = 8
D_SSM = 1024


EPSILON = 1e-06
HIGHEST = lax.Precision.HIGHEST
WINDOWS = (2, 4, 8, 16)


def padded_2(cells, sides, width):
    for axis, dim in sides:
        count = lax.axis_size(axis)
        ends = count - 1
        head = lax.slice_in_dim(cells, 0, width, axis=dim)
        tail = lax.slice_in_dim(cells, cells.shape[dim] - width, cells.shape[dim], axis=dim)
        cells = jnp.concatenate(
            [
                lax.ppermute(tail, axis, [(i, (i + 1) % count) for i in range(ends)]),
                cells,
                lax.ppermute(head, axis, [((i + 1) % count, i) for i in range(ends)]),
            ],
            axis=dim,
        )
    return cells


MESH = pl.DeviceIdType.MESH


def gather_kernel(n_sp, n_tp, w_ref, t_ref, w_out, t_out, send, recv, local_sem):
    z = lax.axis_index("sp")
    f = lax.axis_index("fs")
    c = lax.axis_index("tp")
    fx = f + 1 - 2 * lax.rem(f, 2)
    fy = lax.rem(f + 2, 4)
    rows = w_ref.shape[0]
    half = rows // 2
    x_dev = (z, fx, c)
    y_dev = (z, fy, c)
    z_devs = [(lax.rem(z + d, n_sp), f, c) for d in range(1, n_sp)]
    t_devs = [(z, f, lax.rem(c + d, n_tp)) for d in range(1, n_tp)]
    partners = [x_dev, y_dev] + z_devs + t_devs
    barrier = pltpu.get_barrier_semaphore()
    for dev in partners:
        pl.semaphore_signal(barrier, inc=1, device_id=dev, device_id_type=MESH)
    pl.semaphore_wait(barrier, len(partners))

    def remote(src, dst, index, dev):
        copy = pltpu.make_async_remote_copy(
            src_ref=src,
            dst_ref=dst,
            send_sem=send.at[index],
            recv_sem=recv.at[index],
            device_id=dev,
            device_id_type=MESH,
        )
        copy.start()
        return copy

    base = n_sp - 1
    z_copies = [remote(w_ref, w_out.at[z, f], d, z_devs[d]) for d in range(n_sp - 1)]
    full = []
    relay = []

    def send_full(d):
        if d == 0:
            src = w_ref
            origin = z
        else:
            z_copies[d - 1].wait_recv()
            origin = lax.rem(z - d + n_sp, n_sp)
            src = w_out.at[origin, f]
        dst = w_out.at[origin, f]
        full.append(
            (
                remote(src, dst, base + 4 * d, x_dev),
                remote(src, dst, base + 4 * d + 1, y_dev),
            )
        )

    def send_relay(d):
        origin = lax.rem(z - d + n_sp, n_sp)
        full[d][0].wait_recv()
        part = w_out.at[origin, fx, pl.ds(0, half)]
        first = remote(part, part, base + 4 * d + 2, y_dev)
        full[d][1].wait_recv()
        part = w_out.at[origin, fy, pl.ds(half, half)]
        relay.append((first, remote(part, part, base + 4 * d + 3, x_dev)))

    send_full(0)
    own_w = pltpu.make_async_copy(w_ref, w_out.at[z, f], local_sem.at[0])
    own_w.start()
    own_t = pltpu.make_async_copy(t_ref, t_out.at[c], local_sem.at[1])
    own_t.start()
    tbase = base + 4 * n_sp
    t_copies = [remote(t_ref, t_out.at[c], tbase + d, t_devs[d]) for d in range(n_tp - 1)]
    for d in range(1, n_sp):
        send_full(d)
        send_relay(d - 1)
    send_relay(n_sp - 1)
    for pair in relay:
        for copy in pair:
            copy.wait_recv()
    for copy in t_copies:
        copy.wait_recv()
    for copy in z_copies + t_copies:
        copy.wait_send()
    for pair in full + relay:
        for copy in pair:
            copy.wait_send()
    own_w.wait()
    own_t.wait()


def gather_inputs(weights, tokens):
    n_sp = lax.axis_size("sp")
    n_fs = lax.axis_size("fs")
    n_tp = lax.axis_size("tp")
    rows, cols = weights.shape
    if n_fs != 4:
        return (
            lax.all_gather(weights, ("sp", "fs"), axis=0, tiled=True),
            lax.all_gather(tokens, "tp", axis=0, tiled=True),
        )
    count = (n_sp - 1) + 4 * n_sp + (n_tp - 1)
    wide, toks = pl.pallas_call(
        functools.partial(gather_kernel, n_sp, n_tp),
        out_shape=(
            jax.ShapeDtypeStruct((n_sp, n_fs, rows, cols), weights.dtype),
            jax.ShapeDtypeStruct((n_tp,) + tokens.shape, tokens.dtype),
        ),
        in_specs=[pl.BlockSpec(memory_space=pltpu.VMEM)] * 2,
        out_specs=[pl.BlockSpec(memory_space=pl.ANY)] * 2,
        scratch_shapes=[
            pltpu.SemaphoreType.DMA((count,)),
            pltpu.SemaphoreType.DMA((count,)),
            pltpu.SemaphoreType.DMA((2,)),
        ],
        compiler_params=pltpu.CompilerParams(collective_id=0, has_side_effects=True),
        cost_estimate=pl.CostEstimate(
            flops=0, bytes_accessed=200 * n_sp * n_fs * rows * cols, transcendentals=0
        ),
        name="gather_inputs",
    )(weights, tokens)
    return wide.reshape(n_sp * n_fs * rows, cols), toks.reshape(-1, tokens.shape[1])


class LineGather:
    def __init__(self, own, piece, send, recv):
        self.n = lax.axis_size("sp")
        self.z = lax.axis_index("sp")
        self.f = lax.axis_index("fs")
        self.c = lax.axis_index("tp")
        self.fx = self.f + 1 - 2 * lax.rem(self.f, 2)
        self.fy = lax.rem(self.f + 2, 4)
        self.fd = 3 - self.f
        self.own, self.piece, self.send, self.recv = own, piece, send, recv
        self.x_dev = (self.z, self.fx, self.c)
        self.y_dev = (self.z, self.fy, self.c)
        self.up_dev = (lax.rem(self.z + 1, self.n), self.f, self.c)
        self.down_dev = (lax.rem(self.z + self.n - 1, self.n), self.f, self.c)
        self.order = [self.nearest(k) for k in range(self.n)]
        self.pending = []

    def barrier(self, extra=()):
        barrier = pltpu.get_barrier_semaphore()
        devices = [self.x_dev, self.y_dev, self.up_dev, self.down_dev, *extra]
        for device in devices:
            pl.semaphore_signal(barrier, inc=1, device_id=device, device_id_type=MESH)
        pl.semaphore_wait(barrier, len(devices))

    def nearest(self, k):
        z, n = self.z, self.n
        low = jnp.minimum(z, n - 1 - z)
        sign = 1 if k % 2 == 0 else -1
        paired = z + sign * ((k + 1) // 2)
        past = jnp.where(2 * z < n - 1, z + (k - low), z - (k - low))
        return jnp.where(k <= 2 * low, paired, past)

    def by_line(self, z, p):
        near = jnp.logical_or(p == z + 1, p == z - 1)
        if self.n >= 4:
            near = jnp.logical_or(near, jnp.logical_and(z == 0, p == 2))
            near = jnp.logical_or(near, jnp.logical_and(z == self.n - 1, p == self.n - 3))
        return near

    def copy(self, src, dst, p, s, r, device):
        return pltpu.make_async_remote_copy(
            src_ref=src,
            dst_ref=dst,
            send_sem=self.send.at[p, s],
            recv_sem=self.recv.at[p, r],
            device_id=device,
            device_id_type=MESH,
        )

    def start(self, cond, src, dst, p, s, r, device):
        copy = self.copy(src, dst, p, s, r, device)
        if cond is None:
            copy.start()
        else:
            pl.when(cond)(copy.start)
        self.pending.append((cond, copy))

    def arrive(self, ref, p, r):
        self.copy(ref, ref, p, 0, r, self.x_dev).wait_recv()

    def column(self, k):
        p = self.order[k]
        up = jnp.logical_and(p <= self.z, self.z < self.n - 1)
        down = jnp.logical_and(p >= self.z, self.z > 0)
        for h in range(2):
            ref = self.piece(p, self.f, h)
            src = ref
            if k == 0:
                src = self.own(h)
            else:
                self.arrive(ref, p, h)
            self.start(None, src, ref, p, 4 + h, 2 + h, self.x_dev)
            self.start(None, src, ref, p, 6 + h, 4 + h, self.y_dev)
            self.start(up, src, ref, p, h, h, self.up_dev)
            self.start(down, src, ref, p, 2 + h, h, self.down_dev)

    def sides(self, k):
        p = self.order[k]
        relay = jnp.logical_not(self.by_line(self.z, p))
        for h in range(2):
            x_part = self.piece(p, self.fx, h)
            y_part = self.piece(p, self.fy, h)
            self.arrive(x_part, p, 2 + h)
            if h == 0:
                self.start(relay, x_part, x_part, p, 8, 6, self.y_dev)
            self.arrive(y_part, p, 4 + h)
            if h == 1:
                self.start(relay, y_part, y_part, p, 9, 7, self.x_dev)

    def diagonal(self, k):
        p = self.order[k]
        z, n = self.z, self.n
        up = jnp.logical_and(jnp.logical_and(p <= z, z < n - 1), self.by_line(z + 1, p))
        down = jnp.logical_and(jnp.logical_and(p >= z, z > 0), self.by_line(z - 1, p))
        for h in range(2):
            part = self.piece(p, self.fd, h)
            self.arrive(part, p, 6 + h)
            self.start(up, part, part, p, 10 + h, 6 + h, self.up_dev)
            self.start(down, part, part, p, 12 + h, 6 + h, self.down_dev)

    def drain(self):
        for cond, copy in self.pending:
            if cond is None:
                copy.wait_send()
            else:
                pl.when(cond)(copy.wait_send)


def project_kernel(
    gate_ref,
    value_ref,
    key_ref,
    query_ref,
    pool_ref,
    t_ref,
    gain_ref,
    step_ref,
    out_ref,
    raw_ref,
    buf,
    toks,
    acc,
    send,
    recv,
    pair_sem,
    local_sem,
):
    rows = buf.shape[2]
    half = rows // 2
    mine = t_ref.shape[0]
    length, width = toks.shape
    tile = 256

    def piece(p, f, h):
        return buf.at[p, f, pl.ds(h * half, half)]

    z = lax.axis_index("sp")
    f = lax.axis_index("fs")
    c = lax.axis_index("tp")
    gather = LineGather(lambda h: piece(z, f, h), piece, send, recv)
    parts = []
    for i, ref in enumerate((gate_ref, value_ref, key_ref, query_ref, pool_ref)):
        cols = ref.shape[1]
        start = sum(r.shape[1] for r in (gate_ref, value_ref, key_ref, query_ref, pool_ref)[:i])
        part = pltpu.make_async_copy(
            ref, buf.at[z, f, :, pl.ds(start, cols)], local_sem.at[i]
        )
        part.start()
        parts.append(part)
    own_rows = toks.at[pl.ds(pl.multiple_of(c * mine, mine), mine)]
    own_t = pltpu.make_async_copy(t_ref, own_rows, local_sem.at[5])
    own_t.start()
    partner = (z, f, 1 - c)
    gather.barrier((partner,))
    for part in parts:
        part.wait()
    gather.column(0)
    own_t.wait()
    pair = pltpu.make_async_remote_copy(
        src_ref=t_ref,
        dst_ref=own_rows,
        send_sem=pair_sem.at[0],
        recv_sem=pair_sem.at[1],
        device_id=partner,
        device_id_type=MESH,
    )
    pair.start()
    chunk = 32

    def normalize(start):
        def body(i, carry):
            at = pl.ds(pl.multiple_of(start + i * chunk, chunk), chunk)
            wide = toks[at, :].astype(jnp.float32)
            mean = jnp.mean(wide * wide, axis=-1, keepdims=True)
            toks[at, :] = (wide * lax.rsqrt(mean + EPSILON) * gain_ref[...]).astype(jnp.bfloat16)
            return carry

        lax.fori_loop(0, mine // chunk, body, 0)

    normalize(c * mine)
    pair.wait_recv()
    normalize((1 - c) * mine)

    def multiply(p, member, first=False, last=False):
        at = pl.ds(pl.multiple_of((p * 4 + member) * rows, rows), rows)

        def body(i, carry):
            cols = pl.ds(pl.multiple_of(i * tile, tile), tile)
            for m in range(2):
                lines = pl.ds(m * (length // 2), length // 2)
                part = jnp.dot(
                    toks[lines, at], buf[p, member, :, cols], preferred_element_type=jnp.float32
                )
                if not first:
                    part = part + acc[lines, cols]
                if last:
                    out_ref[lines, cols] = part.astype(jnp.bfloat16)
                else:
                    acc[lines, cols] = part
            return carry

        lax.fori_loop(0, acc.shape[1] // tile, body, 0)

    def step_sizes():
        raw_ref[...] = lax.dot_general(
            step_ref[...], toks[...], (((1,), (1,)), ((), ())), preferred_element_type=jnp.float32
        )

    n = gather.n
    order = gather.order
    for k in range(n + 2):
        if 1 <= k <= n:
            gather.sides(k - 1)
        if 1 <= k < n:
            gather.column(k)
        if 1 <= k <= n:
            multiply(order[k - 1], gather.fx)
        if k < n:
            multiply(order[k], gather.f, first=k == 0)
        if k == 0:
            step_sizes()
        if 1 <= k <= n:
            multiply(order[k - 1], gather.fy)
        if 2 <= k:
            gather.diagonal(k - 2)
            multiply(order[k - 2], gather.fd, last=k == n + 1)
    pair.wait_send()
    gather.drain()


def project(weights, tokens, gain, step_rows):
    n_sp = lax.axis_size("sp")
    rows = weights[0].shape[0]
    cols = sum(w.shape[1] for w in weights)
    length = 2 * tokens.shape[0]
    width = tokens.shape[1]
    anywhere = pl.BlockSpec(memory_space=pl.ANY)
    inside = pl.BlockSpec(memory_space=pltpu.VMEM)
    return pl.pallas_call(
        project_kernel,
        out_shape=(
            jax.ShapeDtypeStruct((length, cols), jnp.bfloat16),
            jax.ShapeDtypeStruct((step_rows.shape[0], length), jnp.float32),
        ),
        in_specs=[anywhere] * 6 + [inside] * 2,
        out_specs=[inside] * 2,
        scratch_shapes=[
            pltpu.VMEM((n_sp, 4, rows, cols), weights[0].dtype),
            pltpu.VMEM((length, width), tokens.dtype),
            pltpu.VMEM((length, cols), jnp.float32),
            pltpu.SemaphoreType.DMA((n_sp, 14)),
            pltpu.SemaphoreType.DMA((n_sp, 8)),
            pltpu.SemaphoreType.DMA((2,)),
            pltpu.SemaphoreType.DMA((6,)),
        ],
        compiler_params=pltpu.CompilerParams(collective_id=0, has_side_effects=True),
        cost_estimate=pl.CostEstimate(
            flops=2 * length * width * cols, bytes_accessed=4 * length * cols, transcendentals=0
        ),
        name="project",
    )(*weights, tokens, gain[None], step_rows)


def output_rows_kernel(w_ref, p_ref, out_ref, send, recv, local_sem):
    rows, cols = w_ref.shape
    z = lax.axis_index("sp")
    f = lax.axis_index("fs")

    def piece(p, member, h):
        at = pl.ds(pl.multiple_of((p * 4 + member) * cols, cols), cols)
        return out_ref.at[pl.ds(h * rows, rows), at]

    gather = LineGather(lambda h: piece(z, f, h), piece, send, recv)
    parts = []
    for h, ref in enumerate((w_ref, p_ref)):
        part = pltpu.make_async_copy(ref, piece(z, f, h), local_sem.at[h])
        part.start()
        parts.append(part)
    gather.barrier()
    for part in parts:
        part.wait()
    for k in range(gather.n + 1):
        if k < gather.n:
            gather.column(k)
        if k >= 1:
            gather.sides(k - 1)
            gather.diagonal(k - 1)
    gather.drain()


def output_rows(w_ssd, w_pool):
    n_sp = lax.axis_size("sp")
    rows, cols = w_ssd.shape
    anywhere = pl.BlockSpec(memory_space=pl.ANY)
    return pl.pallas_call(
        output_rows_kernel,
        out_shape=jax.ShapeDtypeStruct((2 * rows, 4 * n_sp * cols), w_ssd.dtype),
        in_specs=[anywhere] * 2,
        out_specs=pl.BlockSpec(memory_space=pltpu.VMEM),
        scratch_shapes=[
            pltpu.SemaphoreType.DMA((n_sp, 14)),
            pltpu.SemaphoreType.DMA((n_sp, 8)),
            pltpu.SemaphoreType.DMA((2,)),
        ],
        compiler_params=pltpu.CompilerParams(collective_id=1, has_side_effects=True),
        name="output_rows",
    )(w_ssd, w_pool)


def split_heads(first, second, axis, shape):
    places = lax.broadcasted_iota(jnp.int32, shape, axis)
    return jnp.where(places < HEAD_DIM, first, second)


def ends_kernel(blocks, decay_ref, x_ref, k_ref, col_ref, ends_ref, final_ref):
    group = pl.program_id(0)
    tile = (SPAN, 2 * HEAD_DIM)
    for c in range(blocks):
        rows = pl.ds(c * SPAN, SPAN)
        x = x_ref[rows, :].astype(jnp.float32)
        k = k_ref[rows, :]
        for r in range(2):
            weight = split_heads(
                col_ref[0, rows, 4 + 2 * r : 5 + 2 * r],
                col_ref[0, rows, 5 + 2 * r : 6 + 2 * r],
                1,
                tile,
            )
            end = lax.dot_general(
                (x * weight).astype(jnp.bfloat16),
                k,
                (((0,), (0,)), ((), ())),
                preferred_element_type=jnp.float32,
            )
            ends_ref[0, r, c] = end
    states = (2 * HEAD_DIM, STATE)
    for r in range(2):
        total = jnp.zeros(states, jnp.float32)
        for c in range(blocks) if r == 0 else range(blocks - 1, -1, -1):
            at = ((group * blocks + c) * 2 + r) * 2
            scale = split_heads(decay_ref[at], decay_ref[at + 1], 0, states)
            total = total * scale + ends_ref[0, r, c]
        final_ref[0, r] = total


def outputs_kernel(
    blocks, decay_ref, x_ref, k_ref, q_ref, col_ref, row_ref, ends_ref, in_ref, y_ref, prior
):
    group = pl.program_id(0)
    states = (2 * HEAD_DIM, STATE)
    tile = (SPAN, 2 * HEAD_DIM)
    square = (SPAN, SPAN)
    for r in range(2):
        total = in_ref[0, r]
        for c in range(blocks) if r == 0 else range(blocks - 1, -1, -1):
            prior[r, c] = total.astype(jnp.bfloat16)
            at = ((group * blocks + c) * 2 + r) * 2
            scale = split_heads(decay_ref[at], decay_ref[at + 1], 0, states)
            total = total * scale + ends_ref[0, r, c]
    later = lax.broadcasted_iota(jnp.int32, square, 0)
    sooner = lax.broadcasted_iota(jnp.int32, square, 1)
    lower = later >= sooner
    equal = later == sooner
    across = (((1,), (1,)), ((), ()))
    for c in range(blocks):
        rows = pl.ds(c * SPAN, SPAN)
        x = x_ref[rows, :]
        q = q_ref[rows, :]
        scores = lax.dot_general(q, k_ref[rows, :], across, preferred_element_type=jnp.float32)
        parts = []
        for h in range(2):
            cf_l = col_ref[0, rows, 2 * h : 2 * h + 1]
            eb_l = col_ref[0, rows, 2 * h + 1 : 2 * h + 2]
            cf_s = row_ref[0, 4 * h : 4 * h + 1, rows]
            eb_s = row_ref[0, 4 * h + 1 : 4 * h + 2, rows]
            df_s = row_ref[0, 4 * h + 2 : 4 * h + 3, rows]
            db_s = row_ref[0, 4 * h + 3 : 4 * h + 4, rows]
            decay = jnp.exp(jnp.where(lower, cf_l - cf_s, eb_s - eb_l))
            step = jnp.where(equal, df_s + db_s, jnp.where(lower, df_s, db_s))
            parts.append(
                jnp.dot(
                    (scores * decay * step).astype(jnp.bfloat16),
                    x,
                    preferred_element_type=jnp.float32,
                )
            )
        out = split_heads(parts[0], parts[1], 1, tile)
        for r in range(2):
            reach = split_heads(
                col_ref[0, rows, 8 + 2 * r : 9 + 2 * r],
                col_ref[0, rows, 9 + 2 * r : 10 + 2 * r],
                1,
                tile,
            )
            out = out + reach * lax.dot_general(
                q, prior[r, c], across, preferred_element_type=jnp.float32
            )
        y_ref[rows, :] = out


def mixer(activated, width_ssd, width_key, steps, logs, sp_rank):
    length = activated.shape[0]
    heads = steps.shape[1]
    groups = width_key // STATE
    blocks = length // SPAN
    shaped = logs.reshape(2, heads, blocks, SPAN)
    ones = jnp.triu(jnp.ones((SPAN, SPAN), jnp.float32))
    inner = jnp.einsum("rhcs,sl->rhcl", shaped, ones, precision=HIGHEST)
    totals = inner[..., -1:]
    cf = inner[0]
    eb = inner[1] - shaped[1]
    wf = jnp.exp(totals[0] - cf) * steps[0].reshape(cf.shape)
    wb = jnp.exp(eb) * steps[1].reshape(cf.shape)
    reach_f = jnp.exp(cf)
    reach_b = jnp.exp(totals[1] - eb)

    def pair(a):
        return a.reshape(groups, 2, length)

    cf, eb, wf, wb, reach_f, reach_b = map(pair, (cf, eb, wf, wb, reach_f, reach_b))
    df, db = (pair(steps[0]), pair(steps[1]))
    packed = jnp.stack(
        [cf[:, 0], eb[:, 0], cf[:, 1], eb[:, 1]]
        + [wf[:, 0], wf[:, 1], wb[:, 0], wb[:, 1]]
        + [reach_f[:, 0], reach_f[:, 1], reach_b[:, 0], reach_b[:, 1]],
        axis=1,
    )
    cols = jnp.transpose(packed, (0, 2, 1))
    rows = jnp.stack(
        [cf[:, 0], eb[:, 0], df[:, 0], db[:, 0], cf[:, 1], eb[:, 1], df[:, 1], db[:, 1]], axis=1
    )
    block_logs = totals[..., 0]
    decays = jnp.exp(block_logs).reshape(2, groups, 2, blocks)
    decays = jnp.transpose(decays, (1, 3, 0, 2)).reshape(-1)
    smem = pl.BlockSpec(memory_space=pltpu.SMEM)
    x_blocks = width_ssd // STATE

    def wide(offset):
        return pl.BlockSpec((length, STATE), lambda g: (0, g + offset))

    col_spec = pl.BlockSpec((1, length, cols.shape[2]), lambda g: (g, 0, 0))
    ends_spec = pl.BlockSpec((1, 2, blocks, STATE, STATE), lambda g: (g, 0, 0, 0, 0))
    state_spec = pl.BlockSpec((1, 2, STATE, STATE), lambda g: (g, 0, 0, 0))
    ends, finals = pl.pallas_call(
        functools.partial(ends_kernel, blocks),
        grid=(groups,),
        out_shape=(
            jax.ShapeDtypeStruct((groups, 2, blocks, STATE, STATE), jnp.float32),
            jax.ShapeDtypeStruct((groups, 2, STATE, STATE), jnp.float32),
        ),
        in_specs=[smem, wide(0), wide(x_blocks), col_spec],
        out_specs=(ends_spec, state_spec),
        cost_estimate=pl.CostEstimate(
            flops=4 * length * groups * STATE * STATE,
            bytes_accessed=16 * length * groups * STATE,
            transcendentals=0,
        ),
        name="block_ends",
    )(decays, activated, activated, cols)
    device_totals = jnp.sum(block_logs, axis=-1)
    all_totals = lax.all_gather(
        device_totals[None].astype(jnp.bfloat16), "sp", axis=0, tiled=True
    ).astype(jnp.float32)
    states = jnp.transpose(finals, (1, 0, 2, 3)).reshape(2, heads, HEAD_DIM, STATE)
    forward_in, backward_in = prefix_states(all_totals, states.astype(jnp.bfloat16), sp_rank)
    incoming = jnp.stack([forward_in, backward_in]).reshape(2, groups, STATE, STATE)
    incoming = jnp.transpose(incoming, (1, 0, 2, 3))
    return pl.pallas_call(
        functools.partial(outputs_kernel, blocks),
        grid=(groups,),
        out_shape=jax.ShapeDtypeStruct((length, groups * STATE), jnp.float32),
        in_specs=[
            smem,
            wide(0),
            wide(x_blocks),
            wide(x_blocks + groups),
            col_spec,
            pl.BlockSpec((1, 8, length), lambda g: (g, 0, 0)),
            ends_spec,
            state_spec,
        ],
        out_specs=wide(0),
        scratch_shapes=[pltpu.VMEM((2, blocks, STATE, STATE), jnp.bfloat16)],
        cost_estimate=pl.CostEstimate(
            flops=10 * length * groups * STATE * STATE,
            bytes_accessed=40 * length * groups * STATE,
            transcendentals=2 * length * groups * SPAN,
        ),
        name="block_outputs",
    )(decays, activated, activated, activated, cols, rows, ends, incoming)


def prefix_states(all_totals, finals, rank):
    chain_length = all_totals.shape[0]
    device_ids = jnp.arange(chain_length, dtype=jnp.int32)[:, None]
    forward_cum = jnp.cumsum(all_totals[:, 0], axis=0)
    forward_mine = lax.dynamic_slice_in_dim(forward_cum - all_totals[:, 0], rank, 1, 0)
    forward_weight = jnp.exp(jnp.where(device_ids < rank, forward_mine - forward_cum, -jnp.inf))
    backward_cum = jnp.cumsum(all_totals[:, 1], axis=0)
    backward_mine = lax.dynamic_slice_in_dim(backward_cum, rank, 1, 0)
    backward_weight = jnp.exp(
        jnp.where(device_ids > rank, backward_cum - all_totals[:, 1] - backward_mine, -jnp.inf)
    )
    forward_in = jnp.zeros(finals.shape[1:], jnp.float32)
    backward_in = jnp.zeros(finals.shape[1:], jnp.float32)
    for d in range(1, chain_length):
        ahead = [(i, i + d) for i in range(chain_length - d)]
        back = [(i + d, i) for i in range(chain_length - d)]
        from_left = lax.ppermute(finals[0], "sp", ahead).astype(jnp.float32)
        from_right = lax.ppermute(finals[1], "sp", back).astype(jnp.float32)
        left = lax.dynamic_index_in_dim(forward_weight, jnp.maximum(rank - d, 0), 0, False)
        right = lax.dynamic_index_in_dim(
            backward_weight, jnp.minimum(rank + d, chain_length - 1), 0, False
        )
        forward_in = forward_in + left[:, None, None] * from_left
        backward_in = backward_in + right[:, None, None] * from_right
    return (forward_in, backward_in)


def local(
    tokens,
    norm_gain,
    w_gate,
    w_value,
    w_bkey,
    w_query,
    w_pool_in,
    w_step,
    step_bias,
    decay_rate,
    decay_shift,
    conv_value,
    conv_bkey,
    conv_query,
    mix_gain,
    pool_mix,
    pool_gain,
    w_out_ssd,
    w_out_pool,
):
    tp_count = lax.axis_size("tp")
    sp_count = lax.axis_size("sp")
    tp_rank = lax.axis_index("tp")
    sp_rank = lax.axis_index("sp")
    heads_dev = DUALITY_HEADS // tp_count
    groups_dev = GROUPS // tp_count
    pools_dev = POOL_GROUPS // tp_count
    width_ssd = heads_dev * HEAD_DIM
    width_key = groups_dev * STATE
    width_pool = pools_dev * POOL_DIM
    fast = (
        tp_count == 2
        and lax.axis_size("fs") == 4
        and 2 <= sp_count <= 4
        and w_gate.shape[0] % 128 == 0
        and w_out_ssd.shape[1] % 128 == 0
    )
    step_cols = lax.dynamic_slice_in_dim(w_step, tp_rank * heads_dev, heads_dev, 2)
    step_cols = step_cols.reshape(w_step.shape[0], 2 * heads_dev)
    if fast:
        stored, raw_steps = project(
            (w_gate, w_value, w_bkey, w_query, w_pool_in),
            tokens[0],
            norm_gain,
            jnp.transpose(step_cols),
        )
        raw_steps = jnp.transpose(raw_steps)
        out_rows = output_rows(w_out_ssd, w_out_pool)
    else:
        weights = jnp.concatenate([w_gate, w_value, w_bkey, w_query, w_pool_in], axis=1)
        combined, widened = gather_inputs(weights, tokens[0])
        out_rows = lax.all_gather(
            jnp.concatenate([w_out_ssd, w_out_pool], axis=0), ("sp", "fs"), axis=1, tiled=True
        )
        widened = widened.astype(jnp.float32)
        scaling = lax.rsqrt(jnp.mean(widened * widened, axis=-1, keepdims=True) + EPSILON)
        normed = (widened * scaling * norm_gain).astype(jnp.bfloat16)
        stored = jnp.dot(normed, combined, preferred_element_type=jnp.float32).astype(jnp.bfloat16)
        raw_steps = jnp.dot(normed, step_cols, preferred_element_type=jnp.float32)
    length = stored.shape[0]
    padded = padded_2(stored[:, width_ssd:], (("sp", 0),), REACH)
    conv_cols = width_ssd + 2 * width_key
    taps = jnp.concatenate(
        [
            lax.dynamic_slice_in_dim(conv_value, tp_rank * width_ssd, width_ssd, 1),
            lax.dynamic_slice_in_dim(conv_bkey, tp_rank * width_key, width_key, 1),
            lax.dynamic_slice_in_dim(conv_query, tp_rank * width_key, width_key, 1),
        ],
        axis=1,
    ).astype(jnp.float32)
    margin = CONV_WIDTH // 2
    convolved = jnp.zeros((length, conv_cols), jnp.float32)
    for offset in range(CONV_WIDTH):
        begin = REACH - margin + offset
        convolved = (
            convolved
            + padded[begin : begin + length, :conv_cols].astype(jnp.float32) * taps[offset]
        )
    activated = jax.nn.silu(convolved).astype(jnp.bfloat16)
    bias_dev = lax.dynamic_slice_in_dim(step_bias, tp_rank * heads_dev, heads_dev, 1)
    rate_dev = lax.dynamic_slice_in_dim(decay_rate, tp_rank * heads_dev, heads_dev, 1)
    steps = jax.nn.softplus(raw_steps.reshape(length, 2, heads_dev) + bias_dev).transpose(1, 2, 0)
    logs = -rate_dev[:, :, None] * steps - decay_shift[0].transpose(1, 0, 2)
    heads_out = mixer(activated, width_ssd, width_key, steps, logs, sp_rank)
    gated = heads_out * jax.nn.silu(stored[:, :width_ssd].astype(jnp.float32))
    squares = lax.psum(jnp.sum(gated * gated, axis=-1), "tp")
    gain_dev = lax.dynamic_slice_in_dim(mix_gain, tp_rank * width_ssd, width_ssd, 0)
    ssd_mix = (gated * lax.rsqrt(squares / D_SSM + EPSILON)[:, None] * gain_dev).astype(
        jnp.bfloat16
    )
    pool_rows = padded[:, conv_cols:].astype(jnp.float32)
    own_rows = pool_rows[REACH : REACH + length]
    where_global = sp_rank * length + jnp.arange(length, dtype=jnp.int32)
    seq_length = length * sp_count
    window_means = []
    for window in WINDOWS:
        running = jnp.zeros((length, width_pool), jnp.float32)
        for offset in range(-(window // 2), window - window // 2):
            running = running + pool_rows[REACH + offset : REACH + offset + length]
        lower = jnp.clip(where_global - window // 2, 0, seq_length)
        upper = jnp.clip(where_global + window - window // 2, 0, seq_length)
        window_means.append(running / (upper - lower).astype(jnp.float32)[:, None])
    stacked = jnp.stack(window_means).reshape(4, length, pools_dev, POOL_DIM)
    group_ids = tp_rank * pools_dev + jnp.arange(pools_dev, dtype=jnp.int32)
    selector = (jnp.arange(4, dtype=jnp.int32)[:, None] == (group_ids % 4)[None, :]).astype(
        jnp.float32
    )
    means = jnp.sum(stacked * selector[:, None, :, None], axis=0)
    differences = (means - own_rows.reshape(length, pools_dev, POOL_DIM)).astype(jnp.bfloat16)
    pool_weights = lax.dynamic_slice_in_dim(pool_mix, tp_rank * pools_dev, pools_dev, 0)
    mapped = jnp.einsum(
        "rgc,gcd->rgd", differences, pool_weights, preferred_element_type=jnp.float32
    )
    pool_gain_dev = lax.dynamic_slice_in_dim(pool_gain, tp_rank * width_pool, width_pool, 0)
    pool_out = (mapped.reshape(length, width_pool) * pool_gain_dev).astype(jnp.bfloat16)
    mixed = jnp.concatenate([ssd_mix, pool_out], axis=1)
    if tp_count == 2:
        part = length // 2
        away = lax.dynamic_slice_in_dim(mixed, (1 - tp_rank) * part, part, 0)
        home = lax.dynamic_slice_in_dim(mixed, tp_rank * part, part, 0)
        sent = jnp.dot(away, out_rows, preferred_element_type=jnp.float32).astype(jnp.bfloat16)
        received = lax.ppermute(sent, "tp", [(0, 1), (1, 0)])
        kept = lax.optimization_barrier(
            jnp.dot(home, out_rows, preferred_element_type=jnp.float32).astype(jnp.bfloat16)
        )
        summed = (kept.astype(jnp.float32) + received.astype(jnp.float32)).astype(jnp.bfloat16)
    else:
        summed = lax.psum_scatter(
            jnp.dot(mixed, out_rows, preferred_element_type=jnp.float32).astype(jnp.bfloat16),
            "tp",
            scatter_dimension=0,
            tiled=True,
        )
    return summed[None]


def solution(mesh):
    return jax.shard_map(
        local,
        mesh=mesh,
        in_specs=(
            P("fs", ("sp", "tp"), None),
            P(),
            P(("sp", "fs"), "tp"),
            P(("sp", "fs"), "tp"),
            P(("sp", "fs"), "tp"),
            P(("sp", "fs"), "tp"),
            P(("sp", "fs"), "tp"),
            P(),
            P(),
            P(),
            P("fs", "tp", None, "sp"),
            P(),
            P(),
            P(),
            P(),
            P(),
            P(),
            P("tp", ("sp", "fs")),
            P("tp", ("sp", "fs")),
        ),
        out_specs=P("fs", ("sp", "tp"), None),
        check_vma=False,
    )
```

```python
import functools

import jax
import jax.numpy as jnp
from jax import lax
from jax.experimental import pallas as pl
from jax.experimental.pallas import tpu as pltpu
from jax.sharding import PartitionSpec as P

HEAD_DIM = 64
DUALITY_HEADS = 16
GROUPS = 8
STATE = 128
CONV_WIDTH = 5
POOL_GROUPS = 8
POOL_DIM = 128
SPAN = 128
REACH = 8
D_SSM = 1024


EPSILON = 1e-06
HIGHEST = lax.Precision.HIGHEST
WINDOWS = (2, 4, 8, 16)


def padded_2(cells, sides, width):
    for axis, dim in sides:
        count = lax.axis_size(axis)
        ends = count - 1
        head = lax.slice_in_dim(cells, 0, width, axis=dim)
        tail = lax.slice_in_dim(cells, cells.shape[dim] - width, cells.shape[dim], axis=dim)
        cells = jnp.concatenate(
            [
                lax.ppermute(tail, axis, [(i, (i + 1) % count) for i in range(ends)]),
                cells,
                lax.ppermute(head, axis, [((i + 1) % count, i) for i in range(ends)]),
            ],
            axis=dim,
        )
    return cells


MESH = pl.DeviceIdType.MESH


def gather_kernel(n_sp, n_tp, w_ref, t_ref, w_out, t_out, send, recv, local_sem):
    z = lax.axis_index("sp")
    f = lax.axis_index("fs")
    c = lax.axis_index("tp")
    fx = f + 1 - 2 * lax.rem(f, 2)
    fy = lax.rem(f + 2, 4)
    rows = w_ref.shape[0]
    half = rows // 2
    x_dev = (z, fx, c)
    y_dev = (z, fy, c)
    z_devs = [(lax.rem(z + d, n_sp), f, c) for d in range(1, n_sp)]
    t_devs = [(z, f, lax.rem(c + d, n_tp)) for d in range(1, n_tp)]
    partners = [x_dev, y_dev] + z_devs + t_devs
    barrier = pltpu.get_barrier_semaphore()
    for dev in partners:
        pl.semaphore_signal(barrier, inc=1, device_id=dev, device_id_type=MESH)
    pl.semaphore_wait(barrier, len(partners))

    def remote(src, dst, index, dev):
        copy = pltpu.make_async_remote_copy(
            src_ref=src,
            dst_ref=dst,
            send_sem=send.at[index],
            recv_sem=recv.at[index],
            device_id=dev,
            device_id_type=MESH,
        )
        copy.start()
        return copy

    base = n_sp - 1
    z_copies = [remote(w_ref, w_out.at[z, f], d, z_devs[d]) for d in range(n_sp - 1)]
    full = []
    relay = []

    def send_full(d):
        if d == 0:
            src = w_ref
            origin = z
        else:
            z_copies[d - 1].wait_recv()
            origin = lax.rem(z - d + n_sp, n_sp)
            src = w_out.at[origin, f]
        dst = w_out.at[origin, f]
        full.append(
            (
                remote(src, dst, base + 4 * d, x_dev),
                remote(src, dst, base + 4 * d + 1, y_dev),
            )
        )

    def send_relay(d):
        origin = lax.rem(z - d + n_sp, n_sp)
        full[d][0].wait_recv()
        part = w_out.at[origin, fx, pl.ds(0, half)]
        first = remote(part, part, base + 4 * d + 2, y_dev)
        full[d][1].wait_recv()
        part = w_out.at[origin, fy, pl.ds(half, half)]
        relay.append((first, remote(part, part, base + 4 * d + 3, x_dev)))

    send_full(0)
    own_w = pltpu.make_async_copy(w_ref, w_out.at[z, f], local_sem.at[0])
    own_w.start()
    own_t = pltpu.make_async_copy(t_ref, t_out.at[c], local_sem.at[1])
    own_t.start()
    tbase = base + 4 * n_sp
    t_copies = [remote(t_ref, t_out.at[c], tbase + d, t_devs[d]) for d in range(n_tp - 1)]
    for d in range(1, n_sp):
        send_full(d)
        send_relay(d - 1)
    send_relay(n_sp - 1)
    for pair in relay:
        for copy in pair:
            copy.wait_recv()
    for copy in t_copies:
        copy.wait_recv()
    for copy in z_copies + t_copies:
        copy.wait_send()
    for pair in full + relay:
        for copy in pair:
            copy.wait_send()
    own_w.wait()
    own_t.wait()


def gather_inputs(weights, tokens):
    n_sp = lax.axis_size("sp")
    n_fs = lax.axis_size("fs")
    n_tp = lax.axis_size("tp")
    rows, cols = weights.shape
    if n_fs != 4:
        return (
            lax.all_gather(weights, ("sp", "fs"), axis=0, tiled=True),
            lax.all_gather(tokens, "tp", axis=0, tiled=True),
        )
    count = (n_sp - 1) + 4 * n_sp + (n_tp - 1)
    wide, toks = pl.pallas_call(
        functools.partial(gather_kernel, n_sp, n_tp),
        out_shape=(
            jax.ShapeDtypeStruct((n_sp, n_fs, rows, cols), weights.dtype),
            jax.ShapeDtypeStruct((n_tp,) + tokens.shape, tokens.dtype),
        ),
        in_specs=[pl.BlockSpec(memory_space=pltpu.VMEM)] * 2,
        out_specs=[pl.BlockSpec(memory_space=pl.ANY)] * 2,
        scratch_shapes=[
            pltpu.SemaphoreType.DMA((count,)),
            pltpu.SemaphoreType.DMA((count,)),
            pltpu.SemaphoreType.DMA((2,)),
        ],
        compiler_params=pltpu.CompilerParams(collective_id=0, has_side_effects=True),
        cost_estimate=pl.CostEstimate(
            flops=0, bytes_accessed=200 * n_sp * n_fs * rows * cols, transcendentals=0
        ),
        name="gather_inputs",
    )(weights, tokens)
    return wide.reshape(n_sp * n_fs * rows, cols), toks.reshape(-1, tokens.shape[1])


class LineGather:
    def __init__(self, own, piece, send, recv):
        self.n = lax.axis_size("sp")
        self.z = lax.axis_index("sp")
        self.f = lax.axis_index("fs")
        self.c = lax.axis_index("tp")
        self.fx = self.f + 1 - 2 * lax.rem(self.f, 2)
        self.fy = lax.rem(self.f + 2, 4)
        self.fd = 3 - self.f
        self.own, self.piece, self.send, self.recv = own, piece, send, recv
        self.x_dev = (self.z, self.fx, self.c)
        self.y_dev = (self.z, self.fy, self.c)
        self.up_dev = (lax.rem(self.z + 1, self.n), self.f, self.c)
        self.down_dev = (lax.rem(self.z + self.n - 1, self.n), self.f, self.c)
        self.order = [self.nearest(k) for k in range(self.n)]
        self.pending = []

    def barrier(self, extra=()):
        barrier = pltpu.get_barrier_semaphore()
        devices = [self.x_dev, self.y_dev, self.up_dev, self.down_dev, *extra]
        for device in devices:
            pl.semaphore_signal(barrier, inc=1, device_id=device, device_id_type=MESH)
        pl.semaphore_wait(barrier, len(devices))

    def nearest(self, k):
        z, n = self.z, self.n
        low = jnp.minimum(z, n - 1 - z)
        sign = 1 if k % 2 == 0 else -1
        paired = z + sign * ((k + 1) // 2)
        past = jnp.where(2 * z < n - 1, z + (k - low), z - (k - low))
        return jnp.where(k <= 2 * low, paired, past)

    def by_line(self, z, p):
        near = jnp.logical_or(p == z + 1, p == z - 1)
        if self.n >= 4:
            near = jnp.logical_or(near, jnp.logical_and(z == 0, p == 2))
            near = jnp.logical_or(near, jnp.logical_and(z == self.n - 1, p == self.n - 3))
        return near

    def copy(self, src, dst, p, s, r, device):
        return pltpu.make_async_remote_copy(
            src_ref=src,
            dst_ref=dst,
            send_sem=self.send.at[p, s],
            recv_sem=self.recv.at[p, r],
            device_id=device,
            device_id_type=MESH,
        )

    def start(self, cond, src, dst, p, s, r, device):
        copy = self.copy(src, dst, p, s, r, device)
        if cond is None:
            copy.start()
        else:
            pl.when(cond)(copy.start)
        self.pending.append((cond, copy))

    def arrive(self, ref, p, r):
        self.copy(ref, ref, p, 0, r, self.x_dev).wait_recv()

    def column(self, k):
        p = self.order[k]
        up = jnp.logical_and(p <= self.z, self.z < self.n - 1)
        down = jnp.logical_and(p >= self.z, self.z > 0)
        for h in range(2):
            ref = self.piece(p, self.f, h)
            src = ref
            if k == 0:
                src = self.own(h)
            else:
                self.arrive(ref, p, h)
            self.start(None, src, ref, p, 4 + h, 2 + h, self.x_dev)
            self.start(None, src, ref, p, 6 + h, 4 + h, self.y_dev)
            self.start(up, src, ref, p, h, h, self.up_dev)
            self.start(down, src, ref, p, 2 + h, h, self.down_dev)

    def sides(self, k):
        p = self.order[k]
        relay = jnp.logical_not(self.by_line(self.z, p))
        for h in range(2):
            x_part = self.piece(p, self.fx, h)
            y_part = self.piece(p, self.fy, h)
            self.arrive(x_part, p, 2 + h)
            if h == 0:
                self.start(relay, x_part, x_part, p, 8, 6, self.y_dev)
            self.arrive(y_part, p, 4 + h)
            if h == 1:
                self.start(relay, y_part, y_part, p, 9, 7, self.x_dev)

    def diagonal(self, k):
        p = self.order[k]
        z, n = self.z, self.n
        up = jnp.logical_and(jnp.logical_and(p <= z, z < n - 1), self.by_line(z + 1, p))
        down = jnp.logical_and(jnp.logical_and(p >= z, z > 0), self.by_line(z - 1, p))
        for h in range(2):
            part = self.piece(p, self.fd, h)
            self.arrive(part, p, 6 + h)
            self.start(up, part, part, p, 10 + h, 6 + h, self.up_dev)
            self.start(down, part, part, p, 12 + h, 6 + h, self.down_dev)

    def drain(self):
        for cond, copy in self.pending:
            if cond is None:
                copy.wait_send()
            else:
                pl.when(cond)(copy.wait_send)


def project_kernel(
    gate_ref,
    value_ref,
    key_ref,
    query_ref,
    pool_ref,
    t_ref,
    gain_ref,
    step_ref,
    scale_ref,
    shift_ref,
    out_ref,
    rows_ref,
    cols_ref,
    total_ref,
    buf,
    toks,
    acc,
    send,
    recv,
    pair_sem,
    local_sem,
):
    rows = buf.shape[2]
    half = rows // 2
    mine = t_ref.shape[0]
    length, width = toks.shape
    tile = 256

    def piece(p, f, h):
        return buf.at[p, f, pl.ds(h * half, half)]

    z = lax.axis_index("sp")
    f = lax.axis_index("fs")
    c = lax.axis_index("tp")
    gather = LineGather(lambda h: piece(z, f, h), piece, send, recv)
    parts = []
    for i, ref in enumerate((gate_ref, value_ref, key_ref, query_ref, pool_ref)):
        cols = ref.shape[1]
        start = sum(r.shape[1] for r in (gate_ref, value_ref, key_ref, query_ref, pool_ref)[:i])
        part = pltpu.make_async_copy(
            ref, buf.at[z, f, :, pl.ds(start, cols)], local_sem.at[i]
        )
        part.start()
        parts.append(part)
    own_rows = toks.at[pl.ds(pl.multiple_of(c * mine, mine), mine)]
    own_t = pltpu.make_async_copy(t_ref, own_rows, local_sem.at[5])
    own_t.start()
    partner = (z, f, 1 - c)
    gather.barrier((partner,))
    for part in parts:
        part.wait()
    gather.column(0)
    own_t.wait()
    pair = pltpu.make_async_remote_copy(
        src_ref=t_ref,
        dst_ref=own_rows,
        send_sem=pair_sem.at[0],
        recv_sem=pair_sem.at[1],
        device_id=partner,
        device_id_type=MESH,
    )
    pair.start()
    chunk = 32

    def normalize(start):
        def body(i, carry):
            at = pl.ds(pl.multiple_of(start + i * chunk, chunk), chunk)
            wide = toks[at, :].astype(jnp.float32)
            mean = jnp.mean(wide * wide, axis=-1, keepdims=True)
            toks[at, :] = (wide * lax.rsqrt(mean + EPSILON) * gain_ref[...]).astype(jnp.bfloat16)
            return carry

        lax.fori_loop(0, mine // chunk, body, 0)

    normalize(c * mine)
    pair.wait_recv()
    normalize((1 - c) * mine)

    def multiply(p, member, first=False, last=False):
        at = pl.ds(pl.multiple_of((p * 4 + member) * rows, rows), rows)

        def body(i, carry):
            cols = pl.ds(pl.multiple_of(i * tile, tile), tile)
            for m in range(2):
                lines = pl.ds(m * (length // 2), length // 2)
                part = jnp.dot(
                    toks[lines, at], buf[p, member, :, cols], preferred_element_type=jnp.float32
                )
                if not first:
                    part = part + acc[lines, cols]
                if last:
                    out_ref[lines, cols] = part.astype(jnp.bfloat16)
                else:
                    acc[lines, cols] = part
            return carry

        lax.fori_loop(0, acc.shape[1] // tile, body, 0)

    def step_sizes():
        raw = lax.dot_general(
            step_ref[...], toks[...], (((1,), (1,)), ((), ())), preferred_element_type=jnp.float32
        )
        raw = raw + scale_ref[:, :1]
        steps = jnp.maximum(raw, 0.0) + jnp.log1p(jnp.exp(-jnp.abs(raw)))
        logs = -scale_ref[:, SPAN : SPAN + 1] * steps - shift_ref[...]
        lines = raw.shape[0]
        blocks = length // SPAN
        cut = [slice(i * SPAN, (i + 1) * SPAN) for i in range(blocks)]
        steps = jnp.concatenate([steps[:, at] for at in cut], axis=0)
        logs = jnp.concatenate([logs[:, at] for at in cut], axis=0)
        square = (SPAN, SPAN)
        upper = lax.broadcasted_iota(jnp.int32, square, 0) <= lax.broadcasted_iota(
            jnp.int32, square, 1
        )
        inner = jnp.dot(
            logs, upper.astype(jnp.float32), precision=HIGHEST, preferred_element_type=jnp.float32
        )
        total = inner[:, SPAN - 1 :]
        backward = lax.rem(lax.broadcasted_iota(jnp.int32, logs.shape, 0), 2) == 1
        along = inner - jnp.where(backward, logs, 0.0)
        weight = jnp.exp(jnp.where(backward, along, total - along)) * steps
        reach = jnp.exp(jnp.where(backward, total - along, along))
        rows_ref[0] = along
        rows_ref[1] = steps
        rows_ref[2] = jnp.broadcast_to(jnp.exp(total), logs.shape)
        whole = total[:lines]
        for i in range(1, blocks):
            whole = whole + total[i * lines : (i + 1) * lines]
        total_ref[...] = jnp.broadcast_to(whole, total_ref.shape)
        turned = [jnp.transpose(v) for v in (along, weight, reach)]
        for g in range(lines // 4):
            for i in range(blocks):
                for j in range(3):
                    at = i * lines + 4 * g
                    cols_ref[g, cut[i], 4 * j : 4 * j + 4] = turned[j][:, at : at + 4]

    n = gather.n
    order = gather.order
    for k in range(n + 2):
        if 1 <= k <= n:
            gather.sides(k - 1)
        if 1 <= k < n:
            gather.column(k)
        if 1 <= k <= n:
            multiply(order[k - 1], gather.fx)
        if k < n:
            multiply(order[k], gather.f, first=k == 0)
        if k == 0:
            step_sizes()
        if 1 <= k <= n:
            multiply(order[k - 1], gather.fy)
        if 2 <= k:
            gather.diagonal(k - 2)
            multiply(order[k - 2], gather.fd, last=k == n + 1)
    pair.wait_send()
    gather.drain()


def project(weights, tokens, gain, step_rows, scales, shift):
    n_sp = lax.axis_size("sp")
    rows = weights[0].shape[0]
    cols = sum(w.shape[1] for w in weights)
    length = 2 * tokens.shape[0]
    width = tokens.shape[1]
    lines = step_rows.shape[0]
    anywhere = pl.BlockSpec(memory_space=pl.ANY)
    inside = pl.BlockSpec(memory_space=pltpu.VMEM)
    return pl.pallas_call(
        project_kernel,
        out_shape=(
            jax.ShapeDtypeStruct((length, cols), jnp.bfloat16),
            jax.ShapeDtypeStruct((3, lines * length // SPAN, SPAN), jnp.float32),
            jax.ShapeDtypeStruct((lines // 4, length, 12), jnp.float32),
            jax.ShapeDtypeStruct((lines, SPAN), jnp.float32),
        ),
        in_specs=[anywhere] * 6 + [inside] * 4,
        out_specs=[inside] * 4,
        scratch_shapes=[
            pltpu.VMEM((n_sp, 4, rows, cols), weights[0].dtype),
            pltpu.VMEM((length, width), tokens.dtype),
            pltpu.VMEM((length, cols), jnp.float32),
            pltpu.SemaphoreType.DMA((n_sp, 14)),
            pltpu.SemaphoreType.DMA((n_sp, 8)),
            pltpu.SemaphoreType.DMA((2,)),
            pltpu.SemaphoreType.DMA((6,)),
        ],
        compiler_params=pltpu.CompilerParams(collective_id=0, has_side_effects=True),
        cost_estimate=pl.CostEstimate(
            flops=2 * length * width * cols, bytes_accessed=4 * length * cols, transcendentals=0
        ),
        name="project",
    )(*weights, tokens, gain[None], step_rows, scales, shift)


def mixer_kernel(
    stored_ref,
    rows_ref,
    cols_ref,
    total_ref,
    conv_value_ref,
    conv_key_ref,
    conv_query_ref,
    gain_ref,
    pool_mix_ref,
    pool_gain_ref,
    w_ssd_ref,
    w_pool_ref,
    out_ref,
    w_out,
    taps,
    pad,
    act,
    y,
    ends,
    prior,
    finals,
    arrived,
    incoming,
    totals,
    squares,
    mixed,
    away,
    got,
    halo,
    w_send,
    w_recv,
    w_local,
    halo_sem,
    total_sem,
    state_sem,
    square_sem,
    part_sem,
):
    length = stored_ref.shape[0]
    rows, cols = w_ssd_ref.shape
    groups = cols_ref.shape[0]
    lines = total_ref.shape[0]
    blocks = length // SPAN
    width = groups * STATE
    half = length // 2
    edge = halo.shape[1]
    z = lax.axis_index("sp")
    f = lax.axis_index("fs")
    c = lax.axis_index("tp")
    n = lax.axis_size("sp")
    tile = (SPAN, 2 * HEAD_DIM)
    square = (SPAN, SPAN)
    f32 = jnp.float32
    across = (((1,), (1,)), ((), ()))

    def piece(p, member, h):
        at = pl.ds(pl.multiple_of((p * 4 + member) * cols, cols), cols)
        return w_out.at[pl.ds(h * rows, rows), at]

    gather = LineGather(lambda h: piece(z, f, h), piece, w_send, w_recv)
    own = []
    for h, ref in enumerate((w_ssd_ref, w_pool_ref)):
        copy = pltpu.make_async_copy(ref, piece(z, f, h), w_local.at[h])
        copy.start()
        own.append(copy)
    partner = (z, f, 1 - c)
    ahead = [(lax.rem(z + d, n), f, c) for d in range(n)]
    behind = [(lax.rem(z + n - d, n), f, c) for d in range(n)]
    gather.barrier((partner, *ahead[2 : n - 1]))
    pending = []

    def remote(src, dst, sems, index, device, cond=None):
        copy = pltpu.make_async_remote_copy(
            src_ref=src,
            dst_ref=dst,
            send_sem=sems.at[(0, *index)],
            recv_sem=sems.at[(1, *index)],
            device_id=device,
            device_id_type=MESH,
        )
        if cond is None:
            copy.start()
        else:
            pl.when(cond)(copy.start)
        pending.append((cond, copy))
        return copy

    below, above = z > 0, z < n - 1
    sides = pl.ds(width, pad.shape[1])
    from_below = remote(
        stored_ref.at[pl.ds(length - edge, edge), sides], halo.at[0], halo_sem, (0,), ahead[1], above
    )
    from_above = remote(
        stored_ref.at[pl.ds(0, edge), sides], halo.at[1], halo_sem, (1,), behind[1], below
    )
    sums = [
        remote(total_ref, totals.at[z], total_sem, (d - 1,), ahead[d]) for d in range(1, n)
    ]
    for copy in own:
        copy.wait()
    gather.column(0)

    def lanes(i, count=1):
        return pl.ds(pl.multiple_of(i * STATE, STATE), count * STATE)

    def span(i):
        return pl.ds(pl.multiple_of(i * SPAN, SPAN), SPAN)

    for i, ref in enumerate((conv_value_ref, conv_key_ref, conv_query_ref)):
        taps[:CONV_WIDTH, i * width : (i + 1) * width] = ref[
            :, pl.ds(pl.multiple_of(c * width, width), width)
        ].astype(f32)

    def widen(i, carry):
        at = pl.ds(pl.multiple_of(REACH + i * SPAN, REACH), SPAN)
        pad[at, :] = stored_ref[span(i), sides].astype(f32)
        return carry

    lax.fori_loop(0, blocks, widen, 0)

    @pl.when(below)
    def _():
        from_below.wait_recv()
        pad[:REACH, :] = halo[0].astype(f32)[edge - REACH :]

    @pl.when(jnp.logical_not(below))
    def _():
        pad[:REACH, :] = jnp.zeros((REACH, pad.shape[1]), f32)

    @pl.when(above)
    def _():
        from_above.wait_recv()
        pad[REACH + length :, :] = halo[1].astype(f32)[:REACH]

    @pl.when(jnp.logical_not(above))
    def _():
        pad[REACH + length :, :] = jnp.zeros((REACH, pad.shape[1]), f32)

    margin = CONV_WIDTH // 2

    def convolve(i, carry):
        at = lanes(i)
        tap = taps[:, at]
        for b in range(blocks):
            begin = REACH - margin + b * SPAN
            total = pad[begin : begin + SPAN, at] * tap[:1]
            for o in range(1, CONV_WIDTH):
                total = total + pad[begin + o : begin + o + SPAN, at] * tap[o : o + 1]
            act[b * SPAN : (b + 1) * SPAN, at] = jax.nn.silu(total).astype(jnp.bfloat16)
        return carry

    lax.fori_loop(0, 2 * groups, convolve, 0)
    gather.sides(0)
    gather.column(1)
    lax.fori_loop(2 * groups, 3 * groups, convolve, 0)
    step = 4 if blocks % 4 == 0 else 1
    parts = blocks // step

    def block_ends(i, carry):
        g = i // parts
        for u in range(step):
            b = lax.rem(i, parts) * step + u
            at = span(b)
            x = act[at, lanes(g)].astype(f32)
            k = act[at, lanes(groups + g)]
            for r in range(2):
                weight = split_heads(
                    cols_ref[g, at, 4 + r : 5 + r], cols_ref[g, at, 6 + r : 7 + r], 1, tile
                )
                ends[g, r, b] = lax.dot_general(
                    (x * weight).astype(jnp.bfloat16),
                    k,
                    (((0,), (0,)), ((), ())),
                    preferred_element_type=f32,
                )
        return carry

    lax.fori_loop(0, groups * parts, block_ends, 0)

    def scan(g, r, start, each):
        order = range(blocks) if r == 0 else range(blocks - 1, -1, -1)
        carried = list(start)
        for b in order:
            each(b, carried)
            for h in range(2):
                at = b * lines + 4 * g + 2 * h + r
                scale = rows_ref[2, pl.ds(at, 1), :]
                carried[h] = carried[h] * scale + ends[g, r, b, h * HEAD_DIM : (h + 1) * HEAD_DIM]
        return carried

    def own_states(g, carry):
        zero = jnp.zeros((HEAD_DIM, STATE), f32)
        for r in range(2):
            last = scan(g, r, [zero, zero], lambda b, carried: None)
            for h in range(2):
                finals[r, g, h * HEAD_DIM : (h + 1) * HEAD_DIM] = last[h].astype(jnp.bfloat16)
        return carry

    lax.fori_loop(0, groups, own_states, 0)
    gather.sides(1)
    states = []
    for d in range(1, n):
        states.append(
            (
                remote(finals.at[0], arrived.at[0, d - 1], state_sem, (0, d - 1), ahead[d], z + d < n),
                remote(finals.at[1], arrived.at[1, d - 1], state_sem, (1, d - 1), behind[d], z >= d),
            )
        )
    if n > 2:
        gather.column(2)
    gather.diagonal(0)
    later = lax.broadcasted_iota(jnp.int32, square, 0)
    sooner = lax.broadcasted_iota(jnp.int32, square, 1)

    def diagonal_blocks(i, carry):
        g = i // parts
        lower = later >= sooner
        equal = later == sooner
        for u in range(step):
            b = lax.rem(i, parts) * step + u
            at = span(b)
            x = act[at, lanes(g)]
            scores = lax.dot_general(
                act[at, lanes(2 * groups + g)],
                act[at, lanes(groups + g)],
                across,
                preferred_element_type=f32,
            )
            outs = []
            for h in range(2):
                line = b * lines + 4 * g + 2 * h
                cf_l = cols_ref[g, at, 2 * h : 2 * h + 1]
                eb_l = cols_ref[g, at, 2 * h + 1 : 2 * h + 2]
                cf_s = rows_ref[0, pl.ds(line, 1), :]
                eb_s = rows_ref[0, pl.ds(line + 1, 1), :]
                df_s = rows_ref[1, pl.ds(line, 1), :]
                db_s = rows_ref[1, pl.ds(line + 1, 1), :]
                decay = jnp.exp(jnp.where(lower, cf_l - cf_s, eb_s - eb_l))
                size = jnp.where(equal, df_s + db_s, jnp.where(lower, df_s, db_s))
                outs.append(
                    jnp.dot(
                        (scores * decay * size).astype(jnp.bfloat16), x, preferred_element_type=f32
                    )
                )
            y[at, lanes(g)] = split_heads(outs[0], outs[1], 1, tile)
        return carry

    count = groups * parts
    lax.fori_loop(0, count // 2, diagonal_blocks, 0)
    if n > 2:
        gather.sides(2)
    if n > 3:
        gather.column(3)
    gather.diagonal(1)
    lax.fori_loop(count // 2, count, diagonal_blocks, 0)

    def pooled(i, carry):
        where_global = (
            z * length + i * SPAN + lax.broadcasted_iota(jnp.int32, (SPAN, POOL_DIM), 0)
        )
        for j in range(groups):
            window = WINDOWS[j % 4]
            at = slice(3 * width + j * POOL_DIM, 3 * width + (j + 1) * POOL_DIM)
            block = pad[pl.ds(pl.multiple_of(i * SPAN, SPAN), SPAN + 2 * REACH), at]
            first = REACH - window // 2
            running = block[first : first + SPAN]
            for o in range(1, window):
                running = running + block[first + o : first + o + SPAN]
            lower = jnp.maximum(where_global - window // 2, 0)
            upper = jnp.minimum(where_global + window - window // 2, n * length)
            mean = running / (upper - lower).astype(f32)
            diff = (mean - block[REACH : REACH + SPAN]).astype(jnp.bfloat16)
            mapped = jnp.dot(diff, pool_mix_ref[c * groups + j], preferred_element_type=f32)
            gain = pool_gain_ref[:, lanes(c * groups + j)]
            mixed[span(i), width + j * POOL_DIM : width + (j + 1) * POOL_DIM] = (
                mapped * gain
            ).astype(jnp.bfloat16)
        return carry

    lax.fori_loop(0, blocks, pooled, 0)
    if n > 3:
        gather.sides(3)
    if n > 2:
        gather.diagonal(2)
    incoming[...] = jnp.zeros(incoming.shape, f32)
    for copy in sums:
        copy.wait_recv()
    for d in range(1, n):
        for r in range(2):

            def receive(d=d, r=r):
                states[d - 1][r].wait_recv()
                log = jnp.zeros(total_ref.shape, f32)
                for e in range(1, d):
                    log = log + totals[z - e if r == 0 else z + e]
                scale = jnp.exp(log)
                for g in range(groups):
                    for h in range(2):
                        line = 4 * g + 2 * h + r
                        at = slice(h * HEAD_DIM, (h + 1) * HEAD_DIM)
                        incoming[g, r, at] = incoming[g, r, at] + scale[
                            line : line + 1
                        ] * arrived[r, d - 1, g, at].astype(f32)

            pl.when(z >= d if r == 0 else z + d < n)(receive)
    squares[0] = jnp.zeros(squares.shape[1:], f32)

    def outputs(g, carry):
        for r in range(2):

            def keep(b, carried, r=r):
                for h in range(2):
                    prior[b, r * STATE + h * HEAD_DIM : r * STATE + (h + 1) * HEAD_DIM] = carried[
                        h
                    ].astype(jnp.bfloat16)

            scan(g, r, [incoming[g, r, :HEAD_DIM], incoming[g, r, HEAD_DIM:]], keep)
        for b in range(blocks):
            at = span(b)
            far = lax.dot_general(
                act[at, lanes(2 * groups + g)], prior[b], across, preferred_element_type=f32
            )
            out = y[at, lanes(g)]
            for r in range(2):
                reach = split_heads(
                    cols_ref[g, at, 8 + r : 9 + r], cols_ref[g, at, 10 + r : 11 + r], 1, tile
                )
                out = out + reach * far[:, r * STATE : (r + 1) * STATE]
            out = out * jax.nn.silu(stored_ref[at, lanes(g)].astype(f32))
            y[at, lanes(g)] = out
            squares[0, at] = squares[0, at] + jnp.sum(out * out, axis=-1, keepdims=True)
        return carry

    lax.fori_loop(0, groups, outputs, 0)
    other = remote(squares.at[0], squares.at[1], square_sem, (), partner)
    if n > 3:
        gather.diagonal(3)
    other.wait_recv()

    def normalize(b, carry):
        at = span(b)
        scale = lax.rsqrt((squares[0, at] + squares[1, at]) / (2 * width) + EPSILON)
        for g in range(groups):
            mixed[at, g * STATE : (g + 1) * STATE] = (
                y[at, g * STATE : (g + 1) * STATE] * scale * gain_ref[:, lanes(c * groups + g)]
            ).astype(jnp.bfloat16)
        return carry

    lax.fori_loop(0, blocks, normalize, 0)
    chunks = part_sem.shape[1]
    part = out_ref.shape[1] // chunks

    def product(first, i):
        return jnp.dot(
            mixed[pl.ds(pl.multiple_of(first, half), half), :],
            w_out[:, i * part : (i + 1) * part],
            preferred_element_type=f32,
        ).astype(jnp.bfloat16)

    sent = []
    for i in range(chunks):
        at = slice(i * part, (i + 1) * part)
        away[:, at] = product((1 - c) * half, i)
        ref = pl.ds(i * part, part)
        sent.append(remote(away.at[:, ref], got.at[:, ref], part_sem, (i,), partner))
    for i in range(chunks):
        at = slice(i * part, (i + 1) * part)
        kept = product(c * half, i)
        sent[i].wait_recv()
        out_ref[:, at] = (kept.astype(f32) + got[:, at].astype(f32)).astype(jnp.bfloat16)
    for cond, copy in pending:
        if cond is None:
            copy.wait_send()
        else:
            pl.when(cond)(copy.wait_send)
    gather.drain()


def fused_mixer(stored, rows, cols, totals, small, w_ssd, w_pool):
    n = lax.axis_size("sp")
    length = stored.shape[0]
    groups = cols.shape[0]
    width = groups * STATE
    blocks = length // SPAN
    out_rows, out_cols = 2 * w_ssd.shape[0], 4 * n * w_ssd.shape[1]
    anywhere = pl.BlockSpec(memory_space=pl.ANY)
    inside = pl.BlockSpec(memory_space=pltpu.VMEM)
    chunks = 8
    bf16, f32 = jnp.bfloat16, jnp.float32
    dma = pltpu.SemaphoreType.DMA
    return pl.pallas_call(
        mixer_kernel,
        out_shape=jax.ShapeDtypeStruct((length // 2, out_cols), bf16),
        in_specs=[inside] * (4 + len(small)) + [anywhere] * 2,
        out_specs=inside,
        scratch_shapes=[
            pltpu.VMEM((out_rows, out_cols), bf16),
            pltpu.VMEM((8, 3 * width), f32),
            pltpu.VMEM((length + 2 * REACH, 4 * width), f32),
            pltpu.VMEM((length, 3 * width), bf16),
            pltpu.VMEM((length, width), f32),
            pltpu.VMEM((groups, 2, blocks, STATE, STATE), f32),
            pltpu.VMEM((blocks, 2 * STATE, STATE), bf16),
            pltpu.VMEM((2, groups, STATE, STATE), bf16),
            pltpu.VMEM((2, n - 1, groups, STATE, STATE), bf16),
            pltpu.VMEM((groups, 2, STATE, STATE), f32),
            pltpu.VMEM((n,) + totals.shape, f32),
            pltpu.VMEM((2, length, SPAN), f32),
            pltpu.VMEM((length, 2 * width), bf16),
            pltpu.VMEM((length // 2, out_cols), bf16),
            pltpu.VMEM((length // 2, out_cols), bf16),
            pltpu.VMEM((2, 2 * REACH, 4 * width), bf16),
            dma((n, 14)),
            dma((n, 8)),
            dma((2,)),
            dma((2, 2)),
            dma((2, n - 1)),
            dma((2, 2, n - 1)),
            dma((2,)),
            dma((2, chunks)),
        ],
        compiler_params=pltpu.CompilerParams(collective_id=1, has_side_effects=True),
        name="mixer",
    )(stored, rows, cols, totals, *small, w_ssd, w_pool)


def split_heads(first, second, axis, shape):
    places = lax.broadcasted_iota(jnp.int32, shape, axis)
    return jnp.where(places < HEAD_DIM, first, second)


def ends_kernel(blocks, decay_ref, x_ref, k_ref, col_ref, ends_ref, final_ref):
    group = pl.program_id(0)
    tile = (SPAN, 2 * HEAD_DIM)
    for c in range(blocks):
        rows = pl.ds(c * SPAN, SPAN)
        x = x_ref[rows, :].astype(jnp.float32)
        k = k_ref[rows, :]
        for r in range(2):
            weight = split_heads(
                col_ref[0, rows, 4 + 2 * r : 5 + 2 * r],
                col_ref[0, rows, 5 + 2 * r : 6 + 2 * r],
                1,
                tile,
            )
            end = lax.dot_general(
                (x * weight).astype(jnp.bfloat16),
                k,
                (((0,), (0,)), ((), ())),
                preferred_element_type=jnp.float32,
            )
            ends_ref[0, r, c] = end
    states = (2 * HEAD_DIM, STATE)
    for r in range(2):
        total = jnp.zeros(states, jnp.float32)
        for c in range(blocks) if r == 0 else range(blocks - 1, -1, -1):
            at = ((group * blocks + c) * 2 + r) * 2
            scale = split_heads(decay_ref[at], decay_ref[at + 1], 0, states)
            total = total * scale + ends_ref[0, r, c]
        final_ref[0, r] = total


def outputs_kernel(
    blocks, decay_ref, x_ref, k_ref, q_ref, col_ref, row_ref, ends_ref, in_ref, y_ref, prior
):
    group = pl.program_id(0)
    states = (2 * HEAD_DIM, STATE)
    tile = (SPAN, 2 * HEAD_DIM)
    square = (SPAN, SPAN)
    for r in range(2):
        total = in_ref[0, r]
        for c in range(blocks) if r == 0 else range(blocks - 1, -1, -1):
            prior[r, c] = total.astype(jnp.bfloat16)
            at = ((group * blocks + c) * 2 + r) * 2
            scale = split_heads(decay_ref[at], decay_ref[at + 1], 0, states)
            total = total * scale + ends_ref[0, r, c]
    later = lax.broadcasted_iota(jnp.int32, square, 0)
    sooner = lax.broadcasted_iota(jnp.int32, square, 1)
    lower = later >= sooner
    equal = later == sooner
    across = (((1,), (1,)), ((), ()))
    for c in range(blocks):
        rows = pl.ds(c * SPAN, SPAN)
        x = x_ref[rows, :]
        q = q_ref[rows, :]
        scores = lax.dot_general(q, k_ref[rows, :], across, preferred_element_type=jnp.float32)
        parts = []
        for h in range(2):
            cf_l = col_ref[0, rows, 2 * h : 2 * h + 1]
            eb_l = col_ref[0, rows, 2 * h + 1 : 2 * h + 2]
            cf_s = row_ref[0, 4 * h : 4 * h + 1, rows]
            eb_s = row_ref[0, 4 * h + 1 : 4 * h + 2, rows]
            df_s = row_ref[0, 4 * h + 2 : 4 * h + 3, rows]
            db_s = row_ref[0, 4 * h + 3 : 4 * h + 4, rows]
            decay = jnp.exp(jnp.where(lower, cf_l - cf_s, eb_s - eb_l))
            step = jnp.where(equal, df_s + db_s, jnp.where(lower, df_s, db_s))
            parts.append(
                jnp.dot(
                    (scores * decay * step).astype(jnp.bfloat16),
                    x,
                    preferred_element_type=jnp.float32,
                )
            )
        out = split_heads(parts[0], parts[1], 1, tile)
        for r in range(2):
            reach = split_heads(
                col_ref[0, rows, 8 + 2 * r : 9 + 2 * r],
                col_ref[0, rows, 9 + 2 * r : 10 + 2 * r],
                1,
                tile,
            )
            out = out + reach * lax.dot_general(
                q, prior[r, c], across, preferred_element_type=jnp.float32
            )
        y_ref[rows, :] = out


def mixer(activated, width_ssd, width_key, steps, logs, sp_rank):
    length = activated.shape[0]
    heads = steps.shape[1]
    groups = width_key // STATE
    blocks = length // SPAN
    shaped = logs.reshape(2, heads, blocks, SPAN)
    ones = jnp.triu(jnp.ones((SPAN, SPAN), jnp.float32))
    inner = jnp.einsum("rhcs,sl->rhcl", shaped, ones, precision=HIGHEST)
    totals = inner[..., -1:]
    cf = inner[0]
    eb = inner[1] - shaped[1]
    wf = jnp.exp(totals[0] - cf) * steps[0].reshape(cf.shape)
    wb = jnp.exp(eb) * steps[1].reshape(cf.shape)
    reach_f = jnp.exp(cf)
    reach_b = jnp.exp(totals[1] - eb)

    def pair(a):
        return a.reshape(groups, 2, length)

    cf, eb, wf, wb, reach_f, reach_b = map(pair, (cf, eb, wf, wb, reach_f, reach_b))
    df, db = (pair(steps[0]), pair(steps[1]))
    packed = jnp.stack(
        [cf[:, 0], eb[:, 0], cf[:, 1], eb[:, 1]]
        + [wf[:, 0], wf[:, 1], wb[:, 0], wb[:, 1]]
        + [reach_f[:, 0], reach_f[:, 1], reach_b[:, 0], reach_b[:, 1]],
        axis=1,
    )
    cols = jnp.transpose(packed, (0, 2, 1))
    rows = jnp.stack(
        [cf[:, 0], eb[:, 0], df[:, 0], db[:, 0], cf[:, 1], eb[:, 1], df[:, 1], db[:, 1]], axis=1
    )
    block_logs = totals[..., 0]
    decays = jnp.exp(block_logs).reshape(2, groups, 2, blocks)
    decays = jnp.transpose(decays, (1, 3, 0, 2)).reshape(-1)
    smem = pl.BlockSpec(memory_space=pltpu.SMEM)
    x_blocks = width_ssd // STATE

    def wide(offset):
        return pl.BlockSpec((length, STATE), lambda g: (0, g + offset))

    col_spec = pl.BlockSpec((1, length, cols.shape[2]), lambda g: (g, 0, 0))
    ends_spec = pl.BlockSpec((1, 2, blocks, STATE, STATE), lambda g: (g, 0, 0, 0, 0))
    state_spec = pl.BlockSpec((1, 2, STATE, STATE), lambda g: (g, 0, 0, 0))
    ends, finals = pl.pallas_call(
        functools.partial(ends_kernel, blocks),
        grid=(groups,),
        out_shape=(
            jax.ShapeDtypeStruct((groups, 2, blocks, STATE, STATE), jnp.float32),
            jax.ShapeDtypeStruct((groups, 2, STATE, STATE), jnp.float32),
        ),
        in_specs=[smem, wide(0), wide(x_blocks), col_spec],
        out_specs=(ends_spec, state_spec),
        cost_estimate=pl.CostEstimate(
            flops=4 * length * groups * STATE * STATE,
            bytes_accessed=16 * length * groups * STATE,
            transcendentals=0,
        ),
        name="block_ends",
    )(decays, activated, activated, cols)
    device_totals = jnp.sum(block_logs, axis=-1)
    all_totals = lax.all_gather(
        device_totals[None].astype(jnp.bfloat16), "sp", axis=0, tiled=True
    ).astype(jnp.float32)
    states = jnp.transpose(finals, (1, 0, 2, 3)).reshape(2, heads, HEAD_DIM, STATE)
    forward_in, backward_in = prefix_states(all_totals, states.astype(jnp.bfloat16), sp_rank)
    incoming = jnp.stack([forward_in, backward_in]).reshape(2, groups, STATE, STATE)
    incoming = jnp.transpose(incoming, (1, 0, 2, 3))
    return pl.pallas_call(
        functools.partial(outputs_kernel, blocks),
        grid=(groups,),
        out_shape=jax.ShapeDtypeStruct((length, groups * STATE), jnp.float32),
        in_specs=[
            smem,
            wide(0),
            wide(x_blocks),
            wide(x_blocks + groups),
            col_spec,
            pl.BlockSpec((1, 8, length), lambda g: (g, 0, 0)),
            ends_spec,
            state_spec,
        ],
        out_specs=wide(0),
        scratch_shapes=[pltpu.VMEM((2, blocks, STATE, STATE), jnp.bfloat16)],
        cost_estimate=pl.CostEstimate(
            flops=10 * length * groups * STATE * STATE,
            bytes_accessed=40 * length * groups * STATE,
            transcendentals=2 * length * groups * SPAN,
        ),
        name="block_outputs",
    )(decays, activated, activated, activated, cols, rows, ends, incoming)


def prefix_states(all_totals, finals, rank):
    chain_length = all_totals.shape[0]
    device_ids = jnp.arange(chain_length, dtype=jnp.int32)[:, None]
    forward_cum = jnp.cumsum(all_totals[:, 0], axis=0)
    forward_mine = lax.dynamic_slice_in_dim(forward_cum - all_totals[:, 0], rank, 1, 0)
    forward_weight = jnp.exp(jnp.where(device_ids < rank, forward_mine - forward_cum, -jnp.inf))
    backward_cum = jnp.cumsum(all_totals[:, 1], axis=0)
    backward_mine = lax.dynamic_slice_in_dim(backward_cum, rank, 1, 0)
    backward_weight = jnp.exp(
        jnp.where(device_ids > rank, backward_cum - all_totals[:, 1] - backward_mine, -jnp.inf)
    )
    forward_in = jnp.zeros(finals.shape[1:], jnp.float32)
    backward_in = jnp.zeros(finals.shape[1:], jnp.float32)
    for d in range(1, chain_length):
        ahead = [(i, i + d) for i in range(chain_length - d)]
        back = [(i + d, i) for i in range(chain_length - d)]
        from_left = lax.ppermute(finals[0], "sp", ahead).astype(jnp.float32)
        from_right = lax.ppermute(finals[1], "sp", back).astype(jnp.float32)
        left = lax.dynamic_index_in_dim(forward_weight, jnp.maximum(rank - d, 0), 0, False)
        right = lax.dynamic_index_in_dim(
            backward_weight, jnp.minimum(rank + d, chain_length - 1), 0, False
        )
        forward_in = forward_in + left[:, None, None] * from_left
        backward_in = backward_in + right[:, None, None] * from_right
    return (forward_in, backward_in)


def local(
    tokens,
    norm_gain,
    w_gate,
    w_value,
    w_bkey,
    w_query,
    w_pool_in,
    w_step,
    step_bias,
    decay_rate,
    decay_shift,
    conv_value,
    conv_bkey,
    conv_query,
    mix_gain,
    pool_mix,
    pool_gain,
    w_out_ssd,
    w_out_pool,
):
    tp_count = lax.axis_size("tp")
    sp_count = lax.axis_size("sp")
    tp_rank = lax.axis_index("tp")
    sp_rank = lax.axis_index("sp")
    heads_dev = DUALITY_HEADS // tp_count
    groups_dev = GROUPS // tp_count
    pools_dev = POOL_GROUPS // tp_count
    width_ssd = heads_dev * HEAD_DIM
    width_key = groups_dev * STATE
    width_pool = pools_dev * POOL_DIM
    fast = (
        tp_count == 2
        and lax.axis_size("fs") == 4
        and 2 <= sp_count <= 4
        and w_gate.shape[0] % 128 == 0
        and w_out_ssd.shape[1] % 128 == 0
        and pools_dev == groups_dev
        and width_ssd == width_key
        and groups_dev % 4 == 0
        and 2 * tokens.shape[1] * 2 * heads_dev % (SPAN * SPAN) == 0
    )
    step_cols = lax.dynamic_slice_in_dim(w_step, tp_rank * heads_dev, heads_dev, 2)
    bias_dev = lax.dynamic_slice_in_dim(step_bias, tp_rank * heads_dev, heads_dev, 1)
    rate_dev = lax.dynamic_slice_in_dim(decay_rate, tp_rank * heads_dev, heads_dev, 1)
    if fast:
        lines = 2 * heads_dev
        scales = jnp.stack([bias_dev, rate_dev], axis=-1)
        scales = jnp.transpose(scales, (1, 0, 2)).reshape(lines, 2, 1)
        stored, rows, cols, totals = project(
            (w_gate, w_value, w_bkey, w_query, w_pool_in),
            tokens[0],
            norm_gain,
            jnp.transpose(step_cols, (2, 1, 0)).reshape(lines, -1),
            jnp.broadcast_to(scales, (lines, 2, SPAN)).reshape(lines, 2 * SPAN),
            decay_shift.reshape(lines, -1),
        )
        small = (
            conv_value,
            conv_bkey,
            conv_query,
            mix_gain[None],
            pool_mix,
            pool_gain[None],
        )
        return fused_mixer(stored, rows, cols, totals, small, w_out_ssd, w_out_pool)[None]
    step_cols = step_cols.reshape(w_step.shape[0], 2 * heads_dev)
    weights = jnp.concatenate([w_gate, w_value, w_bkey, w_query, w_pool_in], axis=1)
    combined, widened = gather_inputs(weights, tokens[0])
    out_rows = lax.all_gather(
        jnp.concatenate([w_out_ssd, w_out_pool], axis=0), ("sp", "fs"), axis=1, tiled=True
    )
    widened = widened.astype(jnp.float32)
    scaling = lax.rsqrt(jnp.mean(widened * widened, axis=-1, keepdims=True) + EPSILON)
    normed = (widened * scaling * norm_gain).astype(jnp.bfloat16)
    stored = jnp.dot(normed, combined, preferred_element_type=jnp.float32).astype(jnp.bfloat16)
    raw_steps = jnp.dot(normed, step_cols, preferred_element_type=jnp.float32)
    length = stored.shape[0]
    padded = padded_2(stored[:, width_ssd:], (("sp", 0),), REACH)
    conv_cols = width_ssd + 2 * width_key
    taps = jnp.concatenate(
        [
            lax.dynamic_slice_in_dim(conv_value, tp_rank * width_ssd, width_ssd, 1),
            lax.dynamic_slice_in_dim(conv_bkey, tp_rank * width_key, width_key, 1),
            lax.dynamic_slice_in_dim(conv_query, tp_rank * width_key, width_key, 1),
        ],
        axis=1,
    ).astype(jnp.float32)
    margin = CONV_WIDTH // 2
    convolved = jnp.zeros((length, conv_cols), jnp.float32)
    for offset in range(CONV_WIDTH):
        begin = REACH - margin + offset
        convolved = (
            convolved
            + padded[begin : begin + length, :conv_cols].astype(jnp.float32) * taps[offset]
        )
    activated = jax.nn.silu(convolved).astype(jnp.bfloat16)
    steps = jax.nn.softplus(raw_steps.reshape(length, 2, heads_dev) + bias_dev).transpose(1, 2, 0)
    logs = -rate_dev[:, :, None] * steps - decay_shift[0].transpose(1, 0, 2)
    heads_out = mixer(activated, width_ssd, width_key, steps, logs, sp_rank)
    gated = heads_out * jax.nn.silu(stored[:, :width_ssd].astype(jnp.float32))
    squares = lax.psum(jnp.sum(gated * gated, axis=-1), "tp")
    gain_dev = lax.dynamic_slice_in_dim(mix_gain, tp_rank * width_ssd, width_ssd, 0)
    ssd_mix = (gated * lax.rsqrt(squares / D_SSM + EPSILON)[:, None] * gain_dev).astype(
        jnp.bfloat16
    )
    pool_rows = padded[:, conv_cols:].astype(jnp.float32)
    own_rows = pool_rows[REACH : REACH + length]
    where_global = sp_rank * length + jnp.arange(length, dtype=jnp.int32)
    seq_length = length * sp_count
    window_means = []
    for window in WINDOWS:
        running = jnp.zeros((length, width_pool), jnp.float32)
        for offset in range(-(window // 2), window - window // 2):
            running = running + pool_rows[REACH + offset : REACH + offset + length]
        lower = jnp.clip(where_global - window // 2, 0, seq_length)
        upper = jnp.clip(where_global + window - window // 2, 0, seq_length)
        window_means.append(running / (upper - lower).astype(jnp.float32)[:, None])
    stacked = jnp.stack(window_means).reshape(4, length, pools_dev, POOL_DIM)
    group_ids = tp_rank * pools_dev + jnp.arange(pools_dev, dtype=jnp.int32)
    selector = (jnp.arange(4, dtype=jnp.int32)[:, None] == (group_ids % 4)[None, :]).astype(
        jnp.float32
    )
    means = jnp.sum(stacked * selector[:, None, :, None], axis=0)
    differences = (means - own_rows.reshape(length, pools_dev, POOL_DIM)).astype(jnp.bfloat16)
    pool_weights = lax.dynamic_slice_in_dim(pool_mix, tp_rank * pools_dev, pools_dev, 0)
    mapped = jnp.einsum(
        "rgc,gcd->rgd", differences, pool_weights, preferred_element_type=jnp.float32
    )
    pool_gain_dev = lax.dynamic_slice_in_dim(pool_gain, tp_rank * width_pool, width_pool, 0)
    pool_out = (mapped.reshape(length, width_pool) * pool_gain_dev).astype(jnp.bfloat16)
    mixed = jnp.concatenate([ssd_mix, pool_out], axis=1)
    if tp_count == 2:
        part = length // 2
        away = lax.dynamic_slice_in_dim(mixed, (1 - tp_rank) * part, part, 0)
        home = lax.dynamic_slice_in_dim(mixed, tp_rank * part, part, 0)
        sent = jnp.dot(away, out_rows, preferred_element_type=jnp.float32).astype(jnp.bfloat16)
        received = lax.ppermute(sent, "tp", [(0, 1), (1, 0)])
        kept = lax.optimization_barrier(
            jnp.dot(home, out_rows, preferred_element_type=jnp.float32).astype(jnp.bfloat16)
        )
        summed = (kept.astype(jnp.float32) + received.astype(jnp.float32)).astype(jnp.bfloat16)
    else:
        summed = lax.psum_scatter(
            jnp.dot(mixed, out_rows, preferred_element_type=jnp.float32).astype(jnp.bfloat16),
            "tp",
            scatter_dimension=0,
            tiled=True,
        )
    return summed[None]


def solution(mesh):
    return jax.shard_map(
        local,
        mesh=mesh,
        in_specs=(
            P("fs", ("sp", "tp"), None),
            P(),
            P(("sp", "fs"), "tp"),
            P(("sp", "fs"), "tp"),
            P(("sp", "fs"), "tp"),
            P(("sp", "fs"), "tp"),
            P(("sp", "fs"), "tp"),
            P(),
            P(),
            P(),
            P("fs", "tp", None, "sp"),
            P(),
            P(),
            P(),
            P(),
            P(),
            P(),
            P("tp", ("sp", "fs")),
            P("tp", ("sp", "fs")),
        ),
        out_specs=P("fs", ("sp", "tp"), None),
        check_vma=False,
    )
```

```python
import functools

import jax
import jax.numpy as jnp
from jax import lax
from jax.experimental import pallas as pl
from jax.experimental.pallas import tpu as pltpu
from jax.sharding import PartitionSpec as P

HEAD_DIM = 64
DUALITY_HEADS = 16
GROUPS = 8
STATE = 128
CONV_WIDTH = 5
POOL_GROUPS = 8
POOL_DIM = 128
SPAN = 128
REACH = 8
D_SSM = 1024


EPSILON = 1e-06
HIGHEST = lax.Precision.HIGHEST
WINDOWS = (2, 4, 8, 16)


def padded_2(cells, sides, width):
    for axis, dim in sides:
        count = lax.axis_size(axis)
        ends = count - 1
        head = lax.slice_in_dim(cells, 0, width, axis=dim)
        tail = lax.slice_in_dim(cells, cells.shape[dim] - width, cells.shape[dim], axis=dim)
        cells = jnp.concatenate(
            [
                lax.ppermute(tail, axis, [(i, (i + 1) % count) for i in range(ends)]),
                cells,
                lax.ppermute(head, axis, [((i + 1) % count, i) for i in range(ends)]),
            ],
            axis=dim,
        )
    return cells


MESH = pl.DeviceIdType.MESH


def gather_kernel(n_sp, n_tp, w_ref, t_ref, w_out, t_out, send, recv, local_sem):
    z = lax.axis_index("sp")
    f = lax.axis_index("fs")
    c = lax.axis_index("tp")
    fx = f + 1 - 2 * lax.rem(f, 2)
    fy = lax.rem(f + 2, 4)
    rows = w_ref.shape[0]
    half = rows // 2
    x_dev = (z, fx, c)
    y_dev = (z, fy, c)
    z_devs = [(lax.rem(z + d, n_sp), f, c) for d in range(1, n_sp)]
    t_devs = [(z, f, lax.rem(c + d, n_tp)) for d in range(1, n_tp)]
    partners = [x_dev, y_dev] + z_devs + t_devs
    barrier = pltpu.get_barrier_semaphore()
    for dev in partners:
        pl.semaphore_signal(barrier, inc=1, device_id=dev, device_id_type=MESH)
    pl.semaphore_wait(barrier, len(partners))

    def remote(src, dst, index, dev):
        copy = pltpu.make_async_remote_copy(
            src_ref=src,
            dst_ref=dst,
            send_sem=send.at[index],
            recv_sem=recv.at[index],
            device_id=dev,
            device_id_type=MESH,
        )
        copy.start()
        return copy

    base = n_sp - 1
    z_copies = [remote(w_ref, w_out.at[z, f], d, z_devs[d]) for d in range(n_sp - 1)]
    full = []
    relay = []

    def send_full(d):
        if d == 0:
            src = w_ref
            origin = z
        else:
            z_copies[d - 1].wait_recv()
            origin = lax.rem(z - d + n_sp, n_sp)
            src = w_out.at[origin, f]
        dst = w_out.at[origin, f]
        full.append(
            (
                remote(src, dst, base + 4 * d, x_dev),
                remote(src, dst, base + 4 * d + 1, y_dev),
            )
        )

    def send_relay(d):
        origin = lax.rem(z - d + n_sp, n_sp)
        full[d][0].wait_recv()
        part = w_out.at[origin, fx, pl.ds(0, half)]
        first = remote(part, part, base + 4 * d + 2, y_dev)
        full[d][1].wait_recv()
        part = w_out.at[origin, fy, pl.ds(half, half)]
        relay.append((first, remote(part, part, base + 4 * d + 3, x_dev)))

    send_full(0)
    own_w = pltpu.make_async_copy(w_ref, w_out.at[z, f], local_sem.at[0])
    own_w.start()
    own_t = pltpu.make_async_copy(t_ref, t_out.at[c], local_sem.at[1])
    own_t.start()
    tbase = base + 4 * n_sp
    t_copies = [remote(t_ref, t_out.at[c], tbase + d, t_devs[d]) for d in range(n_tp - 1)]
    for d in range(1, n_sp):
        send_full(d)
        send_relay(d - 1)
    send_relay(n_sp - 1)
    for pair in relay:
        for copy in pair:
            copy.wait_recv()
    for copy in t_copies:
        copy.wait_recv()
    for copy in z_copies + t_copies:
        copy.wait_send()
    for pair in full + relay:
        for copy in pair:
            copy.wait_send()
    own_w.wait()
    own_t.wait()


def gather_inputs(weights, tokens):
    n_sp = lax.axis_size("sp")
    n_fs = lax.axis_size("fs")
    n_tp = lax.axis_size("tp")
    rows, cols = weights.shape
    if n_fs != 4:
        return (
            lax.all_gather(weights, ("sp", "fs"), axis=0, tiled=True),
            lax.all_gather(tokens, "tp", axis=0, tiled=True),
        )
    count = (n_sp - 1) + 4 * n_sp + (n_tp - 1)
    wide, toks = pl.pallas_call(
        functools.partial(gather_kernel, n_sp, n_tp),
        out_shape=(
            jax.ShapeDtypeStruct((n_sp, n_fs, rows, cols), weights.dtype),
            jax.ShapeDtypeStruct((n_tp,) + tokens.shape, tokens.dtype),
        ),
        in_specs=[pl.BlockSpec(memory_space=pltpu.VMEM)] * 2,
        out_specs=[pl.BlockSpec(memory_space=pl.ANY)] * 2,
        scratch_shapes=[
            pltpu.SemaphoreType.DMA((count,)),
            pltpu.SemaphoreType.DMA((count,)),
            pltpu.SemaphoreType.DMA((2,)),
        ],
        compiler_params=pltpu.CompilerParams(collective_id=0, has_side_effects=True),
        cost_estimate=pl.CostEstimate(
            flops=0, bytes_accessed=200 * n_sp * n_fs * rows * cols, transcendentals=0
        ),
        name="gather_inputs",
    )(weights, tokens)
    return wide.reshape(n_sp * n_fs * rows, cols), toks.reshape(-1, tokens.shape[1])


class LineGather:
    def __init__(self, piece, send, recv):
        self.n = lax.axis_size("sp")
        self.z = lax.axis_index("sp")
        self.f = lax.axis_index("fs")
        self.c = lax.axis_index("tp")
        self.fx = self.f + 1 - 2 * lax.rem(self.f, 2)
        self.fy = lax.rem(self.f + 2, 4)
        self.fd = 3 - self.f
        self.piece, self.send, self.recv = piece, send, recv
        self.x_dev = (self.z, self.fx, self.c)
        self.y_dev = (self.z, self.fy, self.c)
        self.up_dev = (lax.rem(self.z + 1, self.n), self.f, self.c)
        self.down_dev = (lax.rem(self.z + self.n - 1, self.n), self.f, self.c)
        self.order = [self.nearest(k) for k in range(self.n)]
        self.pending = []

    def barrier(self, extra=()):
        barrier = pltpu.get_barrier_semaphore()
        devices = [self.x_dev, self.y_dev, self.up_dev, self.down_dev, *extra]
        for device in devices:
            pl.semaphore_signal(barrier, inc=1, device_id=device, device_id_type=MESH)
        pl.semaphore_wait(barrier, len(devices))

    def nearest(self, k):
        z, n = self.z, self.n
        low = jnp.minimum(z, n - 1 - z)
        sign = 1 if k % 2 == 0 else -1
        paired = z + sign * ((k + 1) // 2)
        past = jnp.where(2 * z < n - 1, z + (k - low), z - (k - low))
        return jnp.where(k <= 2 * low, paired, past)

    def by_line(self, z, p):
        near = jnp.logical_or(p == z + 1, p == z - 1)
        if self.n >= 4:
            near = jnp.logical_or(near, jnp.logical_and(z == 0, p == 2))
            near = jnp.logical_or(near, jnp.logical_and(z == self.n - 1, p == self.n - 3))
        return near

    def copy(self, src, dst, p, s, r, device):
        return pltpu.make_async_remote_copy(
            src_ref=src,
            dst_ref=dst,
            send_sem=self.send.at[p, s],
            recv_sem=self.recv.at[p, r],
            device_id=device,
            device_id_type=MESH,
        )

    def start(self, cond, src, dst, p, s, r, device):
        copy = self.copy(src, dst, p, s, r, device)
        if cond is None:
            copy.start()
        else:
            pl.when(cond)(copy.start)
        self.pending.append((cond, copy))

    def arrive(self, ref, p, r):
        self.copy(ref, ref, p, 0, r, self.x_dev).wait_recv()

    def column(self, k, halves=(0, 1)):
        p = self.order[k]
        up = jnp.logical_and(p <= self.z, self.z < self.n - 1)
        down = jnp.logical_and(p >= self.z, self.z > 0)
        for h in halves:
            ref = self.piece(p, self.f, h)
            if k > 0:
                self.arrive(ref, p, h)
            self.start(None, ref, ref, p, 4 + h, 2 + h, self.x_dev)
            self.start(None, ref, ref, p, 6 + h, 4 + h, self.y_dev)
            self.start(up, ref, ref, p, h, h, self.up_dev)
            self.start(down, ref, ref, p, 2 + h, h, self.down_dev)

    def sides(self, k, halves=(0, 1)):
        p = self.order[k]
        relay = jnp.logical_not(self.by_line(self.z, p))
        for h in halves:
            x_part = self.piece(p, self.fx, h)
            y_part = self.piece(p, self.fy, h)
            self.arrive(x_part, p, 2 + h)
            if h == 0:
                self.start(relay, x_part, x_part, p, 8, 6, self.y_dev)
            self.arrive(y_part, p, 4 + h)
            if h == 1:
                self.start(relay, y_part, y_part, p, 9, 7, self.x_dev)

    def diagonal(self, k):
        p = self.order[k]
        z, n = self.z, self.n
        up = jnp.logical_and(jnp.logical_and(p <= z, z < n - 1), self.by_line(z + 1, p))
        down = jnp.logical_and(jnp.logical_and(p >= z, z > 0), self.by_line(z - 1, p))
        for h in range(2):
            part = self.piece(p, self.fd, h)
            self.arrive(part, p, 6 + h)
            self.start(up, part, part, p, 10 + h, 6 + h, self.up_dev)
            self.start(down, part, part, p, 12 + h, 6 + h, self.down_dev)

    def stage(self, i):
        ready = []
        if i < self.n:
            self.sides(i)
            ready += [(i, self.fx), (i, self.fy)]
        if i + 1 < self.n:
            self.column(i + 1)
            ready.append((i + 1, self.f))
        if i > 0:
            self.diagonal(i - 1)
            ready.append((i - 1, self.fd))
        return [(self.order[k], member) for k, member in ready]

    def drain(self):
        for cond, copy in self.pending:
            if cond is None:
                copy.wait_send()
            else:
                pl.when(cond)(copy.wait_send)


def layer_kernel(
    gate_ref,
    value_ref,
    key_ref,
    query_ref,
    pool_ref,
    t_ref,
    w_ssd_ref,
    w_pool_ref,
    norm_ref,
    step_ref,
    scale_ref,
    shift_ref,
    conv_value_ref,
    conv_key_ref,
    conv_query_ref,
    gain_ref,
    pool_mix_ref,
    pool_gain_ref,
    kept_ref,
    got,
    mixed_in,
    others_in,
    w_out,
    toks,
    acc,
    gate,
    rows_ref,
    cols_ref,
    total_ref,
    taps,
    pad,
    act,
    y,
    ends,
    prior,
    finals,
    arrived,
    incoming,
    totals,
    squares,
    mixed,
    away,
    w_send,
    w_recv,
    local_sem,
    pair_sem,
    halo_sem,
    total_sem,
    state_sem,
    square_sem,
    part_sem,
):
    length = toks.shape[0]
    mine = t_ref.shape[0]
    half = length // 2
    groups = cols_ref.shape[0]
    lines = total_ref.shape[0]
    blocks = length // SPAN
    width = groups * STATE
    z = lax.axis_index("sp")
    f = lax.axis_index("fs")
    c = lax.axis_index("tp")
    n = lax.axis_size("sp")
    tile = (SPAN, 2 * HEAD_DIM)
    square = (SPAN, SPAN)
    f32 = jnp.float32
    across = (((1,), (1,)), ((), ()))

    def rows_of(buf):
        lot = buf.shape[2] // 2
        return lambda p, member, h: buf.at[p, member, pl.ds(h * lot, lot)]

    def columns_of(p, member, h):
        lot, cols = w_ssd_ref.shape
        at = pl.ds(pl.multiple_of((p * 4 + member) * cols, cols), cols)
        return w_out.at[pl.ds(h * lot, lot), at]

    first = LineGather(rows_of(mixed_in), w_send.at[0], w_recv.at[0])
    second = LineGather(rows_of(others_in), w_send.at[1], w_recv.at[1])
    third = LineGather(columns_of, w_send.at[2], w_recv.at[2])
    partner = (z, f, 1 - c)
    ahead = [(lax.rem(z + d, n), f, c) for d in range(n)]
    behind = [(lax.rem(z + n - d, n), f, c) for d in range(n)]

    def local(src, dst, i):
        copy = pltpu.make_async_copy(src, dst, local_sem.at[i])
        copy.start()
        return copy

    own_rows = toks.at[pl.ds(pl.multiple_of(c * mine, mine), mine)]
    own_first = [
        local(ref, mixed_in.at[z, f, :, pl.ds(i * width, width)], i)
        for i, ref in enumerate((value_ref, key_ref, query_ref))
    ]
    own_tokens = local(t_ref, own_rows, 3)
    own_second = [
        local(ref, others_in.at[z, f, :, pl.ds(i * width, width)], 4 + i)
        for i, ref in enumerate((gate_ref, pool_ref))
    ]
    own_third = [
        local(ref, columns_of(z, f, h), 6 + h) for h, ref in enumerate((w_ssd_ref, w_pool_ref))
    ]
    first.barrier((partner, *ahead[2 : n - 1]))
    pending = []

    def remote(src, dst, sems, index, device, cond=None):
        copy = pltpu.make_async_remote_copy(
            src_ref=src,
            dst_ref=dst,
            send_sem=sems.at[(0, *index)],
            recv_sem=sems.at[(1, *index)],
            device_id=device,
            device_id_type=MESH,
        )
        if cond is None:
            copy.start()
        else:
            pl.when(cond)(copy.start)
        pending.append((cond, copy))
        return copy

    for copy in own_first:
        copy.wait()
    first.column(0)
    own_tokens.wait()
    pair = remote(t_ref, own_rows, pair_sem, (), partner)
    for copy in own_second + own_third:
        copy.wait()
    chunk = 32

    def normalize(start):
        def body(i, carry):
            at = pl.ds(pl.multiple_of(start + i * chunk, chunk), chunk)
            wide = toks[at, :].astype(jnp.float32)
            mean = jnp.mean(wide * wide, axis=-1, keepdims=True)
            toks[at, :] = (wide * lax.rsqrt(mean + EPSILON) * norm_ref[...]).astype(jnp.bfloat16)
            return carry

        lax.fori_loop(0, mine // chunk, body, 0)

    normalize(c * mine)
    pair.wait_recv()
    normalize((1 - c) * mine)

    def lanes(i, count=1):
        return pl.ds(pl.multiple_of(i * STATE, STATE), count * STATE)

    def span(i):
        return pl.ds(pl.multiple_of(i * SPAN, SPAN), SPAN)

    def multiply(buf, p, member, begin=False, store=None):
        depth = buf.shape[2]
        at = pl.ds(pl.multiple_of((p * 4 + member) * depth, depth), depth)
        wide = 256

        def body(i, carry):
            cols = pl.ds(pl.multiple_of(i * wide, wide), wide)
            for m in range(2):
                part = jnp.dot(
                    toks[m * half : (m + 1) * half, at],
                    buf[p, member, :, cols],
                    preferred_element_type=f32,
                )
                if not begin:
                    part = part + acc[m * half : (m + 1) * half, cols]
                if store is None:
                    acc[m * half : (m + 1) * half, cols] = part
                else:
                    store(m, i, wide, part.astype(jnp.bfloat16))
            return carry

        count = buf.shape[3] // wide
        if store is None:
            lax.fori_loop(0, count, body, 0)
        else:
            for i in range(count):
                body(i, 0)

    def store_first(m, i, wide, part):
        at = slice(REACH + m * half, REACH + (m + 1) * half)
        pad[at, i * wide : (i + 1) * wide] = part.astype(f32)

    def store_second(m, i, wide, part):
        if i * wide < width:
            gate[m * half : (m + 1) * half, i * wide : (i + 1) * wide] = part
        else:
            at = slice(REACH + m * half, REACH + (m + 1) * half)
            pad[at, 2 * width + i * wide : 2 * width + (i + 1) * wide] = part.astype(f32)

    def step_sizes():
        raw = lax.dot_general(
            step_ref[...], toks[...], (((1,), (1,)), ((), ())), preferred_element_type=jnp.float32
        )
        raw = raw + scale_ref[:, :1]
        shift = jnp.concatenate([shift_ref[0, h] for h in range(shift_ref.shape[1])], axis=0)
        steps = jnp.maximum(raw, 0.0) + jnp.log1p(jnp.exp(-jnp.abs(raw)))
        logs = -scale_ref[:, SPAN : SPAN + 1] * steps - shift
        cut = [slice(i * SPAN, (i + 1) * SPAN) for i in range(blocks)]
        steps = jnp.concatenate([steps[:, at] for at in cut], axis=0)
        logs = jnp.concatenate([logs[:, at] for at in cut], axis=0)
        square = (SPAN, SPAN)
        upper = lax.broadcasted_iota(jnp.int32, square, 0) <= lax.broadcasted_iota(
            jnp.int32, square, 1
        )
        inner = jnp.dot(
            logs, upper.astype(jnp.float32), precision=HIGHEST, preferred_element_type=jnp.float32
        )
        total = inner[:, SPAN - 1 :]
        backward = lax.rem(lax.broadcasted_iota(jnp.int32, logs.shape, 0), 2) == 1
        along = inner - jnp.where(backward, logs, 0.0)
        weight = jnp.exp(jnp.where(backward, along, total - along)) * steps
        reach = jnp.exp(jnp.where(backward, total - along, along))
        rows_ref[0] = along
        rows_ref[1] = steps
        rows_ref[2] = jnp.broadcast_to(jnp.exp(total), logs.shape)
        whole = total[:lines]
        for i in range(1, blocks):
            whole = whole + total[i * lines : (i + 1) * lines]
        total_ref[...] = jnp.broadcast_to(whole, total_ref.shape)
        turned = [jnp.transpose(v) for v in (along, weight, reach)]
        for g in range(lines // 4):
            for i in range(blocks):
                for j in range(3):
                    at = i * lines + 4 * g
                    cols_ref[g, cut[i], 4 * j : 4 * j + 4] = turned[j][:, at : at + 4]

    order = first.order
    multiply(mixed_in, order[0], f, begin=True)
    step_sizes()
    for i, ref in enumerate((conv_value_ref, conv_key_ref, conv_query_ref)):
        taps[:CONV_WIDTH, i * width : (i + 1) * width] = ref[
            :, pl.ds(pl.multiple_of(c * width, width), width)
        ].astype(f32)
    crossed = []
    for k in range(1, n + 1):
        for h in range(2):
            first.sides(k - 1, (h,))
            if k < n:
                first.column(k, (h,))
        if k == n:
            second.column(0)
        multiply(mixed_in, order[k - 1], first.fx)
        multiply(mixed_in, order[k - 1], first.fy)
        if k < n:
            multiply(mixed_in, order[k], f)
        due = [0] if k == 1 else [k - 2] if k >= 3 else []
        if k == n:
            due = [d for d in range(n) if d not in crossed]
        for d in due:
            first.diagonal(d)
            crossed.append(d)
            done = len(crossed) == n
            multiply(mixed_in, order[d], first.fd, store=store_first if done else None)

    below, above = z > 0, z < n - 1

    def swap_edges(i, at):
        top = remote(
            pad.at[pl.ds(length, REACH), at], pad.at[pl.ds(0, REACH), at], halo_sem, (i, 0), ahead[1], above
        )
        bottom = remote(
            pad.at[pl.ds(REACH, REACH), at],
            pad.at[pl.ds(REACH + length, REACH), at],
            halo_sem,
            (i, 1),
            behind[1],
            below,
        )

        @pl.when(jnp.logical_not(below))
        def _():
            pad[:REACH, at] = jnp.zeros((REACH, at.size), f32)

        @pl.when(jnp.logical_not(above))
        def _():
            pad[REACH + length :, at] = jnp.zeros((REACH, at.size), f32)

        def wait():
            pl.when(below)(top.wait_recv)
            pl.when(above)(bottom.wait_recv)

        return wait

    edges = swap_edges(0, pl.ds(0, 3 * width))
    sums = [
        remote(total_ref, totals.at[z], total_sem, (d - 1,), ahead[d]) for d in range(1, n)
    ]
    queue = [(order[0], f)]
    queue += second.stage(0)
    edges()
    margin = CONV_WIDTH // 2

    def convolve(i, carry):
        at = lanes(i)
        tap = taps[:, at]
        for b in range(blocks):
            begin = REACH - margin + b * SPAN
            total = pad[begin : begin + SPAN, at] * tap[:1]
            for o in range(1, CONV_WIDTH):
                total = total + pad[begin + o : begin + o + SPAN, at] * tap[o : o + 1]
            act[b * SPAN : (b + 1) * SPAN, at] = jax.nn.silu(total).astype(jnp.bfloat16)
        return carry

    lax.fori_loop(0, 2 * groups, convolve, 0)
    queue += second.stage(1)
    step = 4 if blocks % 4 == 0 else 1
    parts = blocks // step

    def block_ends(i, carry):
        g = i // parts
        for u in range(step):
            b = lax.rem(i, parts) * step + u
            at = span(b)
            x = act[at, lanes(g)].astype(f32)
            k = act[at, lanes(groups + g)]
            for r in range(2):
                weight = split_heads(
                    cols_ref[g, at, 4 + r : 5 + r], cols_ref[g, at, 6 + r : 7 + r], 1, tile
                )
                ends[g, r, b] = lax.dot_general(
                    (x * weight).astype(jnp.bfloat16),
                    k,
                    (((0,), (0,)), ((), ())),
                    preferred_element_type=f32,
                )
        return carry

    lax.fori_loop(0, groups * parts, block_ends, 0)

    def scan(g, r, start, each):
        order = range(blocks) if r == 0 else range(blocks - 1, -1, -1)
        carried = list(start)
        for b in order:
            each(b, carried)
            for h in range(2):
                at = b * lines + 4 * g + 2 * h + r
                scale = rows_ref[2, pl.ds(at, 1), :]
                carried[h] = carried[h] * scale + ends[g, r, b, h * HEAD_DIM : (h + 1) * HEAD_DIM]
        return carried

    def own_states(g, carry):
        zero = jnp.zeros((HEAD_DIM, STATE), f32)
        for r in range(2):
            last = scan(g, r, [zero, zero], lambda b, carried: None)
            for h in range(2):
                finals[r, g, h * HEAD_DIM : (h + 1) * HEAD_DIM] = last[h].astype(jnp.bfloat16)
        return carry

    lax.fori_loop(0, groups, own_states, 0)
    if n >= 3:
        queue += second.stage(2)
    states = []
    for d in range(1, n):
        states.append(
            (
                remote(finals.at[0], arrived.at[0, d - 1], state_sem, (0, d - 1), ahead[d], z + d < n),
                remote(finals.at[1], arrived.at[1, d - 1], state_sem, (1, d - 1), behind[d], z >= d),
            )
        )
    third.column(0)
    total = 4 * n
    taken = [0]

    def advance():
        while queue:
            p, member = queue.pop(0)
            taken[0] += 1
            multiply(
                others_in,
                p,
                member,
                begin=taken[0] == 1,
                store=store_second if taken[0] == total else None,
            )

    advance()
    if n >= 4:
        queue += second.stage(3)
    third.stage(0)
    lax.fori_loop(2 * groups, 3 * groups, convolve, 0)
    advance()
    queue += second.stage(n)
    advance()
    margins = swap_edges(1, pl.ds(3 * width, width))
    third.stage(1)
    later = lax.broadcasted_iota(jnp.int32, square, 0)
    sooner = lax.broadcasted_iota(jnp.int32, square, 1)

    def diagonal_blocks(i, carry):
        g = i // parts
        lower = later >= sooner
        equal = later == sooner
        for u in range(step):
            b = lax.rem(i, parts) * step + u
            at = span(b)
            x = act[at, lanes(g)]
            scores = lax.dot_general(
                act[at, lanes(2 * groups + g)],
                act[at, lanes(groups + g)],
                across,
                preferred_element_type=f32,
            )
            outs = []
            for h in range(2):
                line = b * lines + 4 * g + 2 * h
                cf_l = cols_ref[g, at, 2 * h : 2 * h + 1]
                eb_l = cols_ref[g, at, 2 * h + 1 : 2 * h + 2]
                cf_s = rows_ref[0, pl.ds(line, 1), :]
                eb_s = rows_ref[0, pl.ds(line + 1, 1), :]
                df_s = rows_ref[1, pl.ds(line, 1), :]
                db_s = rows_ref[1, pl.ds(line + 1, 1), :]
                decay = jnp.exp(jnp.where(lower, cf_l - cf_s, eb_s - eb_l))
                size = jnp.where(equal, df_s + db_s, jnp.where(lower, df_s, db_s))
                outs.append(
                    jnp.dot(
                        (scores * decay * size).astype(jnp.bfloat16), x, preferred_element_type=f32
                    )
                )
            y[at, lanes(g)] = split_heads(outs[0], outs[1], 1, tile)
        return carry

    count = groups * parts
    lax.fori_loop(0, count // 2, diagonal_blocks, 0)
    if n >= 3:
        third.stage(2)
    lax.fori_loop(count // 2, count, diagonal_blocks, 0)
    margins()

    def pooled(i, carry):
        where_global = (
            z * length + i * SPAN + lax.broadcasted_iota(jnp.int32, (SPAN, POOL_DIM), 0)
        )
        for j in range(groups):
            window = WINDOWS[j % 4]
            at = slice(3 * width + j * POOL_DIM, 3 * width + (j + 1) * POOL_DIM)
            block = pad[pl.ds(pl.multiple_of(i * SPAN, SPAN), SPAN + 2 * REACH), at]
            first = REACH - window // 2
            running = block[first : first + SPAN]
            for o in range(1, window):
                running = running + block[first + o : first + o + SPAN]
            lower = jnp.maximum(where_global - window // 2, 0)
            upper = jnp.minimum(where_global + window - window // 2, n * length)
            mean = running / (upper - lower).astype(f32)
            diff = (mean - block[REACH : REACH + SPAN]).astype(jnp.bfloat16)
            mapped = jnp.dot(diff, pool_mix_ref[c * groups + j], preferred_element_type=f32)
            gain = pool_gain_ref[:, lanes(c * groups + j)]
            mixed[span(i), width + j * POOL_DIM : width + (j + 1) * POOL_DIM] = (
                mapped * gain
            ).astype(jnp.bfloat16)
        return carry

    lax.fori_loop(0, blocks, pooled, 0)
    if n >= 4:
        third.stage(3)
    incoming[...] = jnp.zeros(incoming.shape, f32)
    for copy in sums:
        copy.wait_recv()
    for d in range(1, n):
        for r in range(2):

            def receive(d=d, r=r):
                states[d - 1][r].wait_recv()
                log = jnp.zeros(total_ref.shape, f32)
                for e in range(1, d):
                    log = log + totals[z - e if r == 0 else z + e]
                scale = jnp.exp(log)
                for g in range(groups):
                    for h in range(2):
                        line = 4 * g + 2 * h + r
                        at = slice(h * HEAD_DIM, (h + 1) * HEAD_DIM)
                        incoming[g, r, at] = incoming[g, r, at] + scale[
                            line : line + 1
                        ] * arrived[r, d - 1, g, at].astype(f32)

            pl.when(z >= d if r == 0 else z + d < n)(receive)
    squares[0] = jnp.zeros(squares.shape[1:], f32)

    def outputs(g, carry):
        for r in range(2):

            def keep(b, carried, r=r):
                for h in range(2):
                    prior[b, r * STATE + h * HEAD_DIM : r * STATE + (h + 1) * HEAD_DIM] = carried[
                        h
                    ].astype(jnp.bfloat16)

            scan(g, r, [incoming[g, r, :HEAD_DIM], incoming[g, r, HEAD_DIM:]], keep)
        for b in range(blocks):
            at = span(b)
            far = lax.dot_general(
                act[at, lanes(2 * groups + g)], prior[b], across, preferred_element_type=f32
            )
            out = y[at, lanes(g)]
            for r in range(2):
                reach = split_heads(
                    cols_ref[g, at, 8 + r : 9 + r], cols_ref[g, at, 10 + r : 11 + r], 1, tile
                )
                out = out + reach * far[:, r * STATE : (r + 1) * STATE]
            out = out * jax.nn.silu(gate[at, lanes(g)].astype(f32))
            y[at, lanes(g)] = out
            squares[0, at] = squares[0, at] + jnp.sum(out * out, axis=-1, keepdims=True)
        return carry

    lax.fori_loop(0, groups, outputs, 0)
    other = remote(squares.at[0], squares.at[1], square_sem, (), partner)
    third.stage(n)
    other.wait_recv()

    def scale_rows(b, carry):
        at = span(b)
        scale = lax.rsqrt((squares[0, at] + squares[1, at]) / (2 * width) + EPSILON)
        for g in range(groups):
            mixed[at, g * STATE : (g + 1) * STATE] = (
                y[at, g * STATE : (g + 1) * STATE] * scale * gain_ref[:, lanes(c * groups + g)]
            ).astype(jnp.bfloat16)
        return carry

    lax.fori_loop(0, blocks, scale_rows, 0)
    chunks = part_sem.shape[1]
    part = kept_ref.shape[1] // chunks

    def product(first, i):
        return jnp.dot(
            mixed[pl.ds(pl.multiple_of(first, half), half), :],
            w_out[:, i * part : (i + 1) * part],
            preferred_element_type=f32,
        ).astype(jnp.bfloat16)

    sent = []
    for i in range(chunks):
        at = slice(i * part, (i + 1) * part)
        away[:, at] = product((1 - c) * half, i)
        ref = pl.ds(i * part, part)
        sent.append(remote(away.at[:, ref], got.at[:, ref], part_sem, (i,), partner))
    for i in range(chunks):
        kept_ref[:, i * part : (i + 1) * part] = product(c * half, i)
    for copy in sent:
        copy.wait_recv()
    for cond, copy in pending:
        if cond is None:
            copy.wait_send()
        else:
            pl.when(cond)(copy.wait_send)
    for gather in (first, second, third):
        gather.drain()


def fused_layer(weights, tokens, w_ssd, w_pool, small, groups):
    n = lax.axis_size("sp")
    half, features = tokens.shape
    length = 2 * half
    width = groups * STATE
    lines = 4 * groups
    blocks = length // SPAN
    rows = weights[0].shape[0]
    out_rows, out_cols = 2 * w_ssd.shape[0], 4 * n * w_ssd.shape[1]
    anywhere = pl.BlockSpec(memory_space=pl.ANY)
    inside = pl.BlockSpec(memory_space=pltpu.VMEM)
    chunks = 8
    bf16, f32 = jnp.bfloat16, jnp.float32
    dma = pltpu.SemaphoreType.DMA
    return pl.pallas_call(
        layer_kernel,
        out_shape=[jax.ShapeDtypeStruct((half, out_cols), bf16)] * 2,
        in_specs=[anywhere] * 8 + [inside] * len(small),
        out_specs=[inside] * 2,
        scratch_shapes=[
            pltpu.VMEM((n, 4, rows, 3 * width), bf16),
            pltpu.VMEM((n, 4, rows, 2 * width), bf16),
            pltpu.VMEM((out_rows, out_cols), bf16),
            pltpu.VMEM((length, features), bf16),
            pltpu.VMEM((length, 3 * width), f32),
            pltpu.VMEM((length, width), bf16),
            pltpu.VMEM((3, lines * blocks, SPAN), f32),
            pltpu.VMEM((groups, length, 12), f32),
            pltpu.VMEM((lines, SPAN), f32),
            pltpu.VMEM((8, 3 * width), f32),
            pltpu.VMEM((length + 2 * REACH, 4 * width), f32),
            pltpu.VMEM((length, 3 * width), bf16),
            pltpu.VMEM((length, width), f32),
            pltpu.VMEM((groups, 2, blocks, STATE, STATE), f32),
            pltpu.VMEM((blocks, 2 * STATE, STATE), bf16),
            pltpu.VMEM((2, groups, STATE, STATE), bf16),
            pltpu.VMEM((2, n - 1, groups, STATE, STATE), bf16),
            pltpu.VMEM((groups, 2, STATE, STATE), f32),
            pltpu.VMEM((n, lines, SPAN), f32),
            pltpu.VMEM((2, length, SPAN), f32),
            pltpu.VMEM((length, 2 * width), bf16),
            pltpu.VMEM((half, out_cols), bf16),
            dma((3, n, 14)),
            dma((3, n, 8)),
            dma((8,)),
            dma((2,)),
            dma((2, 2, 2)),
            dma((2, n - 1)),
            dma((2, 2, n - 1)),
            dma((2,)),
            dma((2, chunks)),
        ],
        compiler_params=pltpu.CompilerParams(
            collective_id=0, has_side_effects=True, vmem_limit_bytes=63 * 2**20
        ),
        name="mixer",
    )(*weights, tokens, w_ssd, w_pool, *small)


def split_heads(first, second, axis, shape):
    places = lax.broadcasted_iota(jnp.int32, shape, axis)
    return jnp.where(places < HEAD_DIM, first, second)


def ends_kernel(blocks, decay_ref, x_ref, k_ref, col_ref, ends_ref, final_ref):
    group = pl.program_id(0)
    tile = (SPAN, 2 * HEAD_DIM)
    for c in range(blocks):
        rows = pl.ds(c * SPAN, SPAN)
        x = x_ref[rows, :].astype(jnp.float32)
        k = k_ref[rows, :]
        for r in range(2):
            weight = split_heads(
                col_ref[0, rows, 4 + 2 * r : 5 + 2 * r],
                col_ref[0, rows, 5 + 2 * r : 6 + 2 * r],
                1,
                tile,
            )
            end = lax.dot_general(
                (x * weight).astype(jnp.bfloat16),
                k,
                (((0,), (0,)), ((), ())),
                preferred_element_type=jnp.float32,
            )
            ends_ref[0, r, c] = end
    states = (2 * HEAD_DIM, STATE)
    for r in range(2):
        total = jnp.zeros(states, jnp.float32)
        for c in range(blocks) if r == 0 else range(blocks - 1, -1, -1):
            at = ((group * blocks + c) * 2 + r) * 2
            scale = split_heads(decay_ref[at], decay_ref[at + 1], 0, states)
            total = total * scale + ends_ref[0, r, c]
        final_ref[0, r] = total


def outputs_kernel(
    blocks, decay_ref, x_ref, k_ref, q_ref, col_ref, row_ref, ends_ref, in_ref, y_ref, prior
):
    group = pl.program_id(0)
    states = (2 * HEAD_DIM, STATE)
    tile = (SPAN, 2 * HEAD_DIM)
    square = (SPAN, SPAN)
    for r in range(2):
        total = in_ref[0, r]
        for c in range(blocks) if r == 0 else range(blocks - 1, -1, -1):
            prior[r, c] = total.astype(jnp.bfloat16)
            at = ((group * blocks + c) * 2 + r) * 2
            scale = split_heads(decay_ref[at], decay_ref[at + 1], 0, states)
            total = total * scale + ends_ref[0, r, c]
    later = lax.broadcasted_iota(jnp.int32, square, 0)
    sooner = lax.broadcasted_iota(jnp.int32, square, 1)
    lower = later >= sooner
    equal = later == sooner
    across = (((1,), (1,)), ((), ()))
    for c in range(blocks):
        rows = pl.ds(c * SPAN, SPAN)
        x = x_ref[rows, :]
        q = q_ref[rows, :]
        scores = lax.dot_general(q, k_ref[rows, :], across, preferred_element_type=jnp.float32)
        parts = []
        for h in range(2):
            cf_l = col_ref[0, rows, 2 * h : 2 * h + 1]
            eb_l = col_ref[0, rows, 2 * h + 1 : 2 * h + 2]
            cf_s = row_ref[0, 4 * h : 4 * h + 1, rows]
            eb_s = row_ref[0, 4 * h + 1 : 4 * h + 2, rows]
            df_s = row_ref[0, 4 * h + 2 : 4 * h + 3, rows]
            db_s = row_ref[0, 4 * h + 3 : 4 * h + 4, rows]
            decay = jnp.exp(jnp.where(lower, cf_l - cf_s, eb_s - eb_l))
            step = jnp.where(equal, df_s + db_s, jnp.where(lower, df_s, db_s))
            parts.append(
                jnp.dot(
                    (scores * decay * step).astype(jnp.bfloat16),
                    x,
                    preferred_element_type=jnp.float32,
                )
            )
        out = split_heads(parts[0], parts[1], 1, tile)
        for r in range(2):
            reach = split_heads(
                col_ref[0, rows, 8 + 2 * r : 9 + 2 * r],
                col_ref[0, rows, 9 + 2 * r : 10 + 2 * r],
                1,
                tile,
            )
            out = out + reach * lax.dot_general(
                q, prior[r, c], across, preferred_element_type=jnp.float32
            )
        y_ref[rows, :] = out


def mixer(activated, width_ssd, width_key, steps, logs, sp_rank):
    length = activated.shape[0]
    heads = steps.shape[1]
    groups = width_key // STATE
    blocks = length // SPAN
    shaped = logs.reshape(2, heads, blocks, SPAN)
    ones = jnp.triu(jnp.ones((SPAN, SPAN), jnp.float32))
    inner = jnp.einsum("rhcs,sl->rhcl", shaped, ones, precision=HIGHEST)
    totals = inner[..., -1:]
    cf = inner[0]
    eb = inner[1] - shaped[1]
    wf = jnp.exp(totals[0] - cf) * steps[0].reshape(cf.shape)
    wb = jnp.exp(eb) * steps[1].reshape(cf.shape)
    reach_f = jnp.exp(cf)
    reach_b = jnp.exp(totals[1] - eb)

    def pair(a):
        return a.reshape(groups, 2, length)

    cf, eb, wf, wb, reach_f, reach_b = map(pair, (cf, eb, wf, wb, reach_f, reach_b))
    df, db = (pair(steps[0]), pair(steps[1]))
    packed = jnp.stack(
        [cf[:, 0], eb[:, 0], cf[:, 1], eb[:, 1]]
        + [wf[:, 0], wf[:, 1], wb[:, 0], wb[:, 1]]
        + [reach_f[:, 0], reach_f[:, 1], reach_b[:, 0], reach_b[:, 1]],
        axis=1,
    )
    cols = jnp.transpose(packed, (0, 2, 1))
    rows = jnp.stack(
        [cf[:, 0], eb[:, 0], df[:, 0], db[:, 0], cf[:, 1], eb[:, 1], df[:, 1], db[:, 1]], axis=1
    )
    block_logs = totals[..., 0]
    decays = jnp.exp(block_logs).reshape(2, groups, 2, blocks)
    decays = jnp.transpose(decays, (1, 3, 0, 2)).reshape(-1)
    smem = pl.BlockSpec(memory_space=pltpu.SMEM)
    x_blocks = width_ssd // STATE

    def wide(offset):
        return pl.BlockSpec((length, STATE), lambda g: (0, g + offset))

    col_spec = pl.BlockSpec((1, length, cols.shape[2]), lambda g: (g, 0, 0))
    ends_spec = pl.BlockSpec((1, 2, blocks, STATE, STATE), lambda g: (g, 0, 0, 0, 0))
    state_spec = pl.BlockSpec((1, 2, STATE, STATE), lambda g: (g, 0, 0, 0))
    ends, finals = pl.pallas_call(
        functools.partial(ends_kernel, blocks),
        grid=(groups,),
        out_shape=(
            jax.ShapeDtypeStruct((groups, 2, blocks, STATE, STATE), jnp.float32),
            jax.ShapeDtypeStruct((groups, 2, STATE, STATE), jnp.float32),
        ),
        in_specs=[smem, wide(0), wide(x_blocks), col_spec],
        out_specs=(ends_spec, state_spec),
        cost_estimate=pl.CostEstimate(
            flops=4 * length * groups * STATE * STATE,
            bytes_accessed=16 * length * groups * STATE,
            transcendentals=0,
        ),
        name="block_ends",
    )(decays, activated, activated, cols)
    device_totals = jnp.sum(block_logs, axis=-1)
    all_totals = lax.all_gather(
        device_totals[None].astype(jnp.bfloat16), "sp", axis=0, tiled=True
    ).astype(jnp.float32)
    states = jnp.transpose(finals, (1, 0, 2, 3)).reshape(2, heads, HEAD_DIM, STATE)
    forward_in, backward_in = prefix_states(all_totals, states.astype(jnp.bfloat16), sp_rank)
    incoming = jnp.stack([forward_in, backward_in]).reshape(2, groups, STATE, STATE)
    incoming = jnp.transpose(incoming, (1, 0, 2, 3))
    return pl.pallas_call(
        functools.partial(outputs_kernel, blocks),
        grid=(groups,),
        out_shape=jax.ShapeDtypeStruct((length, groups * STATE), jnp.float32),
        in_specs=[
            smem,
            wide(0),
            wide(x_blocks),
            wide(x_blocks + groups),
            col_spec,
            pl.BlockSpec((1, 8, length), lambda g: (g, 0, 0)),
            ends_spec,
            state_spec,
        ],
        out_specs=wide(0),
        scratch_shapes=[pltpu.VMEM((2, blocks, STATE, STATE), jnp.bfloat16)],
        cost_estimate=pl.CostEstimate(
            flops=10 * length * groups * STATE * STATE,
            bytes_accessed=40 * length * groups * STATE,
            transcendentals=2 * length * groups * SPAN,
        ),
        name="block_outputs",
    )(decays, activated, activated, activated, cols, rows, ends, incoming)


def prefix_states(all_totals, finals, rank):
    chain_length = all_totals.shape[0]
    device_ids = jnp.arange(chain_length, dtype=jnp.int32)[:, None]
    forward_cum = jnp.cumsum(all_totals[:, 0], axis=0)
    forward_mine = lax.dynamic_slice_in_dim(forward_cum - all_totals[:, 0], rank, 1, 0)
    forward_weight = jnp.exp(jnp.where(device_ids < rank, forward_mine - forward_cum, -jnp.inf))
    backward_cum = jnp.cumsum(all_totals[:, 1], axis=0)
    backward_mine = lax.dynamic_slice_in_dim(backward_cum, rank, 1, 0)
    backward_weight = jnp.exp(
        jnp.where(device_ids > rank, backward_cum - all_totals[:, 1] - backward_mine, -jnp.inf)
    )
    forward_in = jnp.zeros(finals.shape[1:], jnp.float32)
    backward_in = jnp.zeros(finals.shape[1:], jnp.float32)
    for d in range(1, chain_length):
        ahead = [(i, i + d) for i in range(chain_length - d)]
        back = [(i + d, i) for i in range(chain_length - d)]
        from_left = lax.ppermute(finals[0], "sp", ahead).astype(jnp.float32)
        from_right = lax.ppermute(finals[1], "sp", back).astype(jnp.float32)
        left = lax.dynamic_index_in_dim(forward_weight, jnp.maximum(rank - d, 0), 0, False)
        right = lax.dynamic_index_in_dim(
            backward_weight, jnp.minimum(rank + d, chain_length - 1), 0, False
        )
        forward_in = forward_in + left[:, None, None] * from_left
        backward_in = backward_in + right[:, None, None] * from_right
    return (forward_in, backward_in)


def local(
    tokens,
    norm_gain,
    w_gate,
    w_value,
    w_bkey,
    w_query,
    w_pool_in,
    w_step,
    step_bias,
    decay_rate,
    decay_shift,
    conv_value,
    conv_bkey,
    conv_query,
    mix_gain,
    pool_mix,
    pool_gain,
    w_out_ssd,
    w_out_pool,
):
    tp_count = lax.axis_size("tp")
    sp_count = lax.axis_size("sp")
    tp_rank = lax.axis_index("tp")
    sp_rank = lax.axis_index("sp")
    heads_dev = DUALITY_HEADS // tp_count
    groups_dev = GROUPS // tp_count
    pools_dev = POOL_GROUPS // tp_count
    width_ssd = heads_dev * HEAD_DIM
    width_key = groups_dev * STATE
    width_pool = pools_dev * POOL_DIM
    fast = (
        tp_count == 2
        and lax.axis_size("fs") == 4
        and 2 <= sp_count <= 4
        and w_gate.shape[0] % 128 == 0
        and w_out_ssd.shape[1] % 128 == 0
        and pools_dev == groups_dev
        and width_ssd == width_key
        and groups_dev % 4 == 0
        and 2 * tokens.shape[1] * 2 * heads_dev % (SPAN * SPAN) == 0
    )
    step_cols = lax.dynamic_slice_in_dim(w_step, tp_rank * heads_dev, heads_dev, 2)
    bias_dev = lax.dynamic_slice_in_dim(step_bias, tp_rank * heads_dev, heads_dev, 1)
    rate_dev = lax.dynamic_slice_in_dim(decay_rate, tp_rank * heads_dev, heads_dev, 1)
    if fast:
        lines = 2 * heads_dev
        scales = jnp.stack([bias_dev, rate_dev], axis=-1)
        scales = jnp.transpose(scales, (1, 0, 2)).reshape(lines, 2, 1)
        small = (
            norm_gain[None],
            jnp.transpose(step_cols, (2, 1, 0)).reshape(lines, -1),
            jnp.broadcast_to(scales, (lines, 2, SPAN)).reshape(lines, 2 * SPAN),
            decay_shift,
            conv_value,
            conv_bkey,
            conv_query,
            mix_gain[None],
            pool_mix,
            pool_gain[None],
        )
        kept, got = fused_layer(
            (w_gate, w_value, w_bkey, w_query, w_pool_in),
            tokens[0],
            w_out_ssd,
            w_out_pool,
            small,
            groups_dev,
        )
        return (kept.astype(jnp.float32) + got.astype(jnp.float32)).astype(jnp.bfloat16)[None]
    step_cols = step_cols.reshape(w_step.shape[0], 2 * heads_dev)
    weights = jnp.concatenate([w_gate, w_value, w_bkey, w_query, w_pool_in], axis=1)
    combined, widened = gather_inputs(weights, tokens[0])
    out_rows = lax.all_gather(
        jnp.concatenate([w_out_ssd, w_out_pool], axis=0), ("sp", "fs"), axis=1, tiled=True
    )
    widened = widened.astype(jnp.float32)
    scaling = lax.rsqrt(jnp.mean(widened * widened, axis=-1, keepdims=True) + EPSILON)
    normed = (widened * scaling * norm_gain).astype(jnp.bfloat16)
    stored = jnp.dot(normed, combined, preferred_element_type=jnp.float32).astype(jnp.bfloat16)
    raw_steps = jnp.dot(normed, step_cols, preferred_element_type=jnp.float32)
    length = stored.shape[0]
    padded = padded_2(stored[:, width_ssd:], (("sp", 0),), REACH)
    conv_cols = width_ssd + 2 * width_key
    taps = jnp.concatenate(
        [
            lax.dynamic_slice_in_dim(conv_value, tp_rank * width_ssd, width_ssd, 1),
            lax.dynamic_slice_in_dim(conv_bkey, tp_rank * width_key, width_key, 1),
            lax.dynamic_slice_in_dim(conv_query, tp_rank * width_key, width_key, 1),
        ],
        axis=1,
    ).astype(jnp.float32)
    margin = CONV_WIDTH // 2
    convolved = jnp.zeros((length, conv_cols), jnp.float32)
    for offset in range(CONV_WIDTH):
        begin = REACH - margin + offset
        convolved = (
            convolved
            + padded[begin : begin + length, :conv_cols].astype(jnp.float32) * taps[offset]
        )
    activated = jax.nn.silu(convolved).astype(jnp.bfloat16)
    steps = jax.nn.softplus(raw_steps.reshape(length, 2, heads_dev) + bias_dev).transpose(1, 2, 0)
    logs = -rate_dev[:, :, None] * steps - decay_shift[0].transpose(1, 0, 2)
    heads_out = mixer(activated, width_ssd, width_key, steps, logs, sp_rank)
    gated = heads_out * jax.nn.silu(stored[:, :width_ssd].astype(jnp.float32))
    squares = lax.psum(jnp.sum(gated * gated, axis=-1), "tp")
    gain_dev = lax.dynamic_slice_in_dim(mix_gain, tp_rank * width_ssd, width_ssd, 0)
    ssd_mix = (gated * lax.rsqrt(squares / D_SSM + EPSILON)[:, None] * gain_dev).astype(
        jnp.bfloat16
    )
    pool_rows = padded[:, conv_cols:].astype(jnp.float32)
    own_rows = pool_rows[REACH : REACH + length]
    where_global = sp_rank * length + jnp.arange(length, dtype=jnp.int32)
    seq_length = length * sp_count
    window_means = []
    for window in WINDOWS:
        running = jnp.zeros((length, width_pool), jnp.float32)
        for offset in range(-(window // 2), window - window // 2):
            running = running + pool_rows[REACH + offset : REACH + offset + length]
        lower = jnp.clip(where_global - window // 2, 0, seq_length)
        upper = jnp.clip(where_global + window - window // 2, 0, seq_length)
        window_means.append(running / (upper - lower).astype(jnp.float32)[:, None])
    stacked = jnp.stack(window_means).reshape(4, length, pools_dev, POOL_DIM)
    group_ids = tp_rank * pools_dev + jnp.arange(pools_dev, dtype=jnp.int32)
    selector = (jnp.arange(4, dtype=jnp.int32)[:, None] == (group_ids % 4)[None, :]).astype(
        jnp.float32
    )
    means = jnp.sum(stacked * selector[:, None, :, None], axis=0)
    differences = (means - own_rows.reshape(length, pools_dev, POOL_DIM)).astype(jnp.bfloat16)
    pool_weights = lax.dynamic_slice_in_dim(pool_mix, tp_rank * pools_dev, pools_dev, 0)
    mapped = jnp.einsum(
        "rgc,gcd->rgd", differences, pool_weights, preferred_element_type=jnp.float32
    )
    pool_gain_dev = lax.dynamic_slice_in_dim(pool_gain, tp_rank * width_pool, width_pool, 0)
    pool_out = (mapped.reshape(length, width_pool) * pool_gain_dev).astype(jnp.bfloat16)
    mixed = jnp.concatenate([ssd_mix, pool_out], axis=1)
    if tp_count == 2:
        part = length // 2
        away = lax.dynamic_slice_in_dim(mixed, (1 - tp_rank) * part, part, 0)
        home = lax.dynamic_slice_in_dim(mixed, tp_rank * part, part, 0)
        sent = jnp.dot(away, out_rows, preferred_element_type=jnp.float32).astype(jnp.bfloat16)
        received = lax.ppermute(sent, "tp", [(0, 1), (1, 0)])
        kept = lax.optimization_barrier(
            jnp.dot(home, out_rows, preferred_element_type=jnp.float32).astype(jnp.bfloat16)
        )
        summed = (kept.astype(jnp.float32) + received.astype(jnp.float32)).astype(jnp.bfloat16)
    else:
        summed = lax.psum_scatter(
            jnp.dot(mixed, out_rows, preferred_element_type=jnp.float32).astype(jnp.bfloat16),
            "tp",
            scatter_dimension=0,
            tiled=True,
        )
    return summed[None]


def solution(mesh):
    return jax.shard_map(
        local,
        mesh=mesh,
        in_specs=(
            P("fs", ("sp", "tp"), None),
            P(),
            P(("sp", "fs"), "tp"),
            P(("sp", "fs"), "tp"),
            P(("sp", "fs"), "tp"),
            P(("sp", "fs"), "tp"),
            P(("sp", "fs"), "tp"),
            P(),
            P(),
            P(),
            P("fs", "tp", None, "sp"),
            P(),
            P(),
            P(),
            P(),
            P(),
            P(),
            P("tp", ("sp", "fs")),
            P("tp", ("sp", "fs")),
        ),
        out_specs=P("fs", ("sp", "tp"), None),
        check_vma=False,
    )
```

```python
import functools

import jax
import jax.numpy as jnp
from jax import lax
from jax.experimental import pallas as pl
from jax.experimental.pallas import tpu as pltpu
from jax.sharding import PartitionSpec as P

HEAD_DIM = 64
DUALITY_HEADS = 16
GROUPS = 8
STATE = 128
CONV_WIDTH = 5
POOL_GROUPS = 8
POOL_DIM = 128
SPAN = 128
REACH = 8
EDGE = 16
VMEM_LIMIT = 63 * 2**20
D_SSM = 1024


EPSILON = 1e-06
HIGHEST = lax.Precision.HIGHEST
WINDOWS = (2, 4, 8, 16)


def padded_2(cells, sides, width):
    for axis, dim in sides:
        count = lax.axis_size(axis)
        ends = count - 1
        head = lax.slice_in_dim(cells, 0, width, axis=dim)
        tail = lax.slice_in_dim(cells, cells.shape[dim] - width, cells.shape[dim], axis=dim)
        cells = jnp.concatenate(
            [
                lax.ppermute(tail, axis, [(i, (i + 1) % count) for i in range(ends)]),
                cells,
                lax.ppermute(head, axis, [((i + 1) % count, i) for i in range(ends)]),
            ],
            axis=dim,
        )
    return cells


MESH = pl.DeviceIdType.MESH


def gather_kernel(n_sp, n_tp, w_ref, t_ref, w_out, t_out, send, recv, local_sem):
    z = lax.axis_index("sp")
    f = lax.axis_index("fs")
    c = lax.axis_index("tp")
    fx = f + 1 - 2 * lax.rem(f, 2)
    fy = lax.rem(f + 2, 4)
    rows = w_ref.shape[0]
    half = rows // 2
    x_dev = (z, fx, c)
    y_dev = (z, fy, c)
    z_devs = [(lax.rem(z + d, n_sp), f, c) for d in range(1, n_sp)]
    t_devs = [(z, f, lax.rem(c + d, n_tp)) for d in range(1, n_tp)]
    partners = [x_dev, y_dev] + z_devs + t_devs
    barrier = pltpu.get_barrier_semaphore()
    for dev in partners:
        pl.semaphore_signal(barrier, inc=1, device_id=dev, device_id_type=MESH)
    pl.semaphore_wait(barrier, len(partners))

    def remote(src, dst, index, dev):
        copy = pltpu.make_async_remote_copy(
            src_ref=src,
            dst_ref=dst,
            send_sem=send.at[index],
            recv_sem=recv.at[index],
            device_id=dev,
            device_id_type=MESH,
        )
        copy.start()
        return copy

    base = n_sp - 1
    z_copies = [remote(w_ref, w_out.at[z, f], d, z_devs[d]) for d in range(n_sp - 1)]
    full = []
    relay = []

    def send_full(d):
        if d == 0:
            src = w_ref
            origin = z
        else:
            z_copies[d - 1].wait_recv()
            origin = lax.rem(z - d + n_sp, n_sp)
            src = w_out.at[origin, f]
        dst = w_out.at[origin, f]
        full.append(
            (
                remote(src, dst, base + 4 * d, x_dev),
                remote(src, dst, base + 4 * d + 1, y_dev),
            )
        )

    def send_relay(d):
        origin = lax.rem(z - d + n_sp, n_sp)
        full[d][0].wait_recv()
        part = w_out.at[origin, fx, pl.ds(0, half)]
        first = remote(part, part, base + 4 * d + 2, y_dev)
        full[d][1].wait_recv()
        part = w_out.at[origin, fy, pl.ds(half, half)]
        relay.append((first, remote(part, part, base + 4 * d + 3, x_dev)))

    send_full(0)
    own_w = pltpu.make_async_copy(w_ref, w_out.at[z, f], local_sem.at[0])
    own_w.start()
    own_t = pltpu.make_async_copy(t_ref, t_out.at[c], local_sem.at[1])
    own_t.start()
    tbase = base + 4 * n_sp
    t_copies = [remote(t_ref, t_out.at[c], tbase + d, t_devs[d]) for d in range(n_tp - 1)]
    for d in range(1, n_sp):
        send_full(d)
        send_relay(d - 1)
    send_relay(n_sp - 1)
    for pair in relay:
        for copy in pair:
            copy.wait_recv()
    for copy in t_copies:
        copy.wait_recv()
    for copy in z_copies + t_copies:
        copy.wait_send()
    for pair in full + relay:
        for copy in pair:
            copy.wait_send()
    own_w.wait()
    own_t.wait()


def gather_inputs(weights, tokens):
    n_sp = lax.axis_size("sp")
    n_fs = lax.axis_size("fs")
    n_tp = lax.axis_size("tp")
    rows, cols = weights.shape
    if n_fs != 4:
        return (
            lax.all_gather(weights, ("sp", "fs"), axis=0, tiled=True),
            lax.all_gather(tokens, "tp", axis=0, tiled=True),
        )
    count = (n_sp - 1) + 4 * n_sp + (n_tp - 1)
    wide, toks = pl.pallas_call(
        functools.partial(gather_kernel, n_sp, n_tp),
        out_shape=(
            jax.ShapeDtypeStruct((n_sp, n_fs, rows, cols), weights.dtype),
            jax.ShapeDtypeStruct((n_tp,) + tokens.shape, tokens.dtype),
        ),
        in_specs=[pl.BlockSpec(memory_space=pltpu.VMEM)] * 2,
        out_specs=[pl.BlockSpec(memory_space=pl.ANY)] * 2,
        scratch_shapes=[
            pltpu.SemaphoreType.DMA((count,)),
            pltpu.SemaphoreType.DMA((count,)),
            pltpu.SemaphoreType.DMA((2,)),
        ],
        compiler_params=pltpu.CompilerParams(collective_id=0, has_side_effects=True),
        cost_estimate=pl.CostEstimate(
            flops=0, bytes_accessed=200 * n_sp * n_fs * rows * cols, transcendentals=0
        ),
        name="gather_inputs",
    )(weights, tokens)
    return wide.reshape(n_sp * n_fs * rows, cols), toks.reshape(-1, tokens.shape[1])


class LineGather:
    def __init__(self, piece, send, recv):
        self.n = lax.axis_size("sp")
        self.z = lax.axis_index("sp")
        self.f = lax.axis_index("fs")
        self.c = lax.axis_index("tp")
        self.fx = self.f + 1 - 2 * lax.rem(self.f, 2)
        self.fy = lax.rem(self.f + 2, 4)
        self.fd = 3 - self.f
        self.piece, self.send, self.recv = piece, send, recv
        self.x_dev = (self.z, self.fx, self.c)
        self.y_dev = (self.z, self.fy, self.c)
        self.up_dev = (lax.rem(self.z + 1, self.n), self.f, self.c)
        self.down_dev = (lax.rem(self.z + self.n - 1, self.n), self.f, self.c)
        self.order = [self.nearest(k) for k in range(self.n)]
        self.pending = []

    def barrier(self, extra=()):
        barrier = pltpu.get_barrier_semaphore()
        devices = [self.x_dev, self.y_dev, self.up_dev, self.down_dev, *extra]
        for device in devices:
            pl.semaphore_signal(barrier, inc=1, device_id=device, device_id_type=MESH)
        pl.semaphore_wait(barrier, len(devices))

    def nearest(self, k):
        z, n = self.z, self.n
        low = jnp.minimum(z, n - 1 - z)
        sign = 1 if k % 2 == 0 else -1
        paired = z + sign * ((k + 1) // 2)
        past = jnp.where(2 * z < n - 1, z + (k - low), z - (k - low))
        return jnp.where(k <= 2 * low, paired, past)

    def hops(self, k):
        lows = [min(z, self.n - 1 - z) for z in range(self.n)]
        return sorted({(k + 1) // 2 if k <= 2 * low else k - low for low in lows})

    def by_line(self, z, p):
        near = jnp.logical_or(p == z + 1, p == z - 1)
        if self.n >= 4:
            near = jnp.logical_or(near, jnp.logical_and(z == 0, p == 2))
            near = jnp.logical_or(near, jnp.logical_and(z == self.n - 1, p == self.n - 3))
        return near

    def copy(self, src, dst, p, s, r, device):
        return pltpu.make_async_remote_copy(
            src_ref=src,
            dst_ref=dst,
            send_sem=self.send.at[p, s],
            recv_sem=self.recv.at[p, r],
            device_id=device,
            device_id_type=MESH,
        )

    def start(self, cond, src, dst, p, s, r, device):
        copy = self.copy(src, dst, p, s, r, device)
        if cond is None:
            copy.start()
        else:
            pl.when(cond)(copy.start)
        self.pending.append((cond, copy))

    def arrive(self, ref, p, r, now=None):
        copy = self.copy(ref, ref, p, 0, r, self.x_dev)
        if now is None:
            copy.wait_recv()
        else:
            pl.when(now)(copy.wait_recv)

    def column(self, k, halves=(0, 1), now=None):
        p = self.order[k]
        up = jnp.logical_and(p <= self.z, self.z < self.n - 1)
        down = jnp.logical_and(p >= self.z, self.z > 0)
        if now is not None:
            up, down = jnp.logical_and(now, up), jnp.logical_and(now, down)
        for h in halves:
            ref = self.piece(p, self.f, h)
            if k > 0:
                self.arrive(ref, p, h, now)
            self.start(now, ref, ref, p, 4 + h, 2 + h, self.x_dev)
            self.start(now, ref, ref, p, 6 + h, 4 + h, self.y_dev)
            self.start(up, ref, ref, p, h, h, self.up_dev)
            self.start(down, ref, ref, p, 2 + h, h, self.down_dev)

    def columns(self, distance, halves=(0, 1)):
        for k in range(1, self.n):
            hops = self.hops(k)
            if hops == [distance]:
                self.column(k, halves)
            elif distance in hops:
                away = self.order[k] - self.z
                now = jnp.logical_or(away == distance, away == -distance)
                self.column(k, halves, now)

    def sides(self, k, halves=(0, 1)):
        p = self.order[k]
        relay = jnp.logical_not(self.by_line(self.z, p))
        for h in halves:
            x_part = self.piece(p, self.fx, h)
            y_part = self.piece(p, self.fy, h)
            self.arrive(x_part, p, 2 + h)
            if h == 0:
                self.start(relay, x_part, x_part, p, 8, 6, self.y_dev)
            self.arrive(y_part, p, 4 + h)
            if h == 1:
                self.start(relay, y_part, y_part, p, 9, 7, self.x_dev)

    def diagonal(self, k, now=None):
        p = self.order[k]
        z, n = self.z, self.n
        up = jnp.logical_and(jnp.logical_and(p <= z, z < n - 1), self.by_line(z + 1, p))
        down = jnp.logical_and(jnp.logical_and(p >= z, z > 0), self.by_line(z - 1, p))
        if now is not None:
            up, down = jnp.logical_and(now, up), jnp.logical_and(now, down)
        for h in range(2):
            part = self.piece(p, self.fd, h)
            self.arrive(part, p, 6 + h, now)
            self.start(up, part, part, p, 10 + h, 6 + h, self.up_dev)
            self.start(down, part, part, p, 12 + h, 6 + h, self.down_dev)

    def diagonals(self, distance):
        for k in range(self.n):
            hops = self.hops(k)
            if hops == [distance]:
                self.diagonal(k)
            elif distance in hops:
                away = self.order[k] - self.z
                self.diagonal(k, jnp.logical_or(away == distance, away == -distance))

    def stage(self, i):
        if i < self.n:
            self.sides(i)
        if i + 1 < self.n:
            self.columns(i + 1)
        if i > 0:
            self.diagonals(i - 1)
            return [self.order[i - 1]]
        return []

    def drain(self):
        for cond, copy in self.pending:
            if cond is None:
                copy.wait_send()
            else:
                pl.when(cond)(copy.wait_send)


def layer_kernel(
    gate_ref,
    value_ref,
    key_ref,
    query_ref,
    pool_ref,
    t_ref,
    w_ssd_ref,
    w_pool_ref,
    norm_ref,
    step_ref,
    scale_ref,
    shift_ref,
    conv_value_ref,
    conv_key_ref,
    conv_query_ref,
    gain_ref,
    pool_mix_ref,
    pool_gain_ref,
    kept_ref,
    got,
    mixed_in,
    others_in,
    w_out,
    toks,
    acc,
    gate,
    rows_ref,
    cols_ref,
    total_ref,
    taps,
    pad,
    act,
    y,
    ends,
    prior,
    finals,
    arrived,
    incoming,
    totals,
    squares,
    mixed,
    away,
    w_send,
    w_recv,
    local_sem,
    pair_sem,
    halo_sem,
    total_sem,
    state_sem,
    square_sem,
    part_sem,
):
    length = toks.shape[0] - 2 * EDGE
    mine = t_ref.shape[0]
    half = length // 2
    groups = cols_ref.shape[0]
    lines = total_ref.shape[0]
    blocks = length // SPAN
    width = groups * STATE
    z = lax.axis_index("sp")
    f = lax.axis_index("fs")
    c = lax.axis_index("tp")
    n = lax.axis_size("sp")
    tile = (SPAN, 2 * HEAD_DIM)
    square = (SPAN, SPAN)
    f32 = jnp.float32
    across = (((1,), (1,)), ((), ()))

    rows = value_ref.shape[0]

    def rows_of(buf):
        def piece(p, member, h):
            at = pl.multiple_of(member * rows + h * (rows // 2), rows // 2)
            return buf.at[p, pl.ds(at, rows // 2)]

        return piece

    own_block = pl.ds(pl.multiple_of(f * rows, rows), rows)

    def columns_of(p, member, h):
        lot, cols = w_ssd_ref.shape
        at = pl.ds(pl.multiple_of((p * 4 + member) * cols, cols), cols)
        return w_out.at[pl.ds(h * lot, lot), at]

    first = LineGather(rows_of(mixed_in), w_send.at[0], w_recv.at[0])
    second = LineGather(rows_of(others_in), w_send.at[1], w_recv.at[1])
    third = LineGather(columns_of, w_send.at[2], w_recv.at[2])
    partner = (z, f, 1 - c)
    ahead = [(lax.rem(z + d, n), f, c) for d in range(n)]
    behind = [(lax.rem(z + n - d, n), f, c) for d in range(n)]

    def local(src, dst, i):
        copy = pltpu.make_async_copy(src, dst, local_sem.at[i])
        copy.start()
        return copy

    own_rows = toks.at[pl.ds(pl.multiple_of(EDGE + c * mine, EDGE), mine)]
    own_first = [
        local(ref, mixed_in.at[z, own_block, pl.ds(i * width, width)], i)
        for i, ref in enumerate((value_ref, key_ref, query_ref))
    ]
    own_tokens = local(t_ref, own_rows, 3)
    own_second = [
        local(ref, others_in.at[z, own_block, pl.ds(i * width, width)], 4 + i)
        for i, ref in enumerate((gate_ref, pool_ref))
    ]
    own_third = [
        local(ref, columns_of(z, f, h), 6 + h) for h, ref in enumerate((w_ssd_ref, w_pool_ref))
    ]
    first.barrier((partner, *ahead[2 : n - 1]))
    pending = []

    def remote(src, dst, sems, index, device, cond=None):
        copy = pltpu.make_async_remote_copy(
            src_ref=src,
            dst_ref=dst,
            send_sem=sems.at[(0, *index)],
            recv_sem=sems.at[(1, *index)],
            device_id=device,
            device_id_type=MESH,
        )
        if cond is None:
            copy.start()
        else:
            pl.when(cond)(copy.start)
        pending.append((cond, copy))
        return copy

    for copy in own_first:
        copy.wait()
    first.column(0)
    own_tokens.wait()
    pair = remote(t_ref, own_rows, pair_sem, (), partner)
    for copy in own_second + own_third:
        copy.wait()
    chunk = 32

    def normalize(start):
        def body(i, carry):
            at = pl.ds(pl.multiple_of(EDGE + start + i * chunk, EDGE), chunk)
            wide = toks[at, :].astype(jnp.float32)
            mean = jnp.mean(wide * wide, axis=-1, keepdims=True)
            toks[at, :] = (wide * lax.rsqrt(mean + EPSILON) * norm_ref[...]).astype(jnp.bfloat16)
            return carry

        lax.fori_loop(0, mine // chunk, body, 0)

    normalize(c * mine)
    pair.wait_recv()
    normalize((1 - c) * mine)
    below, above = z > 0, z < n - 1
    from_below = remote(
        toks.at[pl.ds(length, EDGE)], toks.at[pl.ds(0, EDGE)], halo_sem, (0,), ahead[1], above
    )
    from_above = remote(
        toks.at[pl.ds(EDGE, EDGE)],
        toks.at[pl.ds(EDGE + length, EDGE)],
        halo_sem,
        (1,),
        behind[1],
        below,
    )

    @pl.when(jnp.logical_not(below))
    def _():
        toks[:EDGE, :] = jnp.zeros((EDGE, toks.shape[1]), toks.dtype)

    @pl.when(jnp.logical_not(above))
    def _():
        toks[EDGE + length :, :] = jnp.zeros((EDGE, toks.shape[1]), toks.dtype)


    def lanes(i, count=1):
        return pl.ds(pl.multiple_of(i * STATE, STATE), count * STATE)

    def span(i):
        return pl.ds(pl.multiple_of(i * SPAN, SPAN), SPAN)

    def edged(i):
        return pl.ds(pl.multiple_of(EDGE + i * SPAN, EDGE), SPAN)

    def multiply(buf, p, begin=False, store=None):
        depth = buf.shape[1]
        at = pl.ds(pl.multiple_of(p * depth, depth), depth)
        wide = 256

        def body(i, carry):
            cols = pl.ds(pl.multiple_of(i * wide, wide), wide)
            for m in range(2):
                lot = half + EDGE
                part = jnp.dot(
                    toks[m * lot : (m + 1) * lot, at],
                    buf[p, :, cols],
                    preferred_element_type=f32,
                )
                if not begin:
                    part = part + acc[m * lot : (m + 1) * lot, cols]
                if store is None:
                    acc[m * lot : (m + 1) * lot, cols] = part
                else:
                    store(m, i, wide, part.astype(jnp.bfloat16))
            return carry

        count = buf.shape[2] // wide
        if store is None:
            lax.fori_loop(0, count, body, 0)
        else:
            for i in range(count):
                body(i, 0)

    def store_first(m, i, wide, part):
        lot = part.shape[0]
        pad[m * lot : (m + 1) * lot, i * wide : (i + 1) * wide] = part.astype(f32)

    def store_second(m, i, wide, part):
        lot = part.shape[0]
        if i * wide < width:
            gate[m * lot : (m + 1) * lot, i * wide : (i + 1) * wide] = part
        else:
            pad[m * lot : (m + 1) * lot, 2 * width + i * wide : 2 * width + (i + 1) * wide] = (
                part.astype(f32)
            )

    def step_sizes():
        raw = lax.dot_general(
            step_ref[...], toks[EDGE : EDGE + length, :], (((1,), (1,)), ((), ())), preferred_element_type=jnp.float32
        )
        raw = raw + scale_ref[:, :1]
        shift = jnp.concatenate([shift_ref[0, h] for h in range(shift_ref.shape[1])], axis=0)
        steps = jnp.maximum(raw, 0.0) + jnp.log1p(jnp.exp(-jnp.abs(raw)))
        logs = -scale_ref[:, SPAN : SPAN + 1] * steps - shift
        cut = [slice(i * SPAN, (i + 1) * SPAN) for i in range(blocks)]
        steps = jnp.concatenate([steps[:, at] for at in cut], axis=0)
        logs = jnp.concatenate([logs[:, at] for at in cut], axis=0)
        square = (SPAN, SPAN)
        upper = lax.broadcasted_iota(jnp.int32, square, 0) <= lax.broadcasted_iota(
            jnp.int32, square, 1
        )
        inner = jnp.dot(
            logs, upper.astype(jnp.float32), precision=HIGHEST, preferred_element_type=jnp.float32
        )
        total = inner[:, SPAN - 1 :]
        backward = lax.rem(lax.broadcasted_iota(jnp.int32, logs.shape, 0), 2) == 1
        along = inner - jnp.where(backward, logs, 0.0)
        weight = jnp.exp(jnp.where(backward, along, total - along)) * steps
        reach = jnp.exp(jnp.where(backward, total - along, along))
        rows_ref[0] = along
        rows_ref[1] = steps
        rows_ref[2] = jnp.broadcast_to(jnp.exp(total), logs.shape)
        whole = total[:lines]
        for i in range(1, blocks):
            whole = whole + total[i * lines : (i + 1) * lines]
        total_ref[...] = jnp.broadcast_to(whole, total_ref.shape)
        turned = [jnp.transpose(v) for v in (along, weight, reach)]
        for g in range(lines // 4):
            for i in range(blocks):
                for j in range(3):
                    at = i * lines + 4 * g
                    cols_ref[g, cut[i], 4 * j : 4 * j + 4] = turned[j][:, at : at + 4]

    order = first.order
    step_sizes()
    for i, ref in enumerate((conv_value_ref, conv_key_ref, conv_query_ref)):
        taps[:CONV_WIDTH, i * width : (i + 1) * width] = ref[
            :, pl.ds(pl.multiple_of(c * width, width), width)
        ].astype(f32)
    pl.when(below)(from_below.wait_recv)
    pl.when(above)(from_above.wait_recv)
    multiplied = []

    def advance_first(count):
        for _ in range(count):
            multiplied.append(order[len(multiplied)])
            multiply(
                mixed_in,
                multiplied[-1],
                begin=len(multiplied) == 1,
                store=store_first if len(multiplied) == n else None,
            )

    reached = 0
    for k in range(1, n + 1):
        for h in range(2):
            first.sides(k - 1, (h,))
            first.columns(k, (h,))
        if k == n:
            second.column(0)
        due = 1 if k == 1 else 2 if k == 3 else n if k == n else reached
        while reached < due:
            first.diagonals(reached)
            reached += 1
            advance_first(1)

    sums = [
        remote(total_ref, totals.at[z], total_sem, (d - 1,), ahead[d]) for d in range(1, n)
    ]
    margin = CONV_WIDTH // 2

    def convolve(i, carry):
        at = lanes(i)
        tap = taps[:, at]
        for b in range(blocks):
            begin = EDGE - margin + b * SPAN
            total = pad[begin : begin + SPAN, at] * tap[:1]
            for o in range(1, CONV_WIDTH):
                total = total + pad[begin + o : begin + o + SPAN, at] * tap[o : o + 1]
            act[b * SPAN : (b + 1) * SPAN, at] = jax.nn.silu(total).astype(jnp.bfloat16)
        return carry

    lax.fori_loop(0, 2 * groups, convolve, 0)
    queue = second.stage(0)
    step = 4 if blocks % 4 == 0 else 1
    parts = blocks // step

    def block_ends(i, carry):
        g = i // parts
        for u in range(step):
            b = lax.rem(i, parts) * step + u
            at = span(b)
            x = act[at, lanes(g)].astype(f32)
            k = act[at, lanes(groups + g)]
            for r in range(2):
                weight = split_heads(
                    cols_ref[g, at, 4 + r : 5 + r], cols_ref[g, at, 6 + r : 7 + r], 1, tile
                )
                ends[g, r, b] = lax.dot_general(
                    (x * weight).astype(jnp.bfloat16),
                    k,
                    (((0,), (0,)), ((), ())),
                    preferred_element_type=f32,
                )
        return carry

    lax.fori_loop(0, groups * parts, block_ends, 0)

    def scan(g, r, start, each):
        order = range(blocks) if r == 0 else range(blocks - 1, -1, -1)
        carried = list(start)
        for b in order:
            each(b, carried)
            for h in range(2):
                at = b * lines + 4 * g + 2 * h + r
                scale = rows_ref[2, pl.ds(at, 1), :]
                carried[h] = carried[h] * scale + ends[g, r, b, h * HEAD_DIM : (h + 1) * HEAD_DIM]
        return carried

    def own_states(g, carry):
        zero = jnp.zeros((HEAD_DIM, STATE), f32)
        for r in range(2):
            last = scan(g, r, [zero, zero], lambda b, carried: None)
            for h in range(2):
                finals[r, g, h * HEAD_DIM : (h + 1) * HEAD_DIM] = last[h].astype(jnp.bfloat16)
        return carry

    lax.fori_loop(0, groups, own_states, 0)
    states = []
    for d in range(1, n):
        states.append(
            (
                remote(finals.at[0], arrived.at[0, d - 1], state_sem, (0, d - 1), ahead[d], z + d < n),
                remote(finals.at[1], arrived.at[1, d - 1], state_sem, (1, d - 1), behind[d], z >= d),
            )
        )
    queue += second.stage(1)
    lax.fori_loop(2 * groups, 3 * groups, convolve, 0)
    if n >= 3:
        queue += second.stage(2)
    third.column(0)
    taken = [0]

    def advance():
        while queue:
            p = queue.pop(0)
            taken[0] += 1
            multiply(
                others_in,
                p,
                begin=taken[0] == 1,
                store=store_second if taken[0] == n else None,
            )

    advance()
    later = lax.broadcasted_iota(jnp.int32, square, 0)
    sooner = lax.broadcasted_iota(jnp.int32, square, 1)

    def diagonal_blocks(i, carry):
        g = i // parts
        lower = later >= sooner
        equal = later == sooner
        for u in range(step):
            b = lax.rem(i, parts) * step + u
            at = span(b)
            x = act[at, lanes(g)]
            scores = lax.dot_general(
                act[at, lanes(2 * groups + g)],
                act[at, lanes(groups + g)],
                across,
                preferred_element_type=f32,
            )
            outs = []
            for h in range(2):
                line = b * lines + 4 * g + 2 * h
                cf_l = cols_ref[g, at, 2 * h : 2 * h + 1]
                eb_l = cols_ref[g, at, 2 * h + 1 : 2 * h + 2]
                cf_s = rows_ref[0, pl.ds(line, 1), :]
                eb_s = rows_ref[0, pl.ds(line + 1, 1), :]
                df_s = rows_ref[1, pl.ds(line, 1), :]
                db_s = rows_ref[1, pl.ds(line + 1, 1), :]
                decay = jnp.exp(jnp.where(lower, cf_l - cf_s, eb_s - eb_l))
                size = jnp.where(equal, df_s + db_s, jnp.where(lower, df_s, db_s))
                outs.append(
                    jnp.dot(
                        (scores * decay * size).astype(jnp.bfloat16), x, preferred_element_type=f32
                    )
                )
            y[at, lanes(g)] = split_heads(outs[0], outs[1], 1, tile)
        return carry

    count = groups * parts
    lax.fori_loop(0, count // 2, diagonal_blocks, 0)
    if n >= 4:
        queue += second.stage(3)
    third.stage(0)
    lax.fori_loop(count // 2, count, diagonal_blocks, 0)
    queue += second.stage(n)
    advance()
    third.stage(1)

    def pooled(i, carry):
        where_global = (
            z * length + i * SPAN + lax.broadcasted_iota(jnp.int32, (SPAN, POOL_DIM), 0)
        )
        for j in range(groups):
            window = WINDOWS[j % 4]
            at = slice(3 * width + j * POOL_DIM, 3 * width + (j + 1) * POOL_DIM)
            block = pad[pl.ds(pl.multiple_of(i * SPAN, SPAN), SPAN + 2 * EDGE), at]
            first = EDGE - window // 2
            running = block[first : first + SPAN]
            for o in range(1, window):
                running = running + block[first + o : first + o + SPAN]
            lower = jnp.maximum(where_global - window // 2, 0)
            upper = jnp.minimum(where_global + window - window // 2, n * length)
            mean = running / (upper - lower).astype(f32)
            diff = (mean - block[EDGE : EDGE + SPAN]).astype(jnp.bfloat16)
            mapped = jnp.dot(diff, pool_mix_ref[c * groups + j], preferred_element_type=f32)
            gain = pool_gain_ref[:, lanes(c * groups + j)]
            mixed[span(i), width + j * POOL_DIM : width + (j + 1) * POOL_DIM] = (
                mapped * gain
            ).astype(jnp.bfloat16)
        return carry

    lax.fori_loop(0, blocks, pooled, 0)
    if n >= 3:
        third.stage(2)
    incoming[...] = jnp.zeros(incoming.shape, f32)
    for copy in sums:
        copy.wait_recv()
    for d in range(1, n):
        for r in range(2):

            def receive(d=d, r=r):
                states[d - 1][r].wait_recv()
                log = jnp.zeros(total_ref.shape, f32)
                for e in range(1, d):
                    log = log + totals[z - e if r == 0 else z + e]
                scale = jnp.exp(log)
                for g in range(groups):
                    for h in range(2):
                        line = 4 * g + 2 * h + r
                        at = slice(h * HEAD_DIM, (h + 1) * HEAD_DIM)
                        incoming[g, r, at] = incoming[g, r, at] + scale[
                            line : line + 1
                        ] * arrived[r, d - 1, g, at].astype(f32)

            pl.when(z >= d if r == 0 else z + d < n)(receive)
    squares[0] = jnp.zeros(squares.shape[1:], f32)

    def outputs(g, carry):
        for r in range(2):

            def keep(b, carried, r=r):
                for h in range(2):
                    prior[b, r * STATE + h * HEAD_DIM : r * STATE + (h + 1) * HEAD_DIM] = carried[
                        h
                    ].astype(jnp.bfloat16)

            scan(g, r, [incoming[g, r, :HEAD_DIM], incoming[g, r, HEAD_DIM:]], keep)
        for b in range(blocks):
            at = span(b)
            far = lax.dot_general(
                act[at, lanes(2 * groups + g)], prior[b], across, preferred_element_type=f32
            )
            out = y[at, lanes(g)]
            for r in range(2):
                reach = split_heads(
                    cols_ref[g, at, 8 + r : 9 + r], cols_ref[g, at, 10 + r : 11 + r], 1, tile
                )
                out = out + reach * far[:, r * STATE : (r + 1) * STATE]
            out = out * jax.nn.silu(gate[edged(b), lanes(g)].astype(f32))
            y[at, lanes(g)] = out
            squares[0, at] = squares[0, at] + jnp.sum(out * out, axis=-1, keepdims=True)
        return carry

    lax.fori_loop(0, groups, outputs, 0)
    other = remote(squares.at[0], squares.at[1], square_sem, (), partner)
    if n >= 4:
        third.stage(3)
    other.wait_recv()

    def scale_rows(b, carry):
        at = span(b)
        scale = lax.rsqrt((squares[0, at] + squares[1, at]) / (2 * width) + EPSILON)
        for g in range(groups):
            mixed[at, g * STATE : (g + 1) * STATE] = (
                y[at, g * STATE : (g + 1) * STATE] * scale * gain_ref[:, lanes(c * groups + g)]
            ).astype(jnp.bfloat16)
        return carry

    lax.fori_loop(0, blocks, scale_rows, 0)
    part = kept_ref.shape[1] // n
    wide = part // 2

    def product(head, target, p):
        for i in range(2):
            at = pl.ds(pl.multiple_of(p * part + i * wide, wide), wide)
            target[:, at] = jnp.dot(
                mixed[pl.ds(pl.multiple_of(head, half), half), :],
                w_out[:, at],
                preferred_element_type=f32,
            ).astype(jnp.bfloat16)

    sent = []
    for k in range(n):
        if k == n - 1:
            third.stage(n)
        p = third.order[k]
        product((1 - c) * half, away, p)
        ref = pl.ds(pl.multiple_of(p * part, part), part)
        sent.append(remote(away.at[:, ref], got.at[:, ref], part_sem, (k,), partner))
        if k > 0:
            product(c * half, kept_ref, third.order[k - 1])
    product(c * half, kept_ref, third.order[n - 1])
    for copy in sent:
        copy.wait_recv()
    for cond, copy in pending:
        if cond is None:
            copy.wait_send()
        else:
            pl.when(cond)(copy.wait_send)
    for gather in (first, second, third):
        gather.drain()


def fused_layer(weights, tokens, w_ssd, w_pool, small, groups):
    n = lax.axis_size("sp")
    half, features = tokens.shape
    length = 2 * half
    width = groups * STATE
    lines = 4 * groups
    blocks = length // SPAN
    rows = weights[0].shape[0]
    out_rows, out_cols = 2 * w_ssd.shape[0], 4 * n * w_ssd.shape[1]
    anywhere = pl.BlockSpec(memory_space=pl.ANY)
    inside = pl.BlockSpec(memory_space=pltpu.VMEM)
    bf16, f32 = jnp.bfloat16, jnp.float32
    dma = pltpu.SemaphoreType.DMA
    return pl.pallas_call(
        layer_kernel,
        out_shape=[jax.ShapeDtypeStruct((half, out_cols), bf16)] * 2,
        in_specs=[anywhere] * 8 + [inside] * len(small),
        out_specs=[inside] * 2,
        scratch_shapes=[
            pltpu.VMEM((n, 4 * rows, 3 * width), bf16),
            pltpu.VMEM((n, 4 * rows, 2 * width), bf16),
            pltpu.VMEM((out_rows, out_cols), bf16),
            pltpu.VMEM((length + 2 * EDGE, features), bf16),
            pltpu.VMEM((length + 2 * EDGE, 3 * width), f32),
            pltpu.VMEM((length + 2 * EDGE, width), bf16),
            pltpu.VMEM((3, lines * blocks, SPAN), f32),
            pltpu.VMEM((groups, length, 12), f32),
            pltpu.VMEM((lines, SPAN), f32),
            pltpu.VMEM((8, 3 * width), f32),
            pltpu.VMEM((length + 2 * EDGE, 4 * width), f32),
            pltpu.VMEM((length, 3 * width), bf16),
            pltpu.VMEM((length, width), f32),
            pltpu.VMEM((groups, 2, blocks, STATE, STATE), f32),
            pltpu.VMEM((blocks, 2 * STATE, STATE), bf16),
            pltpu.VMEM((2, groups, STATE, STATE), bf16),
            pltpu.VMEM((2, n - 1, groups, STATE, STATE), bf16),
            pltpu.VMEM((groups, 2, STATE, STATE), f32),
            pltpu.VMEM((n, lines, SPAN), f32),
            pltpu.VMEM((2, length, SPAN), f32),
            pltpu.VMEM((length, 2 * width), bf16),
            pltpu.VMEM((half, out_cols), bf16),
            dma((3, n, 14)),
            dma((3, n, 8)),
            dma((8,)),
            dma((2,)),
            dma((2, 2)),
            dma((2, n - 1)),
            dma((2, 2, n - 1)),
            dma((2,)),
            dma((2, n)),
        ],
        compiler_params=pltpu.CompilerParams(
            collective_id=0, has_side_effects=True, vmem_limit_bytes=VMEM_LIMIT
        ),
        name="mixer",
    )(*weights, tokens, w_ssd, w_pool, *small)


def split_heads(first, second, axis, shape):
    places = lax.broadcasted_iota(jnp.int32, shape, axis)
    return jnp.where(places < HEAD_DIM, first, second)


def ends_kernel(blocks, decay_ref, x_ref, k_ref, col_ref, ends_ref, final_ref):
    group = pl.program_id(0)
    tile = (SPAN, 2 * HEAD_DIM)
    for c in range(blocks):
        rows = pl.ds(c * SPAN, SPAN)
        x = x_ref[rows, :].astype(jnp.float32)
        k = k_ref[rows, :]
        for r in range(2):
            weight = split_heads(
                col_ref[0, rows, 4 + 2 * r : 5 + 2 * r],
                col_ref[0, rows, 5 + 2 * r : 6 + 2 * r],
                1,
                tile,
            )
            end = lax.dot_general(
                (x * weight).astype(jnp.bfloat16),
                k,
                (((0,), (0,)), ((), ())),
                preferred_element_type=jnp.float32,
            )
            ends_ref[0, r, c] = end
    states = (2 * HEAD_DIM, STATE)
    for r in range(2):
        total = jnp.zeros(states, jnp.float32)
        for c in range(blocks) if r == 0 else range(blocks - 1, -1, -1):
            at = ((group * blocks + c) * 2 + r) * 2
            scale = split_heads(decay_ref[at], decay_ref[at + 1], 0, states)
            total = total * scale + ends_ref[0, r, c]
        final_ref[0, r] = total


def outputs_kernel(
    blocks, decay_ref, x_ref, k_ref, q_ref, col_ref, row_ref, ends_ref, in_ref, y_ref, prior
):
    group = pl.program_id(0)
    states = (2 * HEAD_DIM, STATE)
    tile = (SPAN, 2 * HEAD_DIM)
    square = (SPAN, SPAN)
    for r in range(2):
        total = in_ref[0, r]
        for c in range(blocks) if r == 0 else range(blocks - 1, -1, -1):
            prior[r, c] = total.astype(jnp.bfloat16)
            at = ((group * blocks + c) * 2 + r) * 2
            scale = split_heads(decay_ref[at], decay_ref[at + 1], 0, states)
            total = total * scale + ends_ref[0, r, c]
    later = lax.broadcasted_iota(jnp.int32, square, 0)
    sooner = lax.broadcasted_iota(jnp.int32, square, 1)
    lower = later >= sooner
    equal = later == sooner
    across = (((1,), (1,)), ((), ()))
    for c in range(blocks):
        rows = pl.ds(c * SPAN, SPAN)
        x = x_ref[rows, :]
        q = q_ref[rows, :]
        scores = lax.dot_general(q, k_ref[rows, :], across, preferred_element_type=jnp.float32)
        parts = []
        for h in range(2):
            cf_l = col_ref[0, rows, 2 * h : 2 * h + 1]
            eb_l = col_ref[0, rows, 2 * h + 1 : 2 * h + 2]
            cf_s = row_ref[0, 4 * h : 4 * h + 1, rows]
            eb_s = row_ref[0, 4 * h + 1 : 4 * h + 2, rows]
            df_s = row_ref[0, 4 * h + 2 : 4 * h + 3, rows]
            db_s = row_ref[0, 4 * h + 3 : 4 * h + 4, rows]
            decay = jnp.exp(jnp.where(lower, cf_l - cf_s, eb_s - eb_l))
            step = jnp.where(equal, df_s + db_s, jnp.where(lower, df_s, db_s))
            parts.append(
                jnp.dot(
                    (scores * decay * step).astype(jnp.bfloat16),
                    x,
                    preferred_element_type=jnp.float32,
                )
            )
        out = split_heads(parts[0], parts[1], 1, tile)
        for r in range(2):
            reach = split_heads(
                col_ref[0, rows, 8 + 2 * r : 9 + 2 * r],
                col_ref[0, rows, 9 + 2 * r : 10 + 2 * r],
                1,
                tile,
            )
            out = out + reach * lax.dot_general(
                q, prior[r, c], across, preferred_element_type=jnp.float32
            )
        y_ref[rows, :] = out


def mixer(activated, width_ssd, width_key, steps, logs, sp_rank):
    length = activated.shape[0]
    heads = steps.shape[1]
    groups = width_key // STATE
    blocks = length // SPAN
    shaped = logs.reshape(2, heads, blocks, SPAN)
    ones = jnp.triu(jnp.ones((SPAN, SPAN), jnp.float32))
    inner = jnp.einsum("rhcs,sl->rhcl", shaped, ones, precision=HIGHEST)
    totals = inner[..., -1:]
    cf = inner[0]
    eb = inner[1] - shaped[1]
    wf = jnp.exp(totals[0] - cf) * steps[0].reshape(cf.shape)
    wb = jnp.exp(eb) * steps[1].reshape(cf.shape)
    reach_f = jnp.exp(cf)
    reach_b = jnp.exp(totals[1] - eb)

    def pair(a):
        return a.reshape(groups, 2, length)

    cf, eb, wf, wb, reach_f, reach_b = map(pair, (cf, eb, wf, wb, reach_f, reach_b))
    df, db = (pair(steps[0]), pair(steps[1]))
    packed = jnp.stack(
        [cf[:, 0], eb[:, 0], cf[:, 1], eb[:, 1]]
        + [wf[:, 0], wf[:, 1], wb[:, 0], wb[:, 1]]
        + [reach_f[:, 0], reach_f[:, 1], reach_b[:, 0], reach_b[:, 1]],
        axis=1,
    )
    cols = jnp.transpose(packed, (0, 2, 1))
    rows = jnp.stack(
        [cf[:, 0], eb[:, 0], df[:, 0], db[:, 0], cf[:, 1], eb[:, 1], df[:, 1], db[:, 1]], axis=1
    )
    block_logs = totals[..., 0]
    decays = jnp.exp(block_logs).reshape(2, groups, 2, blocks)
    decays = jnp.transpose(decays, (1, 3, 0, 2)).reshape(-1)
    smem = pl.BlockSpec(memory_space=pltpu.SMEM)
    x_blocks = width_ssd // STATE

    def wide(offset):
        return pl.BlockSpec((length, STATE), lambda g: (0, g + offset))

    col_spec = pl.BlockSpec((1, length, cols.shape[2]), lambda g: (g, 0, 0))
    ends_spec = pl.BlockSpec((1, 2, blocks, STATE, STATE), lambda g: (g, 0, 0, 0, 0))
    state_spec = pl.BlockSpec((1, 2, STATE, STATE), lambda g: (g, 0, 0, 0))
    ends, finals = pl.pallas_call(
        functools.partial(ends_kernel, blocks),
        grid=(groups,),
        out_shape=(
            jax.ShapeDtypeStruct((groups, 2, blocks, STATE, STATE), jnp.float32),
            jax.ShapeDtypeStruct((groups, 2, STATE, STATE), jnp.float32),
        ),
        in_specs=[smem, wide(0), wide(x_blocks), col_spec],
        out_specs=(ends_spec, state_spec),
        cost_estimate=pl.CostEstimate(
            flops=4 * length * groups * STATE * STATE,
            bytes_accessed=16 * length * groups * STATE,
            transcendentals=0,
        ),
        name="block_ends",
    )(decays, activated, activated, cols)
    device_totals = jnp.sum(block_logs, axis=-1)
    all_totals = lax.all_gather(
        device_totals[None].astype(jnp.bfloat16), "sp", axis=0, tiled=True
    ).astype(jnp.float32)
    states = jnp.transpose(finals, (1, 0, 2, 3)).reshape(2, heads, HEAD_DIM, STATE)
    forward_in, backward_in = prefix_states(all_totals, states.astype(jnp.bfloat16), sp_rank)
    incoming = jnp.stack([forward_in, backward_in]).reshape(2, groups, STATE, STATE)
    incoming = jnp.transpose(incoming, (1, 0, 2, 3))
    return pl.pallas_call(
        functools.partial(outputs_kernel, blocks),
        grid=(groups,),
        out_shape=jax.ShapeDtypeStruct((length, groups * STATE), jnp.float32),
        in_specs=[
            smem,
            wide(0),
            wide(x_blocks),
            wide(x_blocks + groups),
            col_spec,
            pl.BlockSpec((1, 8, length), lambda g: (g, 0, 0)),
            ends_spec,
            state_spec,
        ],
        out_specs=wide(0),
        scratch_shapes=[pltpu.VMEM((2, blocks, STATE, STATE), jnp.bfloat16)],
        cost_estimate=pl.CostEstimate(
            flops=10 * length * groups * STATE * STATE,
            bytes_accessed=40 * length * groups * STATE,
            transcendentals=2 * length * groups * SPAN,
        ),
        name="block_outputs",
    )(decays, activated, activated, activated, cols, rows, ends, incoming)


def prefix_states(all_totals, finals, rank):
    chain_length = all_totals.shape[0]
    device_ids = jnp.arange(chain_length, dtype=jnp.int32)[:, None]
    forward_cum = jnp.cumsum(all_totals[:, 0], axis=0)
    forward_mine = lax.dynamic_slice_in_dim(forward_cum - all_totals[:, 0], rank, 1, 0)
    forward_weight = jnp.exp(jnp.where(device_ids < rank, forward_mine - forward_cum, -jnp.inf))
    backward_cum = jnp.cumsum(all_totals[:, 1], axis=0)
    backward_mine = lax.dynamic_slice_in_dim(backward_cum, rank, 1, 0)
    backward_weight = jnp.exp(
        jnp.where(device_ids > rank, backward_cum - all_totals[:, 1] - backward_mine, -jnp.inf)
    )
    forward_in = jnp.zeros(finals.shape[1:], jnp.float32)
    backward_in = jnp.zeros(finals.shape[1:], jnp.float32)
    for d in range(1, chain_length):
        ahead = [(i, i + d) for i in range(chain_length - d)]
        back = [(i + d, i) for i in range(chain_length - d)]
        from_left = lax.ppermute(finals[0], "sp", ahead).astype(jnp.float32)
        from_right = lax.ppermute(finals[1], "sp", back).astype(jnp.float32)
        left = lax.dynamic_index_in_dim(forward_weight, jnp.maximum(rank - d, 0), 0, False)
        right = lax.dynamic_index_in_dim(
            backward_weight, jnp.minimum(rank + d, chain_length - 1), 0, False
        )
        forward_in = forward_in + left[:, None, None] * from_left
        backward_in = backward_in + right[:, None, None] * from_right
    return (forward_in, backward_in)


def local(
    tokens,
    norm_gain,
    w_gate,
    w_value,
    w_bkey,
    w_query,
    w_pool_in,
    w_step,
    step_bias,
    decay_rate,
    decay_shift,
    conv_value,
    conv_bkey,
    conv_query,
    mix_gain,
    pool_mix,
    pool_gain,
    w_out_ssd,
    w_out_pool,
):
    tp_count = lax.axis_size("tp")
    sp_count = lax.axis_size("sp")
    tp_rank = lax.axis_index("tp")
    sp_rank = lax.axis_index("sp")
    heads_dev = DUALITY_HEADS // tp_count
    groups_dev = GROUPS // tp_count
    pools_dev = POOL_GROUPS // tp_count
    width_ssd = heads_dev * HEAD_DIM
    width_key = groups_dev * STATE
    width_pool = pools_dev * POOL_DIM
    fast = (
        tp_count == 2
        and lax.axis_size("fs") == 4
        and 2 <= sp_count <= 4
        and w_gate.shape[0] % 128 == 0
        and w_out_ssd.shape[1] % 128 == 0
        and pools_dev == groups_dev
        and width_ssd == width_key
        and groups_dev % 4 == 0
        and 2 * tokens.shape[1] * 2 * heads_dev % (SPAN * SPAN) == 0
    )
    step_cols = lax.dynamic_slice_in_dim(w_step, tp_rank * heads_dev, heads_dev, 2)
    bias_dev = lax.dynamic_slice_in_dim(step_bias, tp_rank * heads_dev, heads_dev, 1)
    rate_dev = lax.dynamic_slice_in_dim(decay_rate, tp_rank * heads_dev, heads_dev, 1)
    if fast:
        lines = 2 * heads_dev
        scales = jnp.stack([bias_dev, rate_dev], axis=-1)
        scales = jnp.transpose(scales, (1, 0, 2)).reshape(lines, 2, 1)
        small = (
            norm_gain[None],
            jnp.transpose(step_cols, (2, 1, 0)).reshape(lines, -1),
            jnp.broadcast_to(scales, (lines, 2, SPAN)).reshape(lines, 2 * SPAN),
            decay_shift,
            conv_value,
            conv_bkey,
            conv_query,
            mix_gain[None],
            pool_mix,
            pool_gain[None],
        )
        kept, got = fused_layer(
            (w_gate, w_value, w_bkey, w_query, w_pool_in),
            tokens[0],
            w_out_ssd,
            w_out_pool,
            small,
            groups_dev,
        )
        return (kept.astype(jnp.float32) + got.astype(jnp.float32)).astype(jnp.bfloat16)[None]
    step_cols = step_cols.reshape(w_step.shape[0], 2 * heads_dev)
    weights = jnp.concatenate([w_gate, w_value, w_bkey, w_query, w_pool_in], axis=1)
    combined, widened = gather_inputs(weights, tokens[0])
    out_rows = lax.all_gather(
        jnp.concatenate([w_out_ssd, w_out_pool], axis=0), ("sp", "fs"), axis=1, tiled=True
    )
    widened = widened.astype(jnp.float32)
    scaling = lax.rsqrt(jnp.mean(widened * widened, axis=-1, keepdims=True) + EPSILON)
    normed = (widened * scaling * norm_gain).astype(jnp.bfloat16)
    stored = jnp.dot(normed, combined, preferred_element_type=jnp.float32).astype(jnp.bfloat16)
    raw_steps = jnp.dot(normed, step_cols, preferred_element_type=jnp.float32)
    length = stored.shape[0]
    padded = padded_2(stored[:, width_ssd:], (("sp", 0),), REACH)
    conv_cols = width_ssd + 2 * width_key
    taps = jnp.concatenate(
        [
            lax.dynamic_slice_in_dim(conv_value, tp_rank * width_ssd, width_ssd, 1),
            lax.dynamic_slice_in_dim(conv_bkey, tp_rank * width_key, width_key, 1),
            lax.dynamic_slice_in_dim(conv_query, tp_rank * width_key, width_key, 1),
        ],
        axis=1,
    ).astype(jnp.float32)
    margin = CONV_WIDTH // 2
    convolved = jnp.zeros((length, conv_cols), jnp.float32)
    for offset in range(CONV_WIDTH):
        begin = REACH - margin + offset
        convolved = (
            convolved
            + padded[begin : begin + length, :conv_cols].astype(jnp.float32) * taps[offset]
        )
    activated = jax.nn.silu(convolved).astype(jnp.bfloat16)
    steps = jax.nn.softplus(raw_steps.reshape(length, 2, heads_dev) + bias_dev).transpose(1, 2, 0)
    logs = -rate_dev[:, :, None] * steps - decay_shift[0].transpose(1, 0, 2)
    heads_out = mixer(activated, width_ssd, width_key, steps, logs, sp_rank)
    gated = heads_out * jax.nn.silu(stored[:, :width_ssd].astype(jnp.float32))
    squares = lax.psum(jnp.sum(gated * gated, axis=-1), "tp")
    gain_dev = lax.dynamic_slice_in_dim(mix_gain, tp_rank * width_ssd, width_ssd, 0)
    ssd_mix = (gated * lax.rsqrt(squares / D_SSM + EPSILON)[:, None] * gain_dev).astype(
        jnp.bfloat16
    )
    pool_rows = padded[:, conv_cols:].astype(jnp.float32)
    own_rows = pool_rows[REACH : REACH + length]
    where_global = sp_rank * length + jnp.arange(length, dtype=jnp.int32)
    seq_length = length * sp_count
    window_means = []
    for window in WINDOWS:
        running = jnp.zeros((length, width_pool), jnp.float32)
        for offset in range(-(window // 2), window - window // 2):
            running = running + pool_rows[REACH + offset : REACH + offset + length]
        lower = jnp.clip(where_global - window // 2, 0, seq_length)
        upper = jnp.clip(where_global + window - window // 2, 0, seq_length)
        window_means.append(running / (upper - lower).astype(jnp.float32)[:, None])
    stacked = jnp.stack(window_means).reshape(4, length, pools_dev, POOL_DIM)
    group_ids = tp_rank * pools_dev + jnp.arange(pools_dev, dtype=jnp.int32)
    selector = (jnp.arange(4, dtype=jnp.int32)[:, None] == (group_ids % 4)[None, :]).astype(
        jnp.float32
    )
    means = jnp.sum(stacked * selector[:, None, :, None], axis=0)
    differences = (means - own_rows.reshape(length, pools_dev, POOL_DIM)).astype(jnp.bfloat16)
    pool_weights = lax.dynamic_slice_in_dim(pool_mix, tp_rank * pools_dev, pools_dev, 0)
    mapped = jnp.einsum(
        "rgc,gcd->rgd", differences, pool_weights, preferred_element_type=jnp.float32
    )
    pool_gain_dev = lax.dynamic_slice_in_dim(pool_gain, tp_rank * width_pool, width_pool, 0)
    pool_out = (mapped.reshape(length, width_pool) * pool_gain_dev).astype(jnp.bfloat16)
    mixed = jnp.concatenate([ssd_mix, pool_out], axis=1)
    if tp_count == 2:
        part = length // 2
        away = lax.dynamic_slice_in_dim(mixed, (1 - tp_rank) * part, part, 0)
        home = lax.dynamic_slice_in_dim(mixed, tp_rank * part, part, 0)
        sent = jnp.dot(away, out_rows, preferred_element_type=jnp.float32).astype(jnp.bfloat16)
        received = lax.ppermute(sent, "tp", [(0, 1), (1, 0)])
        kept = lax.optimization_barrier(
            jnp.dot(home, out_rows, preferred_element_type=jnp.float32).astype(jnp.bfloat16)
        )
        summed = (kept.astype(jnp.float32) + received.astype(jnp.float32)).astype(jnp.bfloat16)
    else:
        summed = lax.psum_scatter(
            jnp.dot(mixed, out_rows, preferred_element_type=jnp.float32).astype(jnp.bfloat16),
            "tp",
            scatter_dimension=0,
            tiled=True,
        )
    return summed[None]


def solution(mesh):
    return jax.shard_map(
        local,
        mesh=mesh,
        in_specs=(
            P("fs", ("sp", "tp"), None),
            P(),
            P(("sp", "fs"), "tp"),
            P(("sp", "fs"), "tp"),
            P(("sp", "fs"), "tp"),
            P(("sp", "fs"), "tp"),
            P(("sp", "fs"), "tp"),
            P(),
            P(),
            P(),
            P("fs", "tp", None, "sp"),
            P(),
            P(),
            P(),
            P(),
            P(),
            P(),
            P("tp", ("sp", "fs")),
            P("tp", ("sp", "fs")),
        ),
        out_specs=P("fs", ("sp", "tp"), None),
        check_vma=False,
    )
```

```python
import functools

import jax
import jax.numpy as jnp
from jax import lax
from jax.experimental import pallas as pl
from jax.experimental.pallas import tpu as pltpu
from jax.sharding import PartitionSpec as P

HEAD_DIM = 64
DUALITY_HEADS = 16
GROUPS = 8
STATE = 128
CONV_WIDTH = 5
POOL_GROUPS = 8
POOL_DIM = 128
SPAN = 128
REACH = 8
EDGE = 16
VMEM_LIMIT = 63 * 2**20
D_SSM = 1024


EPSILON = 1e-06
HIGHEST = lax.Precision.HIGHEST
WINDOWS = (2, 4, 8, 16)


def padded_2(cells, sides, width):
    for axis, dim in sides:
        count = lax.axis_size(axis)
        ends = count - 1
        head = lax.slice_in_dim(cells, 0, width, axis=dim)
        tail = lax.slice_in_dim(cells, cells.shape[dim] - width, cells.shape[dim], axis=dim)
        cells = jnp.concatenate(
            [
                lax.ppermute(tail, axis, [(i, (i + 1) % count) for i in range(ends)]),
                cells,
                lax.ppermute(head, axis, [((i + 1) % count, i) for i in range(ends)]),
            ],
            axis=dim,
        )
    return cells


MESH = pl.DeviceIdType.MESH


def gather_kernel(n_sp, n_tp, w_ref, t_ref, w_out, t_out, send, recv, local_sem):
    z = lax.axis_index("sp")
    f = lax.axis_index("fs")
    c = lax.axis_index("tp")
    fx = f + 1 - 2 * lax.rem(f, 2)
    fy = lax.rem(f + 2, 4)
    rows = w_ref.shape[0]
    half = rows // 2
    x_dev = (z, fx, c)
    y_dev = (z, fy, c)
    z_devs = [(lax.rem(z + d, n_sp), f, c) for d in range(1, n_sp)]
    t_devs = [(z, f, lax.rem(c + d, n_tp)) for d in range(1, n_tp)]
    partners = [x_dev, y_dev] + z_devs + t_devs
    barrier = pltpu.get_barrier_semaphore()
    for dev in partners:
        pl.semaphore_signal(barrier, inc=1, device_id=dev, device_id_type=MESH)
    pl.semaphore_wait(barrier, len(partners))

    def remote(src, dst, index, dev):
        copy = pltpu.make_async_remote_copy(
            src_ref=src,
            dst_ref=dst,
            send_sem=send.at[index],
            recv_sem=recv.at[index],
            device_id=dev,
            device_id_type=MESH,
        )
        copy.start()
        return copy

    base = n_sp - 1
    z_copies = [remote(w_ref, w_out.at[z, f], d, z_devs[d]) for d in range(n_sp - 1)]
    full = []
    relay = []

    def send_full(d):
        if d == 0:
            src = w_ref
            origin = z
        else:
            z_copies[d - 1].wait_recv()
            origin = lax.rem(z - d + n_sp, n_sp)
            src = w_out.at[origin, f]
        dst = w_out.at[origin, f]
        full.append(
            (
                remote(src, dst, base + 4 * d, x_dev),
                remote(src, dst, base + 4 * d + 1, y_dev),
            )
        )

    def send_relay(d):
        origin = lax.rem(z - d + n_sp, n_sp)
        full[d][0].wait_recv()
        part = w_out.at[origin, fx, pl.ds(0, half)]
        first = remote(part, part, base + 4 * d + 2, y_dev)
        full[d][1].wait_recv()
        part = w_out.at[origin, fy, pl.ds(half, half)]
        relay.append((first, remote(part, part, base + 4 * d + 3, x_dev)))

    send_full(0)
    own_w = pltpu.make_async_copy(w_ref, w_out.at[z, f], local_sem.at[0])
    own_w.start()
    own_t = pltpu.make_async_copy(t_ref, t_out.at[c], local_sem.at[1])
    own_t.start()
    tbase = base + 4 * n_sp
    t_copies = [remote(t_ref, t_out.at[c], tbase + d, t_devs[d]) for d in range(n_tp - 1)]
    for d in range(1, n_sp):
        send_full(d)
        send_relay(d - 1)
    send_relay(n_sp - 1)
    for pair in relay:
        for copy in pair:
            copy.wait_recv()
    for copy in t_copies:
        copy.wait_recv()
    for copy in z_copies + t_copies:
        copy.wait_send()
    for pair in full + relay:
        for copy in pair:
            copy.wait_send()
    own_w.wait()
    own_t.wait()


def gather_inputs(weights, tokens):
    n_sp = lax.axis_size("sp")
    n_fs = lax.axis_size("fs")
    n_tp = lax.axis_size("tp")
    rows, cols = weights.shape
    if n_fs != 4:
        return (
            lax.all_gather(weights, ("sp", "fs"), axis=0, tiled=True),
            lax.all_gather(tokens, "tp", axis=0, tiled=True),
        )
    count = (n_sp - 1) + 4 * n_sp + (n_tp - 1)
    wide, toks = pl.pallas_call(
        functools.partial(gather_kernel, n_sp, n_tp),
        out_shape=(
            jax.ShapeDtypeStruct((n_sp, n_fs, rows, cols), weights.dtype),
            jax.ShapeDtypeStruct((n_tp,) + tokens.shape, tokens.dtype),
        ),
        in_specs=[pl.BlockSpec(memory_space=pltpu.VMEM)] * 2,
        out_specs=[pl.BlockSpec(memory_space=pl.ANY)] * 2,
        scratch_shapes=[
            pltpu.SemaphoreType.DMA((count,)),
            pltpu.SemaphoreType.DMA((count,)),
            pltpu.SemaphoreType.DMA((2,)),
        ],
        compiler_params=pltpu.CompilerParams(collective_id=0, has_side_effects=True),
        cost_estimate=pl.CostEstimate(
            flops=0, bytes_accessed=200 * n_sp * n_fs * rows * cols, transcendentals=0
        ),
        name="gather_inputs",
    )(weights, tokens)
    return wide.reshape(n_sp * n_fs * rows, cols), toks.reshape(-1, tokens.shape[1])


class LineGather:
    def __init__(self, piece, send, recv):
        self.n = lax.axis_size("sp")
        self.z = lax.axis_index("sp")
        self.f = lax.axis_index("fs")
        self.c = lax.axis_index("tp")
        self.fx = self.f + 1 - 2 * lax.rem(self.f, 2)
        self.fy = lax.rem(self.f + 2, 4)
        self.fd = 3 - self.f
        self.piece, self.send, self.recv = piece, send, recv
        self.x_dev = (self.z, self.fx, self.c)
        self.y_dev = (self.z, self.fy, self.c)
        self.up_dev = (lax.rem(self.z + 1, self.n), self.f, self.c)
        self.down_dev = (lax.rem(self.z + self.n - 1, self.n), self.f, self.c)
        self.order = [self.nearest(k) for k in range(self.n)]
        self.pending = []

    def barrier(self, extra=()):
        barrier = pltpu.get_barrier_semaphore()
        devices = [self.x_dev, self.y_dev, self.up_dev, self.down_dev, *extra]
        for device in devices:
            pl.semaphore_signal(barrier, inc=1, device_id=device, device_id_type=MESH)
        pl.semaphore_wait(barrier, len(devices))

    def nearest(self, k):
        z, n = self.z, self.n
        low = jnp.minimum(z, n - 1 - z)
        sign = 1 if k % 2 == 0 else -1
        paired = z + sign * ((k + 1) // 2)
        past = jnp.where(2 * z < n - 1, z + (k - low), z - (k - low))
        return jnp.where(k <= 2 * low, paired, past)

    def hops(self, k):
        lows = [min(z, self.n - 1 - z) for z in range(self.n)]
        return sorted({(k + 1) // 2 if k <= 2 * low else k - low for low in lows})

    def by_line(self, z, p):
        near = jnp.logical_or(p == z + 1, p == z - 1)
        if self.n >= 4:
            near = jnp.logical_or(near, jnp.logical_and(z == 0, p == 2))
            near = jnp.logical_or(near, jnp.logical_and(z == self.n - 1, p == self.n - 3))
        return near

    def copy(self, src, dst, p, s, r, device):
        return pltpu.make_async_remote_copy(
            src_ref=src,
            dst_ref=dst,
            send_sem=self.send.at[p, s],
            recv_sem=self.recv.at[p, r],
            device_id=device,
            device_id_type=MESH,
        )

    def start(self, cond, src, dst, p, s, r, device):
        copy = self.copy(src, dst, p, s, r, device)
        if cond is None:
            copy.start()
        else:
            pl.when(cond)(copy.start)
        self.pending.append((cond, copy))

    def arrive(self, ref, p, r, now=None):
        copy = self.copy(ref, ref, p, 0, r, self.x_dev)
        if now is None:
            copy.wait_recv()
        else:
            pl.when(now)(copy.wait_recv)

    def column(self, k, halves=(0, 1), now=None):
        p = self.order[k]
        up = jnp.logical_and(p <= self.z, self.z < self.n - 1)
        down = jnp.logical_and(p >= self.z, self.z > 0)
        if now is not None:
            up, down = jnp.logical_and(now, up), jnp.logical_and(now, down)
        for h in halves:
            ref = self.piece(p, self.f, h)
            if k > 0:
                self.arrive(ref, p, h, now)
            self.start(now, ref, ref, p, 4 + h, 2 + h, self.x_dev)
            self.start(now, ref, ref, p, 6 + h, 4 + h, self.y_dev)
            self.start(up, ref, ref, p, h, h, self.up_dev)
            self.start(down, ref, ref, p, 2 + h, h, self.down_dev)

    def columns(self, distance, halves=(0, 1)):
        for k in range(1, self.n):
            hops = self.hops(k)
            if hops == [distance]:
                self.column(k, halves)
            elif distance in hops:
                away = self.order[k] - self.z
                now = jnp.logical_or(away == distance, away == -distance)
                self.column(k, halves, now)

    def sides(self, k, halves=(0, 1)):
        p = self.order[k]
        relay = jnp.logical_not(self.by_line(self.z, p))
        for h in halves:
            x_part = self.piece(p, self.fx, h)
            y_part = self.piece(p, self.fy, h)
            self.arrive(x_part, p, 2 + h)
            if h == 0:
                self.start(relay, x_part, x_part, p, 8, 6, self.y_dev)
            self.arrive(y_part, p, 4 + h)
            if h == 1:
                self.start(relay, y_part, y_part, p, 9, 7, self.x_dev)

    def diagonal(self, k, now=None):
        p = self.order[k]
        z, n = self.z, self.n
        up = jnp.logical_and(jnp.logical_and(p <= z, z < n - 1), self.by_line(z + 1, p))
        down = jnp.logical_and(jnp.logical_and(p >= z, z > 0), self.by_line(z - 1, p))
        if now is not None:
            up, down = jnp.logical_and(now, up), jnp.logical_and(now, down)
        for h in range(2):
            part = self.piece(p, self.fd, h)
            self.arrive(part, p, 6 + h, now)
            self.start(up, part, part, p, 10 + h, 6 + h, self.up_dev)
            self.start(down, part, part, p, 12 + h, 6 + h, self.down_dev)

    def diagonals(self, distance):
        for k in range(self.n):
            hops = self.hops(k)
            if hops == [distance]:
                self.diagonal(k)
            elif distance in hops:
                away = self.order[k] - self.z
                self.diagonal(k, jnp.logical_or(away == distance, away == -distance))

    def begin(self, i):
        if i < self.n:
            self.sides(i, (0,))
        if i + 1 < self.n:
            self.columns(i + 1, (0,))

    def end(self, i):
        if i < self.n:
            self.sides(i, (1,))
        if i + 1 < self.n:
            self.columns(i + 1, (1,))
        if i > 0:
            self.diagonals(i - 1)
            return [self.order[i - 1]]
        return []

    def stage(self, i):
        if i < self.n:
            self.sides(i)
        if i + 1 < self.n:
            self.columns(i + 1)
        if i > 0:
            self.diagonals(i - 1)
            return [self.order[i - 1]]
        return []

    def drain(self):
        for cond, copy in self.pending:
            if cond is None:
                copy.wait_send()
            else:
                pl.when(cond)(copy.wait_send)


def layer_kernel(
    gate_ref,
    value_ref,
    key_ref,
    query_ref,
    pool_ref,
    t_ref,
    w_ssd_ref,
    w_pool_ref,
    norm_ref,
    step_ref,
    scale_ref,
    shift_ref,
    conv_value_ref,
    conv_key_ref,
    conv_query_ref,
    gain_ref,
    pool_mix_ref,
    pool_gain_ref,
    out_ref,
    mixed_in,
    others_in,
    w_out,
    toks,
    acc,
    gate,
    rows_ref,
    cols_ref,
    total_ref,
    taps,
    pad,
    act,
    y,
    ends,
    prior,
    finals,
    arrived,
    incoming,
    totals,
    squares,
    mixed,
    away,
    got,
    result,
    w_send,
    w_recv,
    local_sem,
    pair_sem,
    halo_sem,
    total_sem,
    state_sem,
    square_sem,
    part_sem,
    out_sem,
):
    length = toks.shape[0] - 2 * EDGE
    mine = t_ref.shape[0]
    half = length // 2
    groups = cols_ref.shape[0]
    lines = total_ref.shape[0]
    blocks = length // SPAN
    width = groups * STATE
    z = lax.axis_index("sp")
    f = lax.axis_index("fs")
    c = lax.axis_index("tp")
    n = lax.axis_size("sp")
    tile = (SPAN, 2 * HEAD_DIM)
    square = (SPAN, SPAN)
    f32 = jnp.float32
    across = (((1,), (1,)), ((), ()))

    rows = value_ref.shape[0]

    def rows_of(buf):
        def piece(p, member, h):
            at = pl.multiple_of(member * rows + h * (rows // 2), rows // 2)
            return buf.at[p, pl.ds(at, rows // 2)]

        return piece

    own_block = pl.ds(pl.multiple_of(f * rows, rows), rows)

    def columns_of(p, member, h):
        lot, cols = w_ssd_ref.shape
        at = pl.ds(pl.multiple_of((p * 4 + member) * cols, cols), cols)
        return w_out.at[pl.ds(h * lot, lot), at]

    first = LineGather(rows_of(mixed_in), w_send.at[0], w_recv.at[0])
    second = LineGather(rows_of(others_in), w_send.at[1], w_recv.at[1])
    third = LineGather(columns_of, w_send.at[2], w_recv.at[2])
    partner = (z, f, 1 - c)
    ahead = [(lax.rem(z + d, n), f, c) for d in range(n)]
    behind = [(lax.rem(z + n - d, n), f, c) for d in range(n)]

    def local(src, dst, i):
        copy = pltpu.make_async_copy(src, dst, local_sem.at[i])
        copy.start()
        return copy

    own_rows = toks.at[pl.ds(pl.multiple_of(EDGE + c * mine, EDGE), mine)]
    own_first = [
        local(ref, mixed_in.at[z, own_block, pl.ds(i * width, width)], i)
        for i, ref in enumerate((value_ref, key_ref, query_ref))
    ]
    own_tokens = local(t_ref, own_rows, 3)
    own_second = [
        local(ref, others_in.at[z, own_block, pl.ds(i * width, width)], 4 + i)
        for i, ref in enumerate((gate_ref, pool_ref))
    ]
    own_third = [
        local(ref, columns_of(z, f, h), 6 + h) for h, ref in enumerate((w_ssd_ref, w_pool_ref))
    ]
    first.barrier((partner, *ahead[2 : n - 1]))
    pending = []

    def remote(src, dst, sems, index, device, cond=None):
        copy = pltpu.make_async_remote_copy(
            src_ref=src,
            dst_ref=dst,
            send_sem=sems.at[(0, *index)],
            recv_sem=sems.at[(1, *index)],
            device_id=device,
            device_id_type=MESH,
        )
        if cond is None:
            copy.start()
        else:
            pl.when(cond)(copy.start)
        pending.append((cond, copy))
        return copy

    for copy in own_first:
        copy.wait()
    first.column(0)
    own_tokens.wait()
    pair = remote(t_ref, own_rows, pair_sem, (), partner)
    for copy in own_second + own_third:
        copy.wait()
    chunk = 32

    def normalize(start):
        def body(i, carry):
            at = pl.ds(pl.multiple_of(EDGE + start + i * chunk, EDGE), chunk)
            wide = toks[at, :].astype(jnp.float32)
            mean = jnp.mean(wide * wide, axis=-1, keepdims=True)
            toks[at, :] = (wide * lax.rsqrt(mean + EPSILON) * norm_ref[...]).astype(jnp.bfloat16)
            return carry

        lax.fori_loop(0, mine // chunk, body, 0)

    normalize(c * mine)
    first.sides(0, (0,))
    first.columns(1, (0,))
    pair.wait_recv()
    normalize((1 - c) * mine)
    below, above = z > 0, z < n - 1
    from_below = remote(
        toks.at[pl.ds(length, EDGE)], toks.at[pl.ds(0, EDGE)], halo_sem, (0,), ahead[1], above
    )
    from_above = remote(
        toks.at[pl.ds(EDGE, EDGE)],
        toks.at[pl.ds(EDGE + length, EDGE)],
        halo_sem,
        (1,),
        behind[1],
        below,
    )

    @pl.when(jnp.logical_not(below))
    def _():
        toks[:EDGE, :] = jnp.zeros((EDGE, toks.shape[1]), toks.dtype)

    @pl.when(jnp.logical_not(above))
    def _():
        toks[EDGE + length :, :] = jnp.zeros((EDGE, toks.shape[1]), toks.dtype)


    def lanes(i, count=1):
        return pl.ds(pl.multiple_of(i * STATE, STATE), count * STATE)

    def span(i):
        return pl.ds(pl.multiple_of(i * SPAN, SPAN), SPAN)

    def edged(i):
        return pl.ds(pl.multiple_of(EDGE + i * SPAN, EDGE), SPAN)

    def multiply(buf, p, begin=False, store=None):
        depth = buf.shape[1]
        at = pl.ds(pl.multiple_of(p * depth, depth), depth)
        wide = 256

        def body(i, carry):
            cols = pl.ds(pl.multiple_of(i * wide, wide), wide)
            for m in range(2):
                lot = half + EDGE
                part = jnp.dot(
                    toks[m * lot : (m + 1) * lot, at],
                    buf[p, :, cols],
                    preferred_element_type=f32,
                )
                if not begin:
                    part = part + acc[m * lot : (m + 1) * lot, cols]
                if store is None:
                    acc[m * lot : (m + 1) * lot, cols] = part
                else:
                    store(m, i, wide, part.astype(jnp.bfloat16))
            return carry

        count = buf.shape[2] // wide
        if store is None:
            lax.fori_loop(0, count, body, 0)
        else:
            for i in range(count):
                body(i, 0)

    def store_first(m, i, wide, part):
        lot = part.shape[0]
        pad[m * lot : (m + 1) * lot, i * wide : (i + 1) * wide] = part.astype(f32)

    def store_second(m, i, wide, part):
        lot = part.shape[0]
        if i * wide < width:
            gate[m * lot : (m + 1) * lot, i * wide : (i + 1) * wide] = part
        else:
            pad[m * lot : (m + 1) * lot, 2 * width + i * wide : 2 * width + (i + 1) * wide] = (
                part.astype(f32)
            )

    def step_sizes():
        raw = lax.dot_general(
            step_ref[...], toks[EDGE : EDGE + length, :], (((1,), (1,)), ((), ())), preferred_element_type=jnp.float32
        )
        raw = raw + scale_ref[:, :1]
        shift = jnp.concatenate([shift_ref[0, h] for h in range(shift_ref.shape[1])], axis=0)
        steps = jnp.maximum(raw, 0.0) + jnp.log1p(jnp.exp(-jnp.abs(raw)))
        logs = -scale_ref[:, SPAN : SPAN + 1] * steps - shift
        cut = [slice(i * SPAN, (i + 1) * SPAN) for i in range(blocks)]
        steps = jnp.concatenate([steps[:, at] for at in cut], axis=0)
        logs = jnp.concatenate([logs[:, at] for at in cut], axis=0)
        square = (SPAN, SPAN)
        upper = lax.broadcasted_iota(jnp.int32, square, 0) <= lax.broadcasted_iota(
            jnp.int32, square, 1
        )
        inner = jnp.dot(
            logs, upper.astype(jnp.float32), precision=HIGHEST, preferred_element_type=jnp.float32
        )
        total = inner[:, SPAN - 1 :]
        backward = lax.rem(lax.broadcasted_iota(jnp.int32, logs.shape, 0), 2) == 1
        along = inner - jnp.where(backward, logs, 0.0)
        weight = jnp.exp(jnp.where(backward, along, total - along)) * steps
        reach = jnp.exp(jnp.where(backward, total - along, along))
        rows_ref[0] = along
        rows_ref[1] = steps
        rows_ref[2] = jnp.broadcast_to(jnp.exp(total), logs.shape)
        whole = total[:lines]
        for i in range(1, blocks):
            whole = whole + total[i * lines : (i + 1) * lines]
        total_ref[...] = jnp.broadcast_to(whole, total_ref.shape)
        turned = [jnp.transpose(v) for v in (along, weight, reach)]
        for g in range(lines // 4):
            for i in range(blocks):
                for j in range(3):
                    at = i * lines + 4 * g
                    cols_ref[g, cut[i], 4 * j : 4 * j + 4] = turned[j][:, at : at + 4]

    order = first.order
    first.sides(0, (1,))
    first.columns(1, (1,))
    for i, ref in enumerate((conv_value_ref, conv_key_ref, conv_query_ref)):
        taps[:CONV_WIDTH, i * width : (i + 1) * width] = ref[
            :, pl.ds(pl.multiple_of(c * width, width), width)
        ].astype(f32)
    pl.when(below)(from_below.wait_recv)
    pl.when(above)(from_above.wait_recv)
    multiplied = []

    def advance_first(count):
        for _ in range(count):
            multiplied.append(order[len(multiplied)])
            multiply(
                mixed_in,
                multiplied[-1],
                begin=len(multiplied) == 1,
                store=store_first if len(multiplied) == n else None,
            )

    reached = 0
    for k in range(1, n + 1):
        for h in range(2) if k > 1 else ():
            first.sides(k - 1, (h,))
            first.columns(k, (h,))
        if k == 2:
            step_sizes()
        if k == n:
            second.column(0)
        due = 1 if k == 1 else 2 if k == 3 else n if k == n else reached
        while reached < due:
            first.diagonals(reached)
            reached += 1
            advance_first(1)

    sums = [
        remote(total_ref, totals.at[z], total_sem, (d - 1,), ahead[d]) for d in range(1, n)
    ]
    margin = CONV_WIDTH // 2

    def convolve(i, carry):
        at = lanes(i)
        tap = taps[:, at]
        for b in range(blocks):
            begin = EDGE - margin + b * SPAN
            total = pad[begin : begin + SPAN, at] * tap[:1]
            for o in range(1, CONV_WIDTH):
                total = total + pad[begin + o : begin + o + SPAN, at] * tap[o : o + 1]
            act[b * SPAN : (b + 1) * SPAN, at] = jax.nn.silu(total).astype(jnp.bfloat16)
        return carry

    lax.fori_loop(0, groups, convolve, 0)
    second.begin(0)
    lax.fori_loop(groups, 2 * groups, convolve, 0)
    queue = second.end(0)
    step = 4 if blocks % 4 == 0 else 1
    parts = blocks // step

    def block_ends(i, carry):
        g = i // parts
        for u in range(step):
            b = lax.rem(i, parts) * step + u
            at = span(b)
            x = act[at, lanes(g)].astype(f32)
            k = act[at, lanes(groups + g)]
            for r in range(2):
                weight = split_heads(
                    cols_ref[g, at, 4 + r : 5 + r], cols_ref[g, at, 6 + r : 7 + r], 1, tile
                )
                ends[g, r, b] = lax.dot_general(
                    (x * weight).astype(jnp.bfloat16),
                    k,
                    (((0,), (0,)), ((), ())),
                    preferred_element_type=f32,
                )
        return carry

    lax.fori_loop(0, groups * parts // 2, block_ends, 0)
    second.begin(1)
    lax.fori_loop(groups * parts // 2, groups * parts, block_ends, 0)

    def scan(g, r, start, each):
        order = range(blocks) if r == 0 else range(blocks - 1, -1, -1)
        carried = list(start)
        for b in order:
            each(b, carried)
            for h in range(2):
                at = b * lines + 4 * g + 2 * h + r
                scale = rows_ref[2, pl.ds(at, 1), :]
                carried[h] = carried[h] * scale + ends[g, r, b, h * HEAD_DIM : (h + 1) * HEAD_DIM]
        return carried

    def own_states(g, carry):
        zero = jnp.zeros((HEAD_DIM, STATE), f32)
        for r in range(2):
            last = scan(g, r, [zero, zero], lambda b, carried: None)
            for h in range(2):
                finals[r, g, h * HEAD_DIM : (h + 1) * HEAD_DIM] = last[h].astype(jnp.bfloat16)
        return carry

    lax.fori_loop(0, groups, own_states, 0)
    states = []
    for d in range(1, n):
        states.append(
            (
                remote(finals.at[0], arrived.at[0, d - 1], state_sem, (0, d - 1), ahead[d], z + d < n),
                remote(finals.at[1], arrived.at[1, d - 1], state_sem, (1, d - 1), behind[d], z >= d),
            )
        )
    queue += second.end(1)
    lax.fori_loop(2 * groups, 3 * groups, convolve, 0)
    if n >= 3:
        queue += second.stage(2)
    third.column(0)
    taken = [0]

    def advance():
        while queue:
            p = queue.pop(0)
            taken[0] += 1
            multiply(
                others_in,
                p,
                begin=taken[0] == 1,
                store=store_second if taken[0] == n else None,
            )

    advance()
    later = lax.broadcasted_iota(jnp.int32, square, 0)
    sooner = lax.broadcasted_iota(jnp.int32, square, 1)

    def diagonal_blocks(i, carry):
        g = i // parts
        lower = later >= sooner
        equal = later == sooner
        for u in range(step):
            b = lax.rem(i, parts) * step + u
            at = span(b)
            x = act[at, lanes(g)]
            scores = lax.dot_general(
                act[at, lanes(2 * groups + g)],
                act[at, lanes(groups + g)],
                across,
                preferred_element_type=f32,
            )
            outs = []
            for h in range(2):
                line = b * lines + 4 * g + 2 * h
                cf_l = cols_ref[g, at, 2 * h : 2 * h + 1]
                eb_l = cols_ref[g, at, 2 * h + 1 : 2 * h + 2]
                cf_s = rows_ref[0, pl.ds(line, 1), :]
                eb_s = rows_ref[0, pl.ds(line + 1, 1), :]
                df_s = rows_ref[1, pl.ds(line, 1), :]
                db_s = rows_ref[1, pl.ds(line + 1, 1), :]
                decay = jnp.exp(jnp.where(lower, cf_l - cf_s, eb_s - eb_l))
                size = jnp.where(equal, df_s + db_s, jnp.where(lower, df_s, db_s))
                outs.append(
                    jnp.dot(
                        (scores * decay * size).astype(jnp.bfloat16), x, preferred_element_type=f32
                    )
                )
            y[at, lanes(g)] = split_heads(outs[0], outs[1], 1, tile)
        return carry

    count = groups * parts
    lax.fori_loop(0, count // 4, diagonal_blocks, 0)
    if n >= 4:
        second.begin(3)
    lax.fori_loop(count // 4, count // 2, diagonal_blocks, 0)
    if n >= 4:
        queue += second.end(3)
    third.begin(0)
    lax.fori_loop(count // 2, 3 * count // 4, diagonal_blocks, 0)
    queue += second.stage(n)
    third.end(0)
    lax.fori_loop(3 * count // 4, count, diagonal_blocks, 0)
    third.begin(1)
    advance()
    third.end(1)

    def pooled(i, carry):
        where_global = (
            z * length + i * SPAN + lax.broadcasted_iota(jnp.int32, (SPAN, POOL_DIM), 0)
        )
        for j in range(groups):
            window = WINDOWS[j % 4]
            at = slice(3 * width + j * POOL_DIM, 3 * width + (j + 1) * POOL_DIM)
            block = pad[pl.ds(pl.multiple_of(i * SPAN, SPAN), SPAN + 2 * EDGE), at]
            first = EDGE - window // 2
            running = block[first : first + SPAN]
            for o in range(1, window):
                running = running + block[first + o : first + o + SPAN]
            lower = jnp.maximum(where_global - window // 2, 0)
            upper = jnp.minimum(where_global + window - window // 2, n * length)
            mean = running / (upper - lower).astype(f32)
            diff = (mean - block[EDGE : EDGE + SPAN]).astype(jnp.bfloat16)
            mapped = jnp.dot(diff, pool_mix_ref[c * groups + j], preferred_element_type=f32)
            gain = pool_gain_ref[:, lanes(c * groups + j)]
            mixed[span(i), width + j * POOL_DIM : width + (j + 1) * POOL_DIM] = (
                mapped * gain
            ).astype(jnp.bfloat16)
        return carry

    lax.fori_loop(0, blocks, pooled, 0)
    if n >= 3:
        third.begin(2)
    incoming[...] = jnp.zeros(incoming.shape, f32)
    for copy in sums:
        copy.wait_recv()
    for d in range(1, n):
        for r in range(2):

            def receive(d=d, r=r):
                states[d - 1][r].wait_recv()
                log = jnp.zeros(total_ref.shape, f32)
                for e in range(1, d):
                    log = log + totals[z - e if r == 0 else z + e]
                scale = jnp.exp(log)
                for g in range(groups):
                    for h in range(2):
                        line = 4 * g + 2 * h + r
                        at = slice(h * HEAD_DIM, (h + 1) * HEAD_DIM)
                        incoming[g, r, at] = incoming[g, r, at] + scale[
                            line : line + 1
                        ] * arrived[r, d - 1, g, at].astype(f32)

            pl.when(z >= d if r == 0 else z + d < n)(receive)
    squares[0] = jnp.zeros(squares.shape[1:], f32)

    def outputs(g, carry):
        for r in range(2):

            def keep(b, carried, r=r):
                for h in range(2):
                    prior[b, r * STATE + h * HEAD_DIM : r * STATE + (h + 1) * HEAD_DIM] = carried[
                        h
                    ].astype(jnp.bfloat16)

            scan(g, r, [incoming[g, r, :HEAD_DIM], incoming[g, r, HEAD_DIM:]], keep)
        for b in range(blocks):
            at = span(b)
            far = lax.dot_general(
                act[at, lanes(2 * groups + g)], prior[b], across, preferred_element_type=f32
            )
            out = y[at, lanes(g)]
            for r in range(2):
                reach = split_heads(
                    cols_ref[g, at, 8 + r : 9 + r], cols_ref[g, at, 10 + r : 11 + r], 1, tile
                )
                out = out + reach * far[:, r * STATE : (r + 1) * STATE]
            out = out * jax.nn.silu(gate[edged(b), lanes(g)].astype(f32))
            y[at, lanes(g)] = out
            squares[0, at] = squares[0, at] + jnp.sum(out * out, axis=-1, keepdims=True)
        return carry

    if n >= 3:
        third.end(2)
    lax.fori_loop(0, groups // 2, outputs, 0)
    if n >= 4:
        third.begin(3)
    lax.fori_loop(groups // 2, groups, outputs, 0)
    other = remote(squares.at[0], squares.at[1], square_sem, (), partner)
    if n >= 4:
        third.end(3)
    other.wait_recv()

    def scale_rows(b, carry):
        at = span(b)
        scale = lax.rsqrt((squares[0, at] + squares[1, at]) / (2 * width) + EPSILON)
        for g in range(groups):
            mixed[at, g * STATE : (g + 1) * STATE] = (
                y[at, g * STATE : (g + 1) * STATE] * scale * gain_ref[:, lanes(c * groups + g)]
            ).astype(jnp.bfloat16)
        return carry

    lax.fori_loop(0, blocks, scale_rows, 0)
    part = result.shape[1] // n
    wide = part // 2

    def product(head, target, p):
        for i in range(2):
            at = pl.ds(pl.multiple_of(p * part + i * wide, wide), wide)
            target[:, at] = jnp.dot(
                mixed[pl.ds(pl.multiple_of(head, half), half), :],
                w_out[:, at],
                preferred_element_type=f32,
            ).astype(jnp.bfloat16)

    sent, written = [], []

    def finish(k):
        p = third.order[k]
        product(c * half, result, p)
        sent[k].wait_recv()
        at = pl.ds(pl.multiple_of(p * part, part), part)
        result[:, at] = (result[:, at].astype(f32) + got[:, at].astype(f32)).astype(jnp.bfloat16)
        copy = pltpu.make_async_copy(result.at[:, at], out_ref.at[:, at], out_sem.at[k])
        copy.start()
        written.append(copy)

    for k in range(n):
        if k == n - 1:
            third.stage(n)
        p = third.order[k]
        product((1 - c) * half, away, p)
        ref = pl.ds(pl.multiple_of(p * part, part), part)
        sent.append(remote(away.at[:, ref], got.at[:, ref], part_sem, (k,), partner))
        if k > 0:
            finish(k - 1)
    finish(n - 1)
    for copy in written:
        copy.wait()
    for cond, copy in pending:
        if cond is None:
            copy.wait_send()
        else:
            pl.when(cond)(copy.wait_send)
    for gather in (first, second, third):
        gather.drain()


def fused_layer(weights, tokens, w_ssd, w_pool, small, groups):
    n = lax.axis_size("sp")
    half, features = tokens.shape
    length = 2 * half
    width = groups * STATE
    lines = 4 * groups
    blocks = length // SPAN
    rows = weights[0].shape[0]
    out_rows, out_cols = 2 * w_ssd.shape[0], 4 * n * w_ssd.shape[1]
    anywhere = pl.BlockSpec(memory_space=pl.ANY)
    inside = pl.BlockSpec(memory_space=pltpu.VMEM)
    bf16, f32 = jnp.bfloat16, jnp.float32
    dma = pltpu.SemaphoreType.DMA
    return pl.pallas_call(
        layer_kernel,
        out_shape=jax.ShapeDtypeStruct((half, out_cols), bf16),
        in_specs=[anywhere] * 8 + [inside] * len(small),
        out_specs=anywhere,
        scratch_shapes=[
            pltpu.VMEM((n, 4 * rows, 3 * width), bf16),
            pltpu.VMEM((n, 4 * rows, 2 * width), bf16),
            pltpu.VMEM((out_rows, out_cols), bf16),
            pltpu.VMEM((length + 2 * EDGE, features), bf16),
            pltpu.VMEM((length + 2 * EDGE, 3 * width), f32),
            pltpu.VMEM((length + 2 * EDGE, width), bf16),
            pltpu.VMEM((3, lines * blocks, SPAN), f32),
            pltpu.VMEM((groups, length, 12), f32),
            pltpu.VMEM((lines, SPAN), f32),
            pltpu.VMEM((8, 3 * width), f32),
            pltpu.VMEM((length + 2 * EDGE, 4 * width), f32),
            pltpu.VMEM((length, 3 * width), bf16),
            pltpu.VMEM((length, width), f32),
            pltpu.VMEM((groups, 2, blocks, STATE, STATE), f32),
            pltpu.VMEM((blocks, 2 * STATE, STATE), bf16),
            pltpu.VMEM((2, groups, STATE, STATE), bf16),
            pltpu.VMEM((2, n - 1, groups, STATE, STATE), bf16),
            pltpu.VMEM((groups, 2, STATE, STATE), f32),
            pltpu.VMEM((n, lines, SPAN), f32),
            pltpu.VMEM((2, length, SPAN), f32),
            pltpu.VMEM((length, 2 * width), bf16),
            pltpu.VMEM((half, out_cols), bf16),
            pltpu.VMEM((half, out_cols), bf16),
            pltpu.VMEM((half, out_cols), bf16),
            dma((3, n, 14)),
            dma((3, n, 8)),
            dma((8,)),
            dma((2,)),
            dma((2, 2)),
            dma((2, n - 1)),
            dma((2, 2, n - 1)),
            dma((2,)),
            dma((2, n)),
            dma((n,)),
        ],
        compiler_params=pltpu.CompilerParams(
            collective_id=0, has_side_effects=True, vmem_limit_bytes=VMEM_LIMIT
        ),
        name="mixer",
    )(*weights, tokens, w_ssd, w_pool, *small)


def split_heads(first, second, axis, shape):
    places = lax.broadcasted_iota(jnp.int32, shape, axis)
    return jnp.where(places < HEAD_DIM, first, second)


def ends_kernel(blocks, decay_ref, x_ref, k_ref, col_ref, ends_ref, final_ref):
    group = pl.program_id(0)
    tile = (SPAN, 2 * HEAD_DIM)
    for c in range(blocks):
        rows = pl.ds(c * SPAN, SPAN)
        x = x_ref[rows, :].astype(jnp.float32)
        k = k_ref[rows, :]
        for r in range(2):
            weight = split_heads(
                col_ref[0, rows, 4 + 2 * r : 5 + 2 * r],
                col_ref[0, rows, 5 + 2 * r : 6 + 2 * r],
                1,
                tile,
            )
            end = lax.dot_general(
                (x * weight).astype(jnp.bfloat16),
                k,
                (((0,), (0,)), ((), ())),
                preferred_element_type=jnp.float32,
            )
            ends_ref[0, r, c] = end
    states = (2 * HEAD_DIM, STATE)
    for r in range(2):
        total = jnp.zeros(states, jnp.float32)
        for c in range(blocks) if r == 0 else range(blocks - 1, -1, -1):
            at = ((group * blocks + c) * 2 + r) * 2
            scale = split_heads(decay_ref[at], decay_ref[at + 1], 0, states)
            total = total * scale + ends_ref[0, r, c]
        final_ref[0, r] = total


def outputs_kernel(
    blocks, decay_ref, x_ref, k_ref, q_ref, col_ref, row_ref, ends_ref, in_ref, y_ref, prior
):
    group = pl.program_id(0)
    states = (2 * HEAD_DIM, STATE)
    tile = (SPAN, 2 * HEAD_DIM)
    square = (SPAN, SPAN)
    for r in range(2):
        total = in_ref[0, r]
        for c in range(blocks) if r == 0 else range(blocks - 1, -1, -1):
            prior[r, c] = total.astype(jnp.bfloat16)
            at = ((group * blocks + c) * 2 + r) * 2
            scale = split_heads(decay_ref[at], decay_ref[at + 1], 0, states)
            total = total * scale + ends_ref[0, r, c]
    later = lax.broadcasted_iota(jnp.int32, square, 0)
    sooner = lax.broadcasted_iota(jnp.int32, square, 1)
    lower = later >= sooner
    equal = later == sooner
    across = (((1,), (1,)), ((), ()))
    for c in range(blocks):
        rows = pl.ds(c * SPAN, SPAN)
        x = x_ref[rows, :]
        q = q_ref[rows, :]
        scores = lax.dot_general(q, k_ref[rows, :], across, preferred_element_type=jnp.float32)
        parts = []
        for h in range(2):
            cf_l = col_ref[0, rows, 2 * h : 2 * h + 1]
            eb_l = col_ref[0, rows, 2 * h + 1 : 2 * h + 2]
            cf_s = row_ref[0, 4 * h : 4 * h + 1, rows]
            eb_s = row_ref[0, 4 * h + 1 : 4 * h + 2, rows]
            df_s = row_ref[0, 4 * h + 2 : 4 * h + 3, rows]
            db_s = row_ref[0, 4 * h + 3 : 4 * h + 4, rows]
            decay = jnp.exp(jnp.where(lower, cf_l - cf_s, eb_s - eb_l))
            step = jnp.where(equal, df_s + db_s, jnp.where(lower, df_s, db_s))
            parts.append(
                jnp.dot(
                    (scores * decay * step).astype(jnp.bfloat16),
                    x,
                    preferred_element_type=jnp.float32,
                )
            )
        out = split_heads(parts[0], parts[1], 1, tile)
        for r in range(2):
            reach = split_heads(
                col_ref[0, rows, 8 + 2 * r : 9 + 2 * r],
                col_ref[0, rows, 9 + 2 * r : 10 + 2 * r],
                1,
                tile,
            )
            out = out + reach * lax.dot_general(
                q, prior[r, c], across, preferred_element_type=jnp.float32
            )
        y_ref[rows, :] = out


def mixer(activated, width_ssd, width_key, steps, logs, sp_rank):
    length = activated.shape[0]
    heads = steps.shape[1]
    groups = width_key // STATE
    blocks = length // SPAN
    shaped = logs.reshape(2, heads, blocks, SPAN)
    ones = jnp.triu(jnp.ones((SPAN, SPAN), jnp.float32))
    inner = jnp.einsum("rhcs,sl->rhcl", shaped, ones, precision=HIGHEST)
    totals = inner[..., -1:]
    cf = inner[0]
    eb = inner[1] - shaped[1]
    wf = jnp.exp(totals[0] - cf) * steps[0].reshape(cf.shape)
    wb = jnp.exp(eb) * steps[1].reshape(cf.shape)
    reach_f = jnp.exp(cf)
    reach_b = jnp.exp(totals[1] - eb)

    def pair(a):
        return a.reshape(groups, 2, length)

    cf, eb, wf, wb, reach_f, reach_b = map(pair, (cf, eb, wf, wb, reach_f, reach_b))
    df, db = (pair(steps[0]), pair(steps[1]))
    packed = jnp.stack(
        [cf[:, 0], eb[:, 0], cf[:, 1], eb[:, 1]]
        + [wf[:, 0], wf[:, 1], wb[:, 0], wb[:, 1]]
        + [reach_f[:, 0], reach_f[:, 1], reach_b[:, 0], reach_b[:, 1]],
        axis=1,
    )
    cols = jnp.transpose(packed, (0, 2, 1))
    rows = jnp.stack(
        [cf[:, 0], eb[:, 0], df[:, 0], db[:, 0], cf[:, 1], eb[:, 1], df[:, 1], db[:, 1]], axis=1
    )
    block_logs = totals[..., 0]
    decays = jnp.exp(block_logs).reshape(2, groups, 2, blocks)
    decays = jnp.transpose(decays, (1, 3, 0, 2)).reshape(-1)
    smem = pl.BlockSpec(memory_space=pltpu.SMEM)
    x_blocks = width_ssd // STATE

    def wide(offset):
        return pl.BlockSpec((length, STATE), lambda g: (0, g + offset))

    col_spec = pl.BlockSpec((1, length, cols.shape[2]), lambda g: (g, 0, 0))
    ends_spec = pl.BlockSpec((1, 2, blocks, STATE, STATE), lambda g: (g, 0, 0, 0, 0))
    state_spec = pl.BlockSpec((1, 2, STATE, STATE), lambda g: (g, 0, 0, 0))
    ends, finals = pl.pallas_call(
        functools.partial(ends_kernel, blocks),
        grid=(groups,),
        out_shape=(
            jax.ShapeDtypeStruct((groups, 2, blocks, STATE, STATE), jnp.float32),
            jax.ShapeDtypeStruct((groups, 2, STATE, STATE), jnp.float32),
        ),
        in_specs=[smem, wide(0), wide(x_blocks), col_spec],
        out_specs=(ends_spec, state_spec),
        cost_estimate=pl.CostEstimate(
            flops=4 * length * groups * STATE * STATE,
            bytes_accessed=16 * length * groups * STATE,
            transcendentals=0,
        ),
        name="block_ends",
    )(decays, activated, activated, cols)
    device_totals = jnp.sum(block_logs, axis=-1)
    all_totals = lax.all_gather(
        device_totals[None].astype(jnp.bfloat16), "sp", axis=0, tiled=True
    ).astype(jnp.float32)
    states = jnp.transpose(finals, (1, 0, 2, 3)).reshape(2, heads, HEAD_DIM, STATE)
    forward_in, backward_in = prefix_states(all_totals, states.astype(jnp.bfloat16), sp_rank)
    incoming = jnp.stack([forward_in, backward_in]).reshape(2, groups, STATE, STATE)
    incoming = jnp.transpose(incoming, (1, 0, 2, 3))
    return pl.pallas_call(
        functools.partial(outputs_kernel, blocks),
        grid=(groups,),
        out_shape=jax.ShapeDtypeStruct((length, groups * STATE), jnp.float32),
        in_specs=[
            smem,
            wide(0),
            wide(x_blocks),
            wide(x_blocks + groups),
            col_spec,
            pl.BlockSpec((1, 8, length), lambda g: (g, 0, 0)),
            ends_spec,
            state_spec,
        ],
        out_specs=wide(0),
        scratch_shapes=[pltpu.VMEM((2, blocks, STATE, STATE), jnp.bfloat16)],
        cost_estimate=pl.CostEstimate(
            flops=10 * length * groups * STATE * STATE,
            bytes_accessed=40 * length * groups * STATE,
            transcendentals=2 * length * groups * SPAN,
        ),
        name="block_outputs",
    )(decays, activated, activated, activated, cols, rows, ends, incoming)


def prefix_states(all_totals, finals, rank):
    chain_length = all_totals.shape[0]
    device_ids = jnp.arange(chain_length, dtype=jnp.int32)[:, None]
    forward_cum = jnp.cumsum(all_totals[:, 0], axis=0)
    forward_mine = lax.dynamic_slice_in_dim(forward_cum - all_totals[:, 0], rank, 1, 0)
    forward_weight = jnp.exp(jnp.where(device_ids < rank, forward_mine - forward_cum, -jnp.inf))
    backward_cum = jnp.cumsum(all_totals[:, 1], axis=0)
    backward_mine = lax.dynamic_slice_in_dim(backward_cum, rank, 1, 0)
    backward_weight = jnp.exp(
        jnp.where(device_ids > rank, backward_cum - all_totals[:, 1] - backward_mine, -jnp.inf)
    )
    forward_in = jnp.zeros(finals.shape[1:], jnp.float32)
    backward_in = jnp.zeros(finals.shape[1:], jnp.float32)
    for d in range(1, chain_length):
        ahead = [(i, i + d) for i in range(chain_length - d)]
        back = [(i + d, i) for i in range(chain_length - d)]
        from_left = lax.ppermute(finals[0], "sp", ahead).astype(jnp.float32)
        from_right = lax.ppermute(finals[1], "sp", back).astype(jnp.float32)
        left = lax.dynamic_index_in_dim(forward_weight, jnp.maximum(rank - d, 0), 0, False)
        right = lax.dynamic_index_in_dim(
            backward_weight, jnp.minimum(rank + d, chain_length - 1), 0, False
        )
        forward_in = forward_in + left[:, None, None] * from_left
        backward_in = backward_in + right[:, None, None] * from_right
    return (forward_in, backward_in)


def local(
    tokens,
    norm_gain,
    w_gate,
    w_value,
    w_bkey,
    w_query,
    w_pool_in,
    w_step,
    step_bias,
    decay_rate,
    decay_shift,
    conv_value,
    conv_bkey,
    conv_query,
    mix_gain,
    pool_mix,
    pool_gain,
    w_out_ssd,
    w_out_pool,
):
    tp_count = lax.axis_size("tp")
    sp_count = lax.axis_size("sp")
    tp_rank = lax.axis_index("tp")
    sp_rank = lax.axis_index("sp")
    heads_dev = DUALITY_HEADS // tp_count
    groups_dev = GROUPS // tp_count
    pools_dev = POOL_GROUPS // tp_count
    width_ssd = heads_dev * HEAD_DIM
    width_key = groups_dev * STATE
    width_pool = pools_dev * POOL_DIM
    fast = (
        tp_count == 2
        and lax.axis_size("fs") == 4
        and 2 <= sp_count <= 4
        and w_gate.shape[0] % 128 == 0
        and w_out_ssd.shape[1] % 128 == 0
        and pools_dev == groups_dev
        and width_ssd == width_key
        and groups_dev % 4 == 0
        and 2 * tokens.shape[1] * 2 * heads_dev % (SPAN * SPAN) == 0
    )
    step_cols = lax.dynamic_slice_in_dim(w_step, tp_rank * heads_dev, heads_dev, 2)
    bias_dev = lax.dynamic_slice_in_dim(step_bias, tp_rank * heads_dev, heads_dev, 1)
    rate_dev = lax.dynamic_slice_in_dim(decay_rate, tp_rank * heads_dev, heads_dev, 1)
    if fast:
        lines = 2 * heads_dev
        scales = jnp.stack([bias_dev, rate_dev], axis=-1)
        scales = jnp.transpose(scales, (1, 0, 2)).reshape(lines, 2, 1)
        small = (
            norm_gain[None],
            jnp.transpose(step_cols, (2, 1, 0)).reshape(lines, -1),
            jnp.broadcast_to(scales, (lines, 2, SPAN)).reshape(lines, 2 * SPAN),
            decay_shift,
            conv_value,
            conv_bkey,
            conv_query,
            mix_gain[None],
            pool_mix,
            pool_gain[None],
        )
        return fused_layer(
            (w_gate, w_value, w_bkey, w_query, w_pool_in),
            tokens[0],
            w_out_ssd,
            w_out_pool,
            small,
            groups_dev,
        )[None]
    step_cols = step_cols.reshape(w_step.shape[0], 2 * heads_dev)
    weights = jnp.concatenate([w_gate, w_value, w_bkey, w_query, w_pool_in], axis=1)
    combined, widened = gather_inputs(weights, tokens[0])
    out_rows = lax.all_gather(
        jnp.concatenate([w_out_ssd, w_out_pool], axis=0), ("sp", "fs"), axis=1, tiled=True
    )
    widened = widened.astype(jnp.float32)
    scaling = lax.rsqrt(jnp.mean(widened * widened, axis=-1, keepdims=True) + EPSILON)
    normed = (widened * scaling * norm_gain).astype(jnp.bfloat16)
    stored = jnp.dot(normed, combined, preferred_element_type=jnp.float32).astype(jnp.bfloat16)
    raw_steps = jnp.dot(normed, step_cols, preferred_element_type=jnp.float32)
    length = stored.shape[0]
    padded = padded_2(stored[:, width_ssd:], (("sp", 0),), REACH)
    conv_cols = width_ssd + 2 * width_key
    taps = jnp.concatenate(
        [
            lax.dynamic_slice_in_dim(conv_value, tp_rank * width_ssd, width_ssd, 1),
            lax.dynamic_slice_in_dim(conv_bkey, tp_rank * width_key, width_key, 1),
            lax.dynamic_slice_in_dim(conv_query, tp_rank * width_key, width_key, 1),
        ],
        axis=1,
    ).astype(jnp.float32)
    margin = CONV_WIDTH // 2
    convolved = jnp.zeros((length, conv_cols), jnp.float32)
    for offset in range(CONV_WIDTH):
        begin = REACH - margin + offset
        convolved = (
            convolved
            + padded[begin : begin + length, :conv_cols].astype(jnp.float32) * taps[offset]
        )
    activated = jax.nn.silu(convolved).astype(jnp.bfloat16)
    steps = jax.nn.softplus(raw_steps.reshape(length, 2, heads_dev) + bias_dev).transpose(1, 2, 0)
    logs = -rate_dev[:, :, None] * steps - decay_shift[0].transpose(1, 0, 2)
    heads_out = mixer(activated, width_ssd, width_key, steps, logs, sp_rank)
    gated = heads_out * jax.nn.silu(stored[:, :width_ssd].astype(jnp.float32))
    squares = lax.psum(jnp.sum(gated * gated, axis=-1), "tp")
    gain_dev = lax.dynamic_slice_in_dim(mix_gain, tp_rank * width_ssd, width_ssd, 0)
    ssd_mix = (gated * lax.rsqrt(squares / D_SSM + EPSILON)[:, None] * gain_dev).astype(
        jnp.bfloat16
    )
    pool_rows = padded[:, conv_cols:].astype(jnp.float32)
    own_rows = pool_rows[REACH : REACH + length]
    where_global = sp_rank * length + jnp.arange(length, dtype=jnp.int32)
    seq_length = length * sp_count
    window_means = []
    for window in WINDOWS:
        running = jnp.zeros((length, width_pool), jnp.float32)
        for offset in range(-(window // 2), window - window // 2):
            running = running + pool_rows[REACH + offset : REACH + offset + length]
        lower = jnp.clip(where_global - window // 2, 0, seq_length)
        upper = jnp.clip(where_global + window - window // 2, 0, seq_length)
        window_means.append(running / (upper - lower).astype(jnp.float32)[:, None])
    stacked = jnp.stack(window_means).reshape(4, length, pools_dev, POOL_DIM)
    group_ids = tp_rank * pools_dev + jnp.arange(pools_dev, dtype=jnp.int32)
    selector = (jnp.arange(4, dtype=jnp.int32)[:, None] == (group_ids % 4)[None, :]).astype(
        jnp.float32
    )
    means = jnp.sum(stacked * selector[:, None, :, None], axis=0)
    differences = (means - own_rows.reshape(length, pools_dev, POOL_DIM)).astype(jnp.bfloat16)
    pool_weights = lax.dynamic_slice_in_dim(pool_mix, tp_rank * pools_dev, pools_dev, 0)
    mapped = jnp.einsum(
        "rgc,gcd->rgd", differences, pool_weights, preferred_element_type=jnp.float32
    )
    pool_gain_dev = lax.dynamic_slice_in_dim(pool_gain, tp_rank * width_pool, width_pool, 0)
    pool_out = (mapped.reshape(length, width_pool) * pool_gain_dev).astype(jnp.bfloat16)
    mixed = jnp.concatenate([ssd_mix, pool_out], axis=1)
    if tp_count == 2:
        part = length // 2
        away = lax.dynamic_slice_in_dim(mixed, (1 - tp_rank) * part, part, 0)
        home = lax.dynamic_slice_in_dim(mixed, tp_rank * part, part, 0)
        sent = jnp.dot(away, out_rows, preferred_element_type=jnp.float32).astype(jnp.bfloat16)
        received = lax.ppermute(sent, "tp", [(0, 1), (1, 0)])
        kept = lax.optimization_barrier(
            jnp.dot(home, out_rows, preferred_element_type=jnp.float32).astype(jnp.bfloat16)
        )
        summed = (kept.astype(jnp.float32) + received.astype(jnp.float32)).astype(jnp.bfloat16)
    else:
        summed = lax.psum_scatter(
            jnp.dot(mixed, out_rows, preferred_element_type=jnp.float32).astype(jnp.bfloat16),
            "tp",
            scatter_dimension=0,
            tiled=True,
        )
    return summed[None]


def solution(mesh):
    return jax.shard_map(
        local,
        mesh=mesh,
        in_specs=(
            P("fs", ("sp", "tp"), None),
            P(),
            P(("sp", "fs"), "tp"),
            P(("sp", "fs"), "tp"),
            P(("sp", "fs"), "tp"),
            P(("sp", "fs"), "tp"),
            P(("sp", "fs"), "tp"),
            P(),
            P(),
            P(),
            P("fs", "tp", None, "sp"),
            P(),
            P(),
            P(),
            P(),
            P(),
            P(),
            P("tp", ("sp", "fs")),
            P("tp", ("sp", "fs")),
        ),
        out_specs=P("fs", ("sp", "tp"), None),
        check_vma=False,
    )
```

```python
import functools

import jax
import jax.numpy as jnp
from jax import lax
from jax.experimental import pallas as pl
from jax.experimental.pallas import tpu as pltpu
from jax.sharding import PartitionSpec as P

HEAD_DIM = 64
DUALITY_HEADS = 16
GROUPS = 8
STATE = 128
CONV_WIDTH = 5
POOL_GROUPS = 8
POOL_DIM = 128
SPAN = 128
REACH = 8
EDGE = 16
VMEM_LIMIT = 63 * 2**20
D_SSM = 1024


EPSILON = 1e-06
HIGHEST = lax.Precision.HIGHEST
WINDOWS = (2, 4, 8, 16)


def padded_2(cells, sides, width):
    for axis, dim in sides:
        count = lax.axis_size(axis)
        ends = count - 1
        head = lax.slice_in_dim(cells, 0, width, axis=dim)
        tail = lax.slice_in_dim(cells, cells.shape[dim] - width, cells.shape[dim], axis=dim)
        cells = jnp.concatenate(
            [
                lax.ppermute(tail, axis, [(i, (i + 1) % count) for i in range(ends)]),
                cells,
                lax.ppermute(head, axis, [((i + 1) % count, i) for i in range(ends)]),
            ],
            axis=dim,
        )
    return cells


MESH = pl.DeviceIdType.MESH


def gather_kernel(n_sp, n_tp, w_ref, t_ref, w_out, t_out, send, recv, local_sem):
    z = lax.axis_index("sp")
    f = lax.axis_index("fs")
    c = lax.axis_index("tp")
    fx = f + 1 - 2 * lax.rem(f, 2)
    fy = lax.rem(f + 2, 4)
    rows = w_ref.shape[0]
    half = rows // 2
    x_dev = (z, fx, c)
    y_dev = (z, fy, c)
    z_devs = [(lax.rem(z + d, n_sp), f, c) for d in range(1, n_sp)]
    t_devs = [(z, f, lax.rem(c + d, n_tp)) for d in range(1, n_tp)]
    partners = [x_dev, y_dev] + z_devs + t_devs
    barrier = pltpu.get_barrier_semaphore()
    for dev in partners:
        pl.semaphore_signal(barrier, inc=1, device_id=dev, device_id_type=MESH)
    pl.semaphore_wait(barrier, len(partners))

    def remote(src, dst, index, dev):
        copy = pltpu.make_async_remote_copy(
            src_ref=src,
            dst_ref=dst,
            send_sem=send.at[index],
            recv_sem=recv.at[index],
            device_id=dev,
            device_id_type=MESH,
        )
        copy.start()
        return copy

    base = n_sp - 1
    z_copies = [remote(w_ref, w_out.at[z, f], d, z_devs[d]) for d in range(n_sp - 1)]
    full = []
    relay = []

    def send_full(d):
        if d == 0:
            src = w_ref
            origin = z
        else:
            z_copies[d - 1].wait_recv()
            origin = lax.rem(z - d + n_sp, n_sp)
            src = w_out.at[origin, f]
        dst = w_out.at[origin, f]
        full.append(
            (
                remote(src, dst, base + 4 * d, x_dev),
                remote(src, dst, base + 4 * d + 1, y_dev),
            )
        )

    def send_relay(d):
        origin = lax.rem(z - d + n_sp, n_sp)
        full[d][0].wait_recv()
        part = w_out.at[origin, fx, pl.ds(0, half)]
        first = remote(part, part, base + 4 * d + 2, y_dev)
        full[d][1].wait_recv()
        part = w_out.at[origin, fy, pl.ds(half, half)]
        relay.append((first, remote(part, part, base + 4 * d + 3, x_dev)))

    send_full(0)
    own_w = pltpu.make_async_copy(w_ref, w_out.at[z, f], local_sem.at[0])
    own_w.start()
    own_t = pltpu.make_async_copy(t_ref, t_out.at[c], local_sem.at[1])
    own_t.start()
    tbase = base + 4 * n_sp
    t_copies = [remote(t_ref, t_out.at[c], tbase + d, t_devs[d]) for d in range(n_tp - 1)]
    for d in range(1, n_sp):
        send_full(d)
        send_relay(d - 1)
    send_relay(n_sp - 1)
    for pair in relay:
        for copy in pair:
            copy.wait_recv()
    for copy in t_copies:
        copy.wait_recv()
    for copy in z_copies + t_copies:
        copy.wait_send()
    for pair in full + relay:
        for copy in pair:
            copy.wait_send()
    own_w.wait()
    own_t.wait()


def gather_inputs(weights, tokens):
    n_sp = lax.axis_size("sp")
    n_fs = lax.axis_size("fs")
    n_tp = lax.axis_size("tp")
    rows, cols = weights.shape
    if n_fs != 4:
        return (
            lax.all_gather(weights, ("sp", "fs"), axis=0, tiled=True),
            lax.all_gather(tokens, "tp", axis=0, tiled=True),
        )
    count = (n_sp - 1) + 4 * n_sp + (n_tp - 1)
    wide, toks = pl.pallas_call(
        functools.partial(gather_kernel, n_sp, n_tp),
        out_shape=(
            jax.ShapeDtypeStruct((n_sp, n_fs, rows, cols), weights.dtype),
            jax.ShapeDtypeStruct((n_tp,) + tokens.shape, tokens.dtype),
        ),
        in_specs=[pl.BlockSpec(memory_space=pltpu.VMEM)] * 2,
        out_specs=[pl.BlockSpec(memory_space=pl.ANY)] * 2,
        scratch_shapes=[
            pltpu.SemaphoreType.DMA((count,)),
            pltpu.SemaphoreType.DMA((count,)),
            pltpu.SemaphoreType.DMA((2,)),
        ],
        compiler_params=pltpu.CompilerParams(collective_id=0, has_side_effects=True),
        cost_estimate=pl.CostEstimate(
            flops=0, bytes_accessed=200 * n_sp * n_fs * rows * cols, transcendentals=0
        ),
        name="gather_inputs",
    )(weights, tokens)
    return wide.reshape(n_sp * n_fs * rows, cols), toks.reshape(-1, tokens.shape[1])


class LineGather:
    def __init__(self, piece, send, recv):
        self.n = lax.axis_size("sp")
        self.z = lax.axis_index("sp")
        self.f = lax.axis_index("fs")
        self.c = lax.axis_index("tp")
        self.fx = self.f + 1 - 2 * lax.rem(self.f, 2)
        self.fy = lax.rem(self.f + 2, 4)
        self.fd = 3 - self.f
        self.piece, self.send, self.recv = piece, send, recv
        self.x_dev = (self.z, self.fx, self.c)
        self.y_dev = (self.z, self.fy, self.c)
        self.up_dev = (lax.rem(self.z + 1, self.n), self.f, self.c)
        self.down_dev = (lax.rem(self.z + self.n - 1, self.n), self.f, self.c)
        self.order = [self.nearest(k) for k in range(self.n)]
        self.pending = []
        self.crossed = 0

    def barrier(self, extra=()):
        barrier = pltpu.get_barrier_semaphore()
        devices = [self.x_dev, self.y_dev, self.up_dev, self.down_dev, *extra]
        for device in devices:
            pl.semaphore_signal(barrier, inc=1, device_id=device, device_id_type=MESH)
        pl.semaphore_wait(barrier, len(devices))

    def nearest(self, k):
        z, n = self.z, self.n
        low = jnp.minimum(z, n - 1 - z)
        sign = 1 if k % 2 == 0 else -1
        paired = z + sign * ((k + 1) // 2)
        past = jnp.where(2 * z < n - 1, z + (k - low), z - (k - low))
        return jnp.where(k <= 2 * low, paired, past)

    def hops(self, k):
        lows = [min(z, self.n - 1 - z) for z in range(self.n)]
        return sorted({(k + 1) // 2 if k <= 2 * low else k - low for low in lows})

    def by_line(self, z, p):
        near = jnp.logical_or(p == z + 1, p == z - 1)
        if self.n >= 4:
            near = jnp.logical_or(near, jnp.logical_and(z == 0, p == 2))
            near = jnp.logical_or(near, jnp.logical_and(z == self.n - 1, p == self.n - 3))
        return near

    def copy(self, src, dst, p, s, r, device):
        return pltpu.make_async_remote_copy(
            src_ref=src,
            dst_ref=dst,
            send_sem=self.send.at[p, s],
            recv_sem=self.recv.at[p, r],
            device_id=device,
            device_id_type=MESH,
        )

    def start(self, cond, src, dst, p, s, r, device):
        copy = self.copy(src, dst, p, s, r, device)
        if cond is None:
            copy.start()
        else:
            pl.when(cond)(copy.start)
        self.pending.append((cond, copy))

    def arrive(self, ref, p, r, now=None):
        copy = self.copy(ref, ref, p, 0, r, self.x_dev)
        if now is None:
            copy.wait_recv()
        else:
            pl.when(now)(copy.wait_recv)

    def column(self, k, halves=(0, 1), now=None):
        p = self.order[k]
        up = jnp.logical_and(p <= self.z, self.z < self.n - 1)
        down = jnp.logical_and(p >= self.z, self.z > 0)
        if now is not None:
            up, down = jnp.logical_and(now, up), jnp.logical_and(now, down)
        for h in halves:
            ref = self.piece(p, self.f, h)
            if k > 0:
                self.arrive(ref, p, h, now)
            self.start(now, ref, ref, p, 4 + h, 2 + h, self.x_dev)
            self.start(now, ref, ref, p, 6 + h, 4 + h, self.y_dev)
            self.start(up, ref, ref, p, h, h, self.up_dev)
            self.start(down, ref, ref, p, 2 + h, h, self.down_dev)

    def columns(self, distance, halves=(0, 1)):
        for k in range(1, self.n):
            hops = self.hops(k)
            if hops == [distance]:
                self.column(k, halves)
            elif distance in hops:
                away = self.order[k] - self.z
                now = jnp.logical_or(away == distance, away == -distance)
                self.column(k, halves, now)

    def sides(self, k, halves=(0, 1)):
        p = self.order[k]
        relay = jnp.logical_not(self.by_line(self.z, p))
        for h in halves:
            x_part = self.piece(p, self.fx, h)
            y_part = self.piece(p, self.fy, h)
            self.arrive(x_part, p, 2 + h)
            if h == 0:
                self.start(relay, x_part, x_part, p, 8, 6, self.y_dev)
            self.arrive(y_part, p, 4 + h)
            if h == 1:
                self.start(relay, y_part, y_part, p, 9, 7, self.x_dev)

    def diagonal(self, k, now=None):
        p = self.order[k]
        z, n = self.z, self.n
        up = jnp.logical_and(jnp.logical_and(p <= z, z < n - 1), self.by_line(z + 1, p))
        down = jnp.logical_and(jnp.logical_and(p >= z, z > 0), self.by_line(z - 1, p))
        if now is not None:
            up, down = jnp.logical_and(now, up), jnp.logical_and(now, down)
        for h in range(2):
            part = self.piece(p, self.fd, h)
            self.arrive(part, p, 6 + h, now)
            self.start(up, part, part, p, 10 + h, 6 + h, self.up_dev)
            self.start(down, part, part, p, 12 + h, 6 + h, self.down_dev)

    def diagonals(self, distance):
        for k in range(self.n):
            hops = self.hops(k)
            if hops == [distance]:
                self.diagonal(k)
            elif distance in hops:
                away = self.order[k] - self.z
                self.diagonal(k, jnp.logical_or(away == distance, away == -distance))

    def begin(self, i):
        if i < self.n:
            self.sides(i, (0,))
        if i + 1 < self.n:
            self.columns(i + 1, (0,))

    def cross(self, due):
        done = []
        while self.crossed < due:
            self.diagonals(self.crossed)
            done.append(self.order[self.crossed])
            self.crossed += 1
        return done

    def end(self, i):
        if i < self.n:
            self.sides(i, (1,))
        if i + 1 < self.n:
            self.columns(i + 1, (1,))
        return self.cross(1 if i == 1 else i - 1 if i >= 3 else 0)

    def stage(self, i):
        self.begin(i)
        return self.end(i)

    def drain(self):
        for cond, copy in self.pending:
            if cond is None:
                copy.wait_send()
            else:
                pl.when(cond)(copy.wait_send)


def layer_kernel(
    gate_ref,
    value_ref,
    key_ref,
    query_ref,
    pool_ref,
    t_ref,
    w_ssd_ref,
    w_pool_ref,
    norm_ref,
    step_ref,
    scale_ref,
    shift_ref,
    conv_value_ref,
    conv_key_ref,
    conv_query_ref,
    gain_ref,
    pool_mix_ref,
    pool_gain_ref,
    out_ref,
    mixed_in,
    others_in,
    w_out,
    toks,
    acc,
    gate,
    rows_ref,
    cols_ref,
    total_ref,
    taps,
    pad,
    act,
    y,
    ends,
    prior,
    finals,
    arrived,
    incoming,
    totals,
    squares,
    mixed,
    away,
    got,
    result,
    w_send,
    w_recv,
    local_sem,
    pair_sem,
    halo_sem,
    total_sem,
    state_sem,
    square_sem,
    part_sem,
    out_sem,
):
    length = toks.shape[0] - 2 * EDGE
    mine = t_ref.shape[0]
    half = length // 2
    groups = cols_ref.shape[0]
    lines = total_ref.shape[0]
    blocks = length // SPAN
    width = groups * STATE
    z = lax.axis_index("sp")
    f = lax.axis_index("fs")
    c = lax.axis_index("tp")
    n = lax.axis_size("sp")
    tile = (SPAN, 2 * HEAD_DIM)
    square = (SPAN, SPAN)
    f32 = jnp.float32
    across = (((1,), (1,)), ((), ()))

    rows = value_ref.shape[0]

    def rows_of(buf):
        def piece(p, member, h):
            at = pl.multiple_of(member * rows + h * (rows // 2), rows // 2)
            return buf.at[p, pl.ds(at, rows // 2)]

        return piece

    own_block = pl.ds(pl.multiple_of(f * rows, rows), rows)

    def columns_of(p, member, h):
        lot, cols = w_ssd_ref.shape
        at = pl.ds(pl.multiple_of((p * 4 + member) * cols, cols), cols)
        return w_out.at[pl.ds(h * lot, lot), at]

    first = LineGather(rows_of(mixed_in), w_send.at[0], w_recv.at[0])
    second = LineGather(rows_of(others_in), w_send.at[1], w_recv.at[1])
    third = LineGather(columns_of, w_send.at[2], w_recv.at[2])
    partner = (z, f, 1 - c)
    ahead = [(lax.rem(z + d, n), f, c) for d in range(n)]
    behind = [(lax.rem(z + n - d, n), f, c) for d in range(n)]

    def local(src, dst, i):
        copy = pltpu.make_async_copy(src, dst, local_sem.at[i])
        copy.start()
        return copy

    own_rows = toks.at[pl.ds(pl.multiple_of(EDGE + c * mine, EDGE), mine)]
    own_first = [
        local(ref, mixed_in.at[z, own_block, pl.ds(i * width, width)], i)
        for i, ref in enumerate((value_ref, key_ref, query_ref))
    ]
    own_tokens = local(t_ref, own_rows, 3)
    own_second = [
        local(ref, others_in.at[z, own_block, pl.ds(i * width, width)], 4 + i)
        for i, ref in enumerate((gate_ref, pool_ref))
    ]
    own_third = [
        local(ref, columns_of(z, f, h), 6 + h) for h, ref in enumerate((w_ssd_ref, w_pool_ref))
    ]
    first.barrier((partner, *ahead[2 : n - 1]))
    pending = []

    def remote(src, dst, sems, index, device, cond=None):
        copy = pltpu.make_async_remote_copy(
            src_ref=src,
            dst_ref=dst,
            send_sem=sems.at[(0, *index)],
            recv_sem=sems.at[(1, *index)],
            device_id=device,
            device_id_type=MESH,
        )
        if cond is None:
            copy.start()
        else:
            pl.when(cond)(copy.start)
        pending.append((cond, copy))
        return copy

    for copy in own_first:
        copy.wait()
    first.column(0)
    own_tokens.wait()
    pair = remote(t_ref, own_rows, pair_sem, (), partner)
    for copy in own_second + own_third:
        copy.wait()
    chunk = 32

    def normalize(start):
        def body(i, carry):
            at = pl.ds(pl.multiple_of(EDGE + start + i * chunk, EDGE), chunk)
            wide = toks[at, :].astype(jnp.float32)
            mean = jnp.mean(wide * wide, axis=-1, keepdims=True)
            toks[at, :] = (wide * lax.rsqrt(mean + EPSILON) * norm_ref[...]).astype(jnp.bfloat16)
            return carry

        lax.fori_loop(0, mine // chunk, body, 0)

    normalize(c * mine)
    first.sides(0, (0,))
    first.columns(1, (0,))
    pair.wait_recv()
    normalize((1 - c) * mine)
    below, above = z > 0, z < n - 1
    from_below = remote(
        toks.at[pl.ds(length, EDGE)], toks.at[pl.ds(0, EDGE)], halo_sem, (0,), ahead[1], above
    )
    from_above = remote(
        toks.at[pl.ds(EDGE, EDGE)],
        toks.at[pl.ds(EDGE + length, EDGE)],
        halo_sem,
        (1,),
        behind[1],
        below,
    )

    @pl.when(jnp.logical_not(below))
    def _():
        toks[:EDGE, :] = jnp.zeros((EDGE, toks.shape[1]), toks.dtype)

    @pl.when(jnp.logical_not(above))
    def _():
        toks[EDGE + length :, :] = jnp.zeros((EDGE, toks.shape[1]), toks.dtype)


    def lanes(i, count=1):
        return pl.ds(pl.multiple_of(i * STATE, STATE), count * STATE)

    def span(i):
        return pl.ds(pl.multiple_of(i * SPAN, SPAN), SPAN)

    def edged(i):
        return pl.ds(pl.multiple_of(EDGE + i * SPAN, EDGE), SPAN)

    def multiply(buf, p, begin=False, store=None):
        depth = buf.shape[1]
        at = pl.ds(pl.multiple_of(p * depth, depth), depth)
        wide = 256

        def body(i, carry):
            cols = pl.ds(pl.multiple_of(i * wide, wide), wide)
            for m in range(2):
                lot = half + EDGE
                part = jnp.dot(
                    toks[m * lot : (m + 1) * lot, at],
                    buf[p, :, cols],
                    preferred_element_type=f32,
                )
                if not begin:
                    part = part + acc[m * lot : (m + 1) * lot, cols]
                if store is None:
                    acc[m * lot : (m + 1) * lot, cols] = part
                else:
                    store(m, i, wide, part.astype(jnp.bfloat16))
            return carry

        count = buf.shape[2] // wide
        if store is None:
            lax.fori_loop(0, count, body, 0)
        else:
            for i in range(count):
                body(i, 0)

    def store_first(m, i, wide, part):
        lot = part.shape[0]
        pad[m * lot : (m + 1) * lot, i * wide : (i + 1) * wide] = part.astype(f32)

    def store_second(m, i, wide, part):
        lot = part.shape[0]
        if i * wide < width:
            gate[m * lot : (m + 1) * lot, i * wide : (i + 1) * wide] = part
        else:
            pad[m * lot : (m + 1) * lot, 2 * width + i * wide : 2 * width + (i + 1) * wide] = (
                part.astype(f32)
            )

    def step_sizes():
        raw = lax.dot_general(
            step_ref[...], toks[EDGE : EDGE + length, :], (((1,), (1,)), ((), ())), preferred_element_type=jnp.float32
        )
        raw = raw + scale_ref[:, :1]
        shift = jnp.concatenate([shift_ref[0, h] for h in range(shift_ref.shape[1])], axis=0)
        steps = jnp.maximum(raw, 0.0) + jnp.log1p(jnp.exp(-jnp.abs(raw)))
        logs = -scale_ref[:, SPAN : SPAN + 1] * steps - shift
        cut = [slice(i * SPAN, (i + 1) * SPAN) for i in range(blocks)]
        steps = jnp.concatenate([steps[:, at] for at in cut], axis=0)
        logs = jnp.concatenate([logs[:, at] for at in cut], axis=0)
        square = (SPAN, SPAN)
        upper = lax.broadcasted_iota(jnp.int32, square, 0) <= lax.broadcasted_iota(
            jnp.int32, square, 1
        )
        inner = jnp.dot(
            logs, upper.astype(jnp.float32), precision=HIGHEST, preferred_element_type=jnp.float32
        )
        total = inner[:, SPAN - 1 :]
        backward = lax.rem(lax.broadcasted_iota(jnp.int32, logs.shape, 0), 2) == 1
        along = inner - jnp.where(backward, logs, 0.0)
        weight = jnp.exp(jnp.where(backward, along, total - along)) * steps
        reach = jnp.exp(jnp.where(backward, total - along, along))
        rows_ref[0] = along
        rows_ref[1] = steps
        rows_ref[2] = jnp.broadcast_to(jnp.exp(total), logs.shape)
        whole = total[:lines]
        for i in range(1, blocks):
            whole = whole + total[i * lines : (i + 1) * lines]
        total_ref[...] = jnp.broadcast_to(whole, total_ref.shape)
        turned = [jnp.transpose(v) for v in (along, weight, reach)]
        for g in range(lines // 4):
            for i in range(blocks):
                for j in range(3):
                    at = i * lines + 4 * g
                    cols_ref[g, cut[i], 4 * j : 4 * j + 4] = turned[j][:, at : at + 4]

    order = first.order
    first.sides(0, (1,))
    first.columns(1, (1,))
    for i, ref in enumerate((conv_value_ref, conv_key_ref, conv_query_ref)):
        taps[:CONV_WIDTH, i * width : (i + 1) * width] = ref[
            :, pl.ds(pl.multiple_of(c * width, width), width)
        ].astype(f32)
    pl.when(below)(from_below.wait_recv)
    pl.when(above)(from_above.wait_recv)
    multiplied = []

    def advance_first(count):
        for _ in range(count):
            multiplied.append(order[len(multiplied)])
            multiply(
                mixed_in,
                multiplied[-1],
                begin=len(multiplied) == 1,
                store=store_first if len(multiplied) == n else None,
            )

    reached = 0
    for k in range(1, n + 1):
        for h in range(2) if k > 1 else ():
            first.sides(k - 1, (h,))
            first.columns(k, (h,))
        if k == 2:
            step_sizes()
        if k == n:
            second.column(0)
        due = 1 if k == 1 else 2 if k == 3 else n if k == n else reached
        while reached < due:
            first.diagonals(reached)
            reached += 1
            advance_first(1)

    sums = [
        remote(total_ref, totals.at[z], total_sem, (d - 1,), ahead[d]) for d in range(1, n)
    ]
    margin = CONV_WIDTH // 2

    def convolve(i, carry):
        at = lanes(i)
        tap = taps[:, at]
        for b in range(blocks):
            begin = EDGE - margin + b * SPAN
            total = pad[begin : begin + SPAN, at] * tap[:1]
            for o in range(1, CONV_WIDTH):
                total = total + pad[begin + o : begin + o + SPAN, at] * tap[o : o + 1]
            act[b * SPAN : (b + 1) * SPAN, at] = jax.nn.silu(total).astype(jnp.bfloat16)
        return carry

    lax.fori_loop(0, groups, convolve, 0)
    second.begin(0)
    lax.fori_loop(groups, 2 * groups, convolve, 0)
    queue = second.end(0)
    step = 4 if blocks % 4 == 0 else 1
    parts = blocks // step

    def block_ends(i, carry):
        g = i // parts
        for u in range(step):
            b = lax.rem(i, parts) * step + u
            at = span(b)
            x = act[at, lanes(g)].astype(f32)
            k = act[at, lanes(groups + g)]
            for r in range(2):
                weight = split_heads(
                    cols_ref[g, at, 4 + r : 5 + r], cols_ref[g, at, 6 + r : 7 + r], 1, tile
                )
                ends[g, r, b] = lax.dot_general(
                    (x * weight).astype(jnp.bfloat16),
                    k,
                    (((0,), (0,)), ((), ())),
                    preferred_element_type=f32,
                )
        return carry

    lax.fori_loop(0, groups * parts // 2, block_ends, 0)
    second.begin(1)
    lax.fori_loop(groups * parts // 2, groups * parts, block_ends, 0)

    def scan(g, r, start, each):
        order = range(blocks) if r == 0 else range(blocks - 1, -1, -1)
        carried = list(start)
        for b in order:
            each(b, carried)
            for h in range(2):
                at = b * lines + 4 * g + 2 * h + r
                scale = rows_ref[2, pl.ds(at, 1), :]
                carried[h] = carried[h] * scale + ends[g, r, b, h * HEAD_DIM : (h + 1) * HEAD_DIM]
        return carried

    def own_states(g, carry):
        zero = jnp.zeros((HEAD_DIM, STATE), f32)
        for r in range(2):
            last = scan(g, r, [zero, zero], lambda b, carried: None)
            for h in range(2):
                finals[r, g, h * HEAD_DIM : (h + 1) * HEAD_DIM] = last[h].astype(jnp.bfloat16)
        return carry

    lax.fori_loop(0, groups, own_states, 0)
    states = []
    for d in range(1, n):
        states.append(
            (
                remote(finals.at[0], arrived.at[0, d - 1], state_sem, (0, d - 1), ahead[d], z + d < n),
                remote(finals.at[1], arrived.at[1, d - 1], state_sem, (1, d - 1), behind[d], z >= d),
            )
        )
    queue += second.end(1)
    lax.fori_loop(2 * groups, 3 * groups, convolve, 0)
    if n >= 3:
        queue += second.stage(2)
    third.column(0)
    taken = [0]

    def advance():
        while queue:
            p = queue.pop(0)
            taken[0] += 1
            multiply(
                others_in,
                p,
                begin=taken[0] == 1,
                store=store_second if taken[0] == n else None,
            )

    advance()
    later = lax.broadcasted_iota(jnp.int32, square, 0)
    sooner = lax.broadcasted_iota(jnp.int32, square, 1)

    def diagonal_blocks(i, carry):
        g = i // parts
        lower = later >= sooner
        equal = later == sooner
        for u in range(step):
            b = lax.rem(i, parts) * step + u
            at = span(b)
            x = act[at, lanes(g)]
            scores = lax.dot_general(
                act[at, lanes(2 * groups + g)],
                act[at, lanes(groups + g)],
                across,
                preferred_element_type=f32,
            )
            outs = []
            for h in range(2):
                line = b * lines + 4 * g + 2 * h
                cf_l = cols_ref[g, at, 2 * h : 2 * h + 1]
                eb_l = cols_ref[g, at, 2 * h + 1 : 2 * h + 2]
                cf_s = rows_ref[0, pl.ds(line, 1), :]
                eb_s = rows_ref[0, pl.ds(line + 1, 1), :]
                df_s = rows_ref[1, pl.ds(line, 1), :]
                db_s = rows_ref[1, pl.ds(line + 1, 1), :]
                decay = jnp.exp(jnp.where(lower, cf_l - cf_s, eb_s - eb_l))
                size = jnp.where(equal, df_s + db_s, jnp.where(lower, df_s, db_s))
                outs.append(
                    jnp.dot(
                        (scores * decay * size).astype(jnp.bfloat16), x, preferred_element_type=f32
                    )
                )
            y[at, lanes(g)] = split_heads(outs[0], outs[1], 1, tile)
        return carry

    count = groups * parts
    lax.fori_loop(0, count // 4, diagonal_blocks, 0)
    if n >= 4:
        second.begin(3)
    lax.fori_loop(count // 4, count // 2, diagonal_blocks, 0)
    if n >= 4:
        queue += second.end(3)
    third.begin(0)
    lax.fori_loop(count // 2, 3 * count // 4, diagonal_blocks, 0)
    queue += second.cross(n)
    third.end(0)
    lax.fori_loop(3 * count // 4, count, diagonal_blocks, 0)
    third.begin(1)
    advance()
    third.end(1)

    def pooled(i, carry):
        where_global = (
            z * length + i * SPAN + lax.broadcasted_iota(jnp.int32, (SPAN, POOL_DIM), 0)
        )
        for j in range(groups):
            window = WINDOWS[j % 4]
            at = slice(3 * width + j * POOL_DIM, 3 * width + (j + 1) * POOL_DIM)
            block = pad[pl.ds(pl.multiple_of(i * SPAN, SPAN), SPAN + 2 * EDGE), at]
            first = EDGE - window // 2
            running = block[first : first + SPAN]
            for o in range(1, window):
                running = running + block[first + o : first + o + SPAN]
            lower = jnp.maximum(where_global - window // 2, 0)
            upper = jnp.minimum(where_global + window - window // 2, n * length)
            mean = running / (upper - lower).astype(f32)
            diff = (mean - block[EDGE : EDGE + SPAN]).astype(jnp.bfloat16)
            mapped = jnp.dot(diff, pool_mix_ref[c * groups + j], preferred_element_type=f32)
            gain = pool_gain_ref[:, lanes(c * groups + j)]
            mixed[span(i), width + j * POOL_DIM : width + (j + 1) * POOL_DIM] = (
                mapped * gain
            ).astype(jnp.bfloat16)
        return carry

    lax.fori_loop(0, blocks, pooled, 0)
    if n >= 3:
        third.begin(2)
    incoming[...] = jnp.zeros(incoming.shape, f32)
    for copy in sums:
        copy.wait_recv()
    for d in range(1, n):
        for r in range(2):

            def receive(d=d, r=r):
                states[d - 1][r].wait_recv()
                log = jnp.zeros(total_ref.shape, f32)
                for e in range(1, d):
                    log = log + totals[z - e if r == 0 else z + e]
                scale = jnp.exp(log)
                for g in range(groups):
                    for h in range(2):
                        line = 4 * g + 2 * h + r
                        at = slice(h * HEAD_DIM, (h + 1) * HEAD_DIM)
                        incoming[g, r, at] = incoming[g, r, at] + scale[
                            line : line + 1
                        ] * arrived[r, d - 1, g, at].astype(f32)

            pl.when(z >= d if r == 0 else z + d < n)(receive)
    squares[0] = jnp.zeros(squares.shape[1:], f32)

    def outputs(g, carry):
        for r in range(2):

            def keep(b, carried, r=r):
                for h in range(2):
                    prior[b, r * STATE + h * HEAD_DIM : r * STATE + (h + 1) * HEAD_DIM] = carried[
                        h
                    ].astype(jnp.bfloat16)

            scan(g, r, [incoming[g, r, :HEAD_DIM], incoming[g, r, HEAD_DIM:]], keep)
        for b in range(blocks):
            at = span(b)
            far = lax.dot_general(
                act[at, lanes(2 * groups + g)], prior[b], across, preferred_element_type=f32
            )
            out = y[at, lanes(g)]
            for r in range(2):
                reach = split_heads(
                    cols_ref[g, at, 8 + r : 9 + r], cols_ref[g, at, 10 + r : 11 + r], 1, tile
                )
                out = out + reach * far[:, r * STATE : (r + 1) * STATE]
            out = out * jax.nn.silu(gate[edged(b), lanes(g)].astype(f32))
            y[at, lanes(g)] = out
            squares[0, at] = squares[0, at] + jnp.sum(out * out, axis=-1, keepdims=True)
        return carry

    if n >= 3:
        third.end(2)
    lax.fori_loop(0, groups // 2, outputs, 0)
    if n >= 4:
        third.begin(3)
    lax.fori_loop(groups // 2, groups, outputs, 0)
    other = remote(squares.at[0], squares.at[1], square_sem, (), partner)
    if n >= 4:
        third.end(3)
    other.wait_recv()

    def scale_rows(b, carry):
        at = span(b)
        scale = lax.rsqrt((squares[0, at] + squares[1, at]) / (2 * width) + EPSILON)
        for g in range(groups):
            mixed[at, g * STATE : (g + 1) * STATE] = (
                y[at, g * STATE : (g + 1) * STATE] * scale * gain_ref[:, lanes(c * groups + g)]
            ).astype(jnp.bfloat16)
        return carry

    lax.fori_loop(0, blocks, scale_rows, 0)
    part = result.shape[1] // n
    wide = part // 2

    def product(head, target, p):
        for i in range(2):
            at = pl.ds(pl.multiple_of(p * part + i * wide, wide), wide)
            target[:, at] = jnp.dot(
                mixed[pl.ds(pl.multiple_of(head, half), half), :],
                w_out[:, at],
                preferred_element_type=f32,
            ).astype(jnp.bfloat16)

    sent, written = [], []

    def finish(k):
        p = third.order[k]
        product(c * half, result, p)
        sent[k].wait_recv()
        at = pl.ds(pl.multiple_of(p * part, part), part)
        result[:, at] = (result[:, at].astype(f32) + got[:, at].astype(f32)).astype(jnp.bfloat16)
        copy = pltpu.make_async_copy(result.at[:, at], out_ref.at[:, at], out_sem.at[k])
        copy.start()
        written.append(copy)

    for k in range(n):
        third.cross(k + 1)
        p = third.order[k]
        product((1 - c) * half, away, p)
        ref = pl.ds(pl.multiple_of(p * part, part), part)
        sent.append(remote(away.at[:, ref], got.at[:, ref], part_sem, (k,), partner))
        if k > 0:
            finish(k - 1)
    finish(n - 1)
    for copy in written:
        copy.wait()
    for cond, copy in pending:
        if cond is None:
            copy.wait_send()
        else:
            pl.when(cond)(copy.wait_send)
    for gather in (first, second, third):
        gather.drain()


def fused_layer(weights, tokens, w_ssd, w_pool, small, groups):
    n = lax.axis_size("sp")
    half, features = tokens.shape
    length = 2 * half
    width = groups * STATE
    lines = 4 * groups
    blocks = length // SPAN
    rows = weights[0].shape[0]
    out_rows, out_cols = 2 * w_ssd.shape[0], 4 * n * w_ssd.shape[1]
    anywhere = pl.BlockSpec(memory_space=pl.ANY)
    inside = pl.BlockSpec(memory_space=pltpu.VMEM)
    bf16, f32 = jnp.bfloat16, jnp.float32
    dma = pltpu.SemaphoreType.DMA
    return pl.pallas_call(
        layer_kernel,
        out_shape=jax.ShapeDtypeStruct((half, out_cols), bf16),
        in_specs=[anywhere] * 8 + [inside] * len(small),
        out_specs=anywhere,
        scratch_shapes=[
            pltpu.VMEM((n, 4 * rows, 3 * width), bf16),
            pltpu.VMEM((n, 4 * rows, 2 * width), bf16),
            pltpu.VMEM((out_rows, out_cols), bf16),
            pltpu.VMEM((length + 2 * EDGE, features), bf16),
            pltpu.VMEM((length + 2 * EDGE, 3 * width), f32),
            pltpu.VMEM((length + 2 * EDGE, width), bf16),
            pltpu.VMEM((3, lines * blocks, SPAN), f32),
            pltpu.VMEM((groups, length, 12), f32),
            pltpu.VMEM((lines, SPAN), f32),
            pltpu.VMEM((8, 3 * width), f32),
            pltpu.VMEM((length + 2 * EDGE, 4 * width), f32),
            pltpu.VMEM((length, 3 * width), bf16),
            pltpu.VMEM((length, width), f32),
            pltpu.VMEM((groups, 2, blocks, STATE, STATE), f32),
            pltpu.VMEM((blocks, 2 * STATE, STATE), bf16),
            pltpu.VMEM((2, groups, STATE, STATE), bf16),
            pltpu.VMEM((2, n - 1, groups, STATE, STATE), bf16),
            pltpu.VMEM((groups, 2, STATE, STATE), f32),
            pltpu.VMEM((n, lines, SPAN), f32),
            pltpu.VMEM((2, length, SPAN), f32),
            pltpu.VMEM((length, 2 * width), bf16),
            pltpu.VMEM((half, out_cols), bf16),
            pltpu.VMEM((half, out_cols), bf16),
            pltpu.VMEM((half, out_cols), bf16),
            dma((3, n, 14)),
            dma((3, n, 8)),
            dma((8,)),
            dma((2,)),
            dma((2, 2)),
            dma((2, n - 1)),
            dma((2, 2, n - 1)),
            dma((2,)),
            dma((2, n)),
            dma((n,)),
        ],
        compiler_params=pltpu.CompilerParams(
            collective_id=0, has_side_effects=True, vmem_limit_bytes=VMEM_LIMIT
        ),
        name="mixer",
    )(*weights, tokens, w_ssd, w_pool, *small)


def split_heads(first, second, axis, shape):
    places = lax.broadcasted_iota(jnp.int32, shape, axis)
    return jnp.where(places < HEAD_DIM, first, second)


def ends_kernel(blocks, decay_ref, x_ref, k_ref, col_ref, ends_ref, final_ref):
    group = pl.program_id(0)
    tile = (SPAN, 2 * HEAD_DIM)
    for c in range(blocks):
        rows = pl.ds(c * SPAN, SPAN)
        x = x_ref[rows, :].astype(jnp.float32)
        k = k_ref[rows, :]
        for r in range(2):
            weight = split_heads(
                col_ref[0, rows, 4 + 2 * r : 5 + 2 * r],
                col_ref[0, rows, 5 + 2 * r : 6 + 2 * r],
                1,
                tile,
            )
            end = lax.dot_general(
                (x * weight).astype(jnp.bfloat16),
                k,
                (((0,), (0,)), ((), ())),
                preferred_element_type=jnp.float32,
            )
            ends_ref[0, r, c] = end
    states = (2 * HEAD_DIM, STATE)
    for r in range(2):
        total = jnp.zeros(states, jnp.float32)
        for c in range(blocks) if r == 0 else range(blocks - 1, -1, -1):
            at = ((group * blocks + c) * 2 + r) * 2
            scale = split_heads(decay_ref[at], decay_ref[at + 1], 0, states)
            total = total * scale + ends_ref[0, r, c]
        final_ref[0, r] = total


def outputs_kernel(
    blocks, decay_ref, x_ref, k_ref, q_ref, col_ref, row_ref, ends_ref, in_ref, y_ref, prior
):
    group = pl.program_id(0)
    states = (2 * HEAD_DIM, STATE)
    tile = (SPAN, 2 * HEAD_DIM)
    square = (SPAN, SPAN)
    for r in range(2):
        total = in_ref[0, r]
        for c in range(blocks) if r == 0 else range(blocks - 1, -1, -1):
            prior[r, c] = total.astype(jnp.bfloat16)
            at = ((group * blocks + c) * 2 + r) * 2
            scale = split_heads(decay_ref[at], decay_ref[at + 1], 0, states)
            total = total * scale + ends_ref[0, r, c]
    later = lax.broadcasted_iota(jnp.int32, square, 0)
    sooner = lax.broadcasted_iota(jnp.int32, square, 1)
    lower = later >= sooner
    equal = later == sooner
    across = (((1,), (1,)), ((), ()))
    for c in range(blocks):
        rows = pl.ds(c * SPAN, SPAN)
        x = x_ref[rows, :]
        q = q_ref[rows, :]
        scores = lax.dot_general(q, k_ref[rows, :], across, preferred_element_type=jnp.float32)
        parts = []
        for h in range(2):
            cf_l = col_ref[0, rows, 2 * h : 2 * h + 1]
            eb_l = col_ref[0, rows, 2 * h + 1 : 2 * h + 2]
            cf_s = row_ref[0, 4 * h : 4 * h + 1, rows]
            eb_s = row_ref[0, 4 * h + 1 : 4 * h + 2, rows]
            df_s = row_ref[0, 4 * h + 2 : 4 * h + 3, rows]
            db_s = row_ref[0, 4 * h + 3 : 4 * h + 4, rows]
            decay = jnp.exp(jnp.where(lower, cf_l - cf_s, eb_s - eb_l))
            step = jnp.where(equal, df_s + db_s, jnp.where(lower, df_s, db_s))
            parts.append(
                jnp.dot(
                    (scores * decay * step).astype(jnp.bfloat16),
                    x,
                    preferred_element_type=jnp.float32,
                )
            )
        out = split_heads(parts[0], parts[1], 1, tile)
        for r in range(2):
            reach = split_heads(
                col_ref[0, rows, 8 + 2 * r : 9 + 2 * r],
                col_ref[0, rows, 9 + 2 * r : 10 + 2 * r],
                1,
                tile,
            )
            out = out + reach * lax.dot_general(
                q, prior[r, c], across, preferred_element_type=jnp.float32
            )
        y_ref[rows, :] = out


def mixer(activated, width_ssd, width_key, steps, logs, sp_rank):
    length = activated.shape[0]
    heads = steps.shape[1]
    groups = width_key // STATE
    blocks = length // SPAN
    shaped = logs.reshape(2, heads, blocks, SPAN)
    ones = jnp.triu(jnp.ones((SPAN, SPAN), jnp.float32))
    inner = jnp.einsum("rhcs,sl->rhcl", shaped, ones, precision=HIGHEST)
    totals = inner[..., -1:]
    cf = inner[0]
    eb = inner[1] - shaped[1]
    wf = jnp.exp(totals[0] - cf) * steps[0].reshape(cf.shape)
    wb = jnp.exp(eb) * steps[1].reshape(cf.shape)
    reach_f = jnp.exp(cf)
    reach_b = jnp.exp(totals[1] - eb)

    def pair(a):
        return a.reshape(groups, 2, length)

    cf, eb, wf, wb, reach_f, reach_b = map(pair, (cf, eb, wf, wb, reach_f, reach_b))
    df, db = (pair(steps[0]), pair(steps[1]))
    packed = jnp.stack(
        [cf[:, 0], eb[:, 0], cf[:, 1], eb[:, 1]]
        + [wf[:, 0], wf[:, 1], wb[:, 0], wb[:, 1]]
        + [reach_f[:, 0], reach_f[:, 1], reach_b[:, 0], reach_b[:, 1]],
        axis=1,
    )
    cols = jnp.transpose(packed, (0, 2, 1))
    rows = jnp.stack(
        [cf[:, 0], eb[:, 0], df[:, 0], db[:, 0], cf[:, 1], eb[:, 1], df[:, 1], db[:, 1]], axis=1
    )
    block_logs = totals[..., 0]
    decays = jnp.exp(block_logs).reshape(2, groups, 2, blocks)
    decays = jnp.transpose(decays, (1, 3, 0, 2)).reshape(-1)
    smem = pl.BlockSpec(memory_space=pltpu.SMEM)
    x_blocks = width_ssd // STATE

    def wide(offset):
        return pl.BlockSpec((length, STATE), lambda g: (0, g + offset))

    col_spec = pl.BlockSpec((1, length, cols.shape[2]), lambda g: (g, 0, 0))
    ends_spec = pl.BlockSpec((1, 2, blocks, STATE, STATE), lambda g: (g, 0, 0, 0, 0))
    state_spec = pl.BlockSpec((1, 2, STATE, STATE), lambda g: (g, 0, 0, 0))
    ends, finals = pl.pallas_call(
        functools.partial(ends_kernel, blocks),
        grid=(groups,),
        out_shape=(
            jax.ShapeDtypeStruct((groups, 2, blocks, STATE, STATE), jnp.float32),
            jax.ShapeDtypeStruct((groups, 2, STATE, STATE), jnp.float32),
        ),
        in_specs=[smem, wide(0), wide(x_blocks), col_spec],
        out_specs=(ends_spec, state_spec),
        cost_estimate=pl.CostEstimate(
            flops=4 * length * groups * STATE * STATE,
            bytes_accessed=16 * length * groups * STATE,
            transcendentals=0,
        ),
        name="block_ends",
    )(decays, activated, activated, cols)
    device_totals = jnp.sum(block_logs, axis=-1)
    all_totals = lax.all_gather(
        device_totals[None].astype(jnp.bfloat16), "sp", axis=0, tiled=True
    ).astype(jnp.float32)
    states = jnp.transpose(finals, (1, 0, 2, 3)).reshape(2, heads, HEAD_DIM, STATE)
    forward_in, backward_in = prefix_states(all_totals, states.astype(jnp.bfloat16), sp_rank)
    incoming = jnp.stack([forward_in, backward_in]).reshape(2, groups, STATE, STATE)
    incoming = jnp.transpose(incoming, (1, 0, 2, 3))
    return pl.pallas_call(
        functools.partial(outputs_kernel, blocks),
        grid=(groups,),
        out_shape=jax.ShapeDtypeStruct((length, groups * STATE), jnp.float32),
        in_specs=[
            smem,
            wide(0),
            wide(x_blocks),
            wide(x_blocks + groups),
            col_spec,
            pl.BlockSpec((1, 8, length), lambda g: (g, 0, 0)),
            ends_spec,
            state_spec,
        ],
        out_specs=wide(0),
        scratch_shapes=[pltpu.VMEM((2, blocks, STATE, STATE), jnp.bfloat16)],
        cost_estimate=pl.CostEstimate(
            flops=10 * length * groups * STATE * STATE,
            bytes_accessed=40 * length * groups * STATE,
            transcendentals=2 * length * groups * SPAN,
        ),
        name="block_outputs",
    )(decays, activated, activated, activated, cols, rows, ends, incoming)


def prefix_states(all_totals, finals, rank):
    chain_length = all_totals.shape[0]
    device_ids = jnp.arange(chain_length, dtype=jnp.int32)[:, None]
    forward_cum = jnp.cumsum(all_totals[:, 0], axis=0)
    forward_mine = lax.dynamic_slice_in_dim(forward_cum - all_totals[:, 0], rank, 1, 0)
    forward_weight = jnp.exp(jnp.where(device_ids < rank, forward_mine - forward_cum, -jnp.inf))
    backward_cum = jnp.cumsum(all_totals[:, 1], axis=0)
    backward_mine = lax.dynamic_slice_in_dim(backward_cum, rank, 1, 0)
    backward_weight = jnp.exp(
        jnp.where(device_ids > rank, backward_cum - all_totals[:, 1] - backward_mine, -jnp.inf)
    )
    forward_in = jnp.zeros(finals.shape[1:], jnp.float32)
    backward_in = jnp.zeros(finals.shape[1:], jnp.float32)
    for d in range(1, chain_length):
        ahead = [(i, i + d) for i in range(chain_length - d)]
        back = [(i + d, i) for i in range(chain_length - d)]
        from_left = lax.ppermute(finals[0], "sp", ahead).astype(jnp.float32)
        from_right = lax.ppermute(finals[1], "sp", back).astype(jnp.float32)
        left = lax.dynamic_index_in_dim(forward_weight, jnp.maximum(rank - d, 0), 0, False)
        right = lax.dynamic_index_in_dim(
            backward_weight, jnp.minimum(rank + d, chain_length - 1), 0, False
        )
        forward_in = forward_in + left[:, None, None] * from_left
        backward_in = backward_in + right[:, None, None] * from_right
    return (forward_in, backward_in)


def local(
    tokens,
    norm_gain,
    w_gate,
    w_value,
    w_bkey,
    w_query,
    w_pool_in,
    w_step,
    step_bias,
    decay_rate,
    decay_shift,
    conv_value,
    conv_bkey,
    conv_query,
    mix_gain,
    pool_mix,
    pool_gain,
    w_out_ssd,
    w_out_pool,
):
    tp_count = lax.axis_size("tp")
    sp_count = lax.axis_size("sp")
    tp_rank = lax.axis_index("tp")
    sp_rank = lax.axis_index("sp")
    heads_dev = DUALITY_HEADS // tp_count
    groups_dev = GROUPS // tp_count
    pools_dev = POOL_GROUPS // tp_count
    width_ssd = heads_dev * HEAD_DIM
    width_key = groups_dev * STATE
    width_pool = pools_dev * POOL_DIM
    fast = (
        tp_count == 2
        and lax.axis_size("fs") == 4
        and 2 <= sp_count <= 4
        and w_gate.shape[0] % 128 == 0
        and w_out_ssd.shape[1] % 128 == 0
        and pools_dev == groups_dev
        and width_ssd == width_key
        and groups_dev % 4 == 0
        and 2 * tokens.shape[1] * 2 * heads_dev % (SPAN * SPAN) == 0
    )
    step_cols = lax.dynamic_slice_in_dim(w_step, tp_rank * heads_dev, heads_dev, 2)
    bias_dev = lax.dynamic_slice_in_dim(step_bias, tp_rank * heads_dev, heads_dev, 1)
    rate_dev = lax.dynamic_slice_in_dim(decay_rate, tp_rank * heads_dev, heads_dev, 1)
    if fast:
        lines = 2 * heads_dev
        scales = jnp.stack([bias_dev, rate_dev], axis=-1)
        scales = jnp.transpose(scales, (1, 0, 2)).reshape(lines, 2, 1)
        small = (
            norm_gain[None],
            jnp.transpose(step_cols, (2, 1, 0)).reshape(lines, -1),
            jnp.broadcast_to(scales, (lines, 2, SPAN)).reshape(lines, 2 * SPAN),
            decay_shift,
            conv_value,
            conv_bkey,
            conv_query,
            mix_gain[None],
            pool_mix,
            pool_gain[None],
        )
        return fused_layer(
            (w_gate, w_value, w_bkey, w_query, w_pool_in),
            tokens[0],
            w_out_ssd,
            w_out_pool,
            small,
            groups_dev,
        )[None]
    step_cols = step_cols.reshape(w_step.shape[0], 2 * heads_dev)
    weights = jnp.concatenate([w_gate, w_value, w_bkey, w_query, w_pool_in], axis=1)
    combined, widened = gather_inputs(weights, tokens[0])
    out_rows = lax.all_gather(
        jnp.concatenate([w_out_ssd, w_out_pool], axis=0), ("sp", "fs"), axis=1, tiled=True
    )
    widened = widened.astype(jnp.float32)
    scaling = lax.rsqrt(jnp.mean(widened * widened, axis=-1, keepdims=True) + EPSILON)
    normed = (widened * scaling * norm_gain).astype(jnp.bfloat16)
    stored = jnp.dot(normed, combined, preferred_element_type=jnp.float32).astype(jnp.bfloat16)
    raw_steps = jnp.dot(normed, step_cols, preferred_element_type=jnp.float32)
    length = stored.shape[0]
    padded = padded_2(stored[:, width_ssd:], (("sp", 0),), REACH)
    conv_cols = width_ssd + 2 * width_key
    taps = jnp.concatenate(
        [
            lax.dynamic_slice_in_dim(conv_value, tp_rank * width_ssd, width_ssd, 1),
            lax.dynamic_slice_in_dim(conv_bkey, tp_rank * width_key, width_key, 1),
            lax.dynamic_slice_in_dim(conv_query, tp_rank * width_key, width_key, 1),
        ],
        axis=1,
    ).astype(jnp.float32)
    margin = CONV_WIDTH // 2
    convolved = jnp.zeros((length, conv_cols), jnp.float32)
    for offset in range(CONV_WIDTH):
        begin = REACH - margin + offset
        convolved = (
            convolved
            + padded[begin : begin + length, :conv_cols].astype(jnp.float32) * taps[offset]
        )
    activated = jax.nn.silu(convolved).astype(jnp.bfloat16)
    steps = jax.nn.softplus(raw_steps.reshape(length, 2, heads_dev) + bias_dev).transpose(1, 2, 0)
    logs = -rate_dev[:, :, None] * steps - decay_shift[0].transpose(1, 0, 2)
    heads_out = mixer(activated, width_ssd, width_key, steps, logs, sp_rank)
    gated = heads_out * jax.nn.silu(stored[:, :width_ssd].astype(jnp.float32))
    squares = lax.psum(jnp.sum(gated * gated, axis=-1), "tp")
    gain_dev = lax.dynamic_slice_in_dim(mix_gain, tp_rank * width_ssd, width_ssd, 0)
    ssd_mix = (gated * lax.rsqrt(squares / D_SSM + EPSILON)[:, None] * gain_dev).astype(
        jnp.bfloat16
    )
    pool_rows = padded[:, conv_cols:].astype(jnp.float32)
    own_rows = pool_rows[REACH : REACH + length]
    where_global = sp_rank * length + jnp.arange(length, dtype=jnp.int32)
    seq_length = length * sp_count
    window_means = []
    for window in WINDOWS:
        running = jnp.zeros((length, width_pool), jnp.float32)
        for offset in range(-(window // 2), window - window // 2):
            running = running + pool_rows[REACH + offset : REACH + offset + length]
        lower = jnp.clip(where_global - window // 2, 0, seq_length)
        upper = jnp.clip(where_global + window - window // 2, 0, seq_length)
        window_means.append(running / (upper - lower).astype(jnp.float32)[:, None])
    stacked = jnp.stack(window_means).reshape(4, length, pools_dev, POOL_DIM)
    group_ids = tp_rank * pools_dev + jnp.arange(pools_dev, dtype=jnp.int32)
    selector = (jnp.arange(4, dtype=jnp.int32)[:, None] == (group_ids % 4)[None, :]).astype(
        jnp.float32
    )
    means = jnp.sum(stacked * selector[:, None, :, None], axis=0)
    differences = (means - own_rows.reshape(length, pools_dev, POOL_DIM)).astype(jnp.bfloat16)
    pool_weights = lax.dynamic_slice_in_dim(pool_mix, tp_rank * pools_dev, pools_dev, 0)
    mapped = jnp.einsum(
        "rgc,gcd->rgd", differences, pool_weights, preferred_element_type=jnp.float32
    )
    pool_gain_dev = lax.dynamic_slice_in_dim(pool_gain, tp_rank * width_pool, width_pool, 0)
    pool_out = (mapped.reshape(length, width_pool) * pool_gain_dev).astype(jnp.bfloat16)
    mixed = jnp.concatenate([ssd_mix, pool_out], axis=1)
    if tp_count == 2:
        part = length // 2
        away = lax.dynamic_slice_in_dim(mixed, (1 - tp_rank) * part, part, 0)
        home = lax.dynamic_slice_in_dim(mixed, tp_rank * part, part, 0)
        sent = jnp.dot(away, out_rows, preferred_element_type=jnp.float32).astype(jnp.bfloat16)
        received = lax.ppermute(sent, "tp", [(0, 1), (1, 0)])
        kept = lax.optimization_barrier(
            jnp.dot(home, out_rows, preferred_element_type=jnp.float32).astype(jnp.bfloat16)
        )
        summed = (kept.astype(jnp.float32) + received.astype(jnp.float32)).astype(jnp.bfloat16)
    else:
        summed = lax.psum_scatter(
            jnp.dot(mixed, out_rows, preferred_element_type=jnp.float32).astype(jnp.bfloat16),
            "tp",
            scatter_dimension=0,
            tiled=True,
        )
    return summed[None]


def solution(mesh):
    return jax.shard_map(
        local,
        mesh=mesh,
        in_specs=(
            P("fs", ("sp", "tp"), None),
            P(),
            P(("sp", "fs"), "tp"),
            P(("sp", "fs"), "tp"),
            P(("sp", "fs"), "tp"),
            P(("sp", "fs"), "tp"),
            P(("sp", "fs"), "tp"),
            P(),
            P(),
            P(),
            P("fs", "tp", None, "sp"),
            P(),
            P(),
            P(),
            P(),
            P(),
            P(),
            P("tp", ("sp", "fs")),
            P("tp", ("sp", "fs")),
        ),
        out_specs=P("fs", ("sp", "tp"), None),
        check_vma=False,
    )
```
